32 devices in a mesh: kv: 8 (over z, x), tp: 4 (over y, core).
Axes of the slice: x: 2, y: 2, z: 4, core: 2. Of those that a mesh axis runs over, the one named last changes fastest.
Arguments:
- tokens: bfloat16 [16384, 2048], P('kv'), may hold values from -6 to 6
- norm_gain: bfloat16 [2048], replicated, may hold values from 0.099609375 to 1.8984375
- query_weight: bfloat16 [2048, 1024], P(None, 'tp'), may hold values from -0.125 to 0.125
- cmp_key_weight: bfloat16 [2048, 512], P(None, 'tp'), may hold values from -0.125 to 0.125
- cmp_value_weight: bfloat16 [2048, 512], P(None, 'tp'), may hold values from -0.125 to 0.125
- sel_key_weight: bfloat16 [2048, 512], P(None, 'tp'), may hold values from -0.125 to 0.125
- sel_value_weight: bfloat16 [2048, 512], P(None, 'tp'), may hold values from -0.125 to 0.125
- branch_weight: bfloat16 [2, 2048, 16], replicated, may hold values from -0.125 to 0.125
- key_embed: bfloat16 [8, 32, 64], P('tp'), may hold values from -3 to 3
- key_inner: bfloat16 [8, 2048, 64], P('tp'), may hold values from -0.125 to 0.125
- key_outer: bfloat16 [8, 64, 64], P('tp'), may hold values from -0.75 to 0.75
- value_embed: bfloat16 [8, 32, 64], P('tp'), may hold values from -3 to 3
- value_inner: bfloat16 [8, 2048, 64], P('tp'), may hold values from -0.125 to 0.125
- value_outer: bfloat16 [8, 64, 64], P('tp'), may hold values from -0.75 to 0.75
- out_weight: bfloat16 [1024, 2048], replicated, may hold values from -0.1875 to 0.1875
- chosen: int32 [8, 128, 8], P('tp'), may hold values from 0 to 255, as said below
Outputs:
- attended: bfloat16 [16384, 2048], P(('kv', 'tp'))
The draws below stay inside these ranges and needn't reach their ends.
Inputs may be any that keep to these rules, and one draw needn't show every extreme that they name: `chosen`: each entry is the index of a block of 64 positions in the whole sequence. For every key head and query block, its 8 entries lie in 8 different aligned spans of 2048 positions (at most one from any span), and none lies inside the query block's own positions.
All inputs are finite; a program needn't handle non-finite values.
Results may differ from the reference program's by a relative error of at most 0.0075.
Values may be sent and summed in bfloat16 or wider, within the bound.
A program may use at most 128 MiB of HBM per device.

```python
import jax
import jax.numpy as jnp
from jax import lax

D = 2048
HEADS = 16
KV_HEADS = 8
HEAD_DIM = 64
CMP_BLOCK = 32
SEL_BLOCK = 64
Q_BLOCK = 128
FAR_PICKS = 8
TOK_DEV = 2048
SEQ = 16384


def draw_chosen(key, part):
    interval_limits = SEQ // TOK_DEV
    per_span = TOK_DEV // Q_BLOCK
    span_blocks = TOK_DEV // SEL_BLOCK
    own_blocks = Q_BLOCK // SEL_BLOCK
    query_blocks = SEQ // Q_BLOCK
    key_noise, key_inner, key_shift = jax.random.split(key, 3)
    diagonal_group = jnp.arange(query_blocks, dtype=jnp.int32) // per_span
    local_index = jnp.arange(query_blocks, dtype=jnp.int32) % per_span
    eligible_group = jnp.arange(interval_limits, dtype=jnp.int32)
    jitter_perturbation = jax.random.randint(key_noise, (KV_HEADS, query_blocks, interval_limits), 0, 2 ** 16)
    preference_increment = jnp.where(eligible_group[None, :] <= diagonal_group[:, None], 2 ** 24, 0)
    preference_increment = preference_increment + jnp.where(eligible_group[None, :] == diagonal_group[:, None] - 1, 2 ** 26, 0)
    preference_increment = preference_increment + jnp.where(eligible_group[None, :] == diagonal_group[:, None] - interval_limits // 2, 2 ** 26, 0)
    preference_increment = preference_increment + jnp.where(eligible_group[None, :] == 0, 2 ** 25, 0)
    group_relevance = jitter_perturbation * interval_limits + eligible_group[None, None, :] + preference_increment[None]
    _, picked = lax.top_k(group_relevance, FAR_PICKS)
    inside = jax.random.randint(key_inner, (KV_HEADS, query_blocks, FAR_PICKS), 0, span_blocks)
    offset = jax.random.randint(key_shift, (KV_HEADS, query_blocks, FAR_PICKS), 0, span_blocks - own_blocks)
    shifted = (local_index[None, :, None] * own_blocks + own_blocks + offset) % span_blocks
    within = jnp.where(picked == diagonal_group[None, :, None], shifted, inside)
    return (picked * span_blocks + within).astype(jnp.int32)


def block_scale(rng, dims, pieces, smallest, top_value):
    def one(axis_at, blocks):
        draws = jax.random.uniform(jax.random.fold_in(jax.random.fold_in(rng, 6), axis_at), (blocks,), jnp.float32, smallest / len(pieces), top_value / len(pieces))
        return jnp.repeat(jnp.exp(draws), dims[axis_at] // blocks).reshape((-1,) + (1,) * (len(dims) - axis_at - 1))

    factor_of = one(*pieces[0])
    for cut in pieces[1:]:
        factor_of = factor_of * one(*cut)
    return factor_of


def bell_draw(own_key, shape, scale, bound, cuts=(), kind=jnp.bfloat16):
    level = block_scale(own_key, shape, cuts, -0.22, 0.18) if cuts else 1.0
    result = jax.random.normal(own_key, shape, jnp.float32) * scale * level
    return jnp.minimum(jnp.maximum(result, -bound), bound).astype(kind)


def setup_inputs(seed: int = 0) -> dict:
    splits = jax.random.split(jax.random.key(seed), 17)
    return {
        "tokens": bell_draw(splits[0], (SEQ, D), 1.0, 6.0, ((0, 8),)),
        "norm_gain": jnp.clip(1.0 + 0.18 * jax.random.normal(splits[1], (D,), jnp.float32), 0.099609375, 1.8984375).astype(jnp.bfloat16),
        "query_weight": bell_draw(splits[2], (D, HEADS * HEAD_DIM), D ** -0.5, 0.125, ((1, 4),)),
        "cmp_key_weight": bell_draw(splits[3], (D, KV_HEADS * HEAD_DIM), D ** -0.5, 0.125, ((1, 4),)),
        "cmp_value_weight": bell_draw(splits[4], (D, KV_HEADS * HEAD_DIM), D ** -0.5, 0.125, ((1, 4),)),
        "sel_key_weight": bell_draw(splits[5], (D, KV_HEADS * HEAD_DIM), D ** -0.5, 0.125, ((1, 4),)),
        "sel_value_weight": bell_draw(splits[6], (D, KV_HEADS * HEAD_DIM), D ** -0.5, 0.125, ((1, 4),)),
        "branch_weight": bell_draw(splits[7], (2, D, HEADS), D ** -0.5, 0.125),
        "key_embed": bell_draw(splits[8], (KV_HEADS, CMP_BLOCK, HEAD_DIM), 0.5, 3.0, ((0, 4),)),
        "key_inner": bell_draw(splits[9], (KV_HEADS, CMP_BLOCK * HEAD_DIM, HEAD_DIM), (CMP_BLOCK * HEAD_DIM) ** -0.5, 0.125, ((0, 4),)),
        "key_outer": bell_draw(splits[10], (KV_HEADS, HEAD_DIM, HEAD_DIM), HEAD_DIM ** -0.5, 0.75, ((0, 4),)),
        "value_embed": bell_draw(splits[11], (KV_HEADS, CMP_BLOCK, HEAD_DIM), 0.5, 3.0, ((0, 4),)),
        "value_inner": bell_draw(splits[12], (KV_HEADS, CMP_BLOCK * HEAD_DIM, HEAD_DIM), (CMP_BLOCK * HEAD_DIM) ** -0.5, 0.125, ((0, 4),)),
        "value_outer": bell_draw(splits[13], (KV_HEADS, HEAD_DIM, HEAD_DIM), HEAD_DIM ** -0.5, 0.75, ((0, 4),)),
        "out_weight": bell_draw(splits[14], (HEADS * HEAD_DIM, D), (HEADS * HEAD_DIM) ** -0.5, 0.1875),
        "chosen": draw_chosen(jax.random.fold_in(splits[16], 71), 0),
    }


ROPE_BASE = 10000.0
norm_eps = 1e-06
masked_score = -1000000000.0

def rotate(values_in, positions):
    half_dim = values_in.shape[-1] // 2
    inverse = ROPE_BASE ** (-jnp.arange(half_dim, dtype=jnp.float32) / half_dim)
    rotary_phases = positions.astype(jnp.float32)[:, None] * inverse[None, :]
    cosine = jnp.cos(rotary_phases)[:, None, :]
    sine = jnp.sin(rotary_phases)[:, None, :]
    first_half = values_in[..., :half_dim]
    second_half = values_in[..., half_dim:]
    return jnp.concatenate([first_half * cosine - second_half * sine, second_half * cosine + first_half * sine], axis=-1)

def summarize(raw_rows, embed, inner, outer):
    block_count = raw_rows.shape[0] // CMP_BLOCK
    blocked = raw_rows.reshape(block_count, CMP_BLOCK, KV_HEADS, HEAD_DIM).transpose(2, 0, 1, 3).astype(jnp.float32)
    blocked = (blocked + embed.astype(jnp.float32)[:, None]).astype(jnp.bfloat16)
    blocked = blocked.reshape(KV_HEADS, block_count, CMP_BLOCK * HEAD_DIM)
    hidden = jax.nn.gelu(jnp.einsum('knc,kce->kne', blocked.astype(jnp.float32), inner.astype(jnp.float32))).astype(jnp.bfloat16)
    return jnp.einsum('kne,kef->knf', hidden.astype(jnp.float32), outer.astype(jnp.float32)).astype(jnp.bfloat16)

def reference(tokens, norm_gain, query_weight, cmp_key_weight, cmp_value_weight, sel_key_weight, sel_value_weight, branch_weight, key_embed, key_inner, key_outer, value_embed, value_inner, value_outer, out_weight, chosen):
    length = tokens.shape[0]
    group_size = HEADS // KV_HEADS
    positions = jnp.arange(length, dtype=jnp.int32)
    scale = HEAD_DIM ** (-0.5)
    expanded_mask = tokens.astype(jnp.float32)
    normed = (expanded_mask * lax.rsqrt(lax.optimization_barrier(jnp.mean(expanded_mask * expanded_mask, axis=-1, keepdims=True)) + norm_eps) * norm_gain.astype(jnp.float32)).astype(jnp.bfloat16)

    def project(weight_in):
        return jnp.dot(normed, weight_in, preferred_element_type=jnp.float32)
    query = project(query_weight).reshape(length, HEADS, HEAD_DIM)
    q_plain = query.astype(jnp.bfloat16)
    q_turn = rotate(query, positions).astype(jnp.bfloat16)
    cmp_key = project(cmp_key_weight).astype(jnp.bfloat16).reshape(length, KV_HEADS, HEAD_DIM)
    cmp_value = project(cmp_value_weight).astype(jnp.bfloat16).reshape(length, KV_HEADS, HEAD_DIM)
    sel_key = rotate(project(sel_key_weight).reshape(length, KV_HEADS, HEAD_DIM), positions).astype(jnp.bfloat16)
    selected_value = project(sel_value_weight).astype(jnp.bfloat16).reshape(length, KV_HEADS, HEAD_DIM)
    gate_cmp = jax.nn.sigmoid(project(branch_weight[0]))
    gate_sel = jax.nn.sigmoid(project(branch_weight[1]))
    summary_key = summarize(cmp_key, key_embed, key_inner, key_outer)
    summary_value = summarize(cmp_value, value_embed, value_inner, value_outer)
    summary_count = summary_key.shape[1]
    block_end = (jnp.arange(summary_count, dtype=jnp.int32) + 1) * CMP_BLOCK - 1

    def compress_head(packed_rows):
        head_query, head_keys, head_values = packed_rows
        scores = jnp.einsum('tgd,cd->tgc', head_query.astype(jnp.float32), head_keys.astype(jnp.float32)) * scale
        allowed_keys = (block_end[None, :] <= positions[:, None])[:, None, :]
        probs = jax.nn.softmax(jnp.where(allowed_keys, scores, masked_score), axis=-1) * allowed_keys.astype(jnp.float32)
        return jnp.einsum('tgc,cd->tgd', probs.astype(jnp.bfloat16).astype(jnp.float32), head_values.astype(jnp.float32))
    q_group = q_plain.reshape(length, KV_HEADS, group_size, HEAD_DIM).transpose(1, 0, 2, 3)
    out_cmp = lax.map(compress_head, (q_group, summary_key, summary_value))
    out_cmp = out_cmp.transpose(1, 0, 2, 3).reshape(length, HEADS, HEAD_DIM)
    query_blocks = length // Q_BLOCK
    block_pos = jnp.arange(query_blocks, dtype=jnp.int32)[:, None] * Q_BLOCK + jnp.arange(Q_BLOCK, dtype=jnp.int32)[None, :]

    def select_head(packed_rows):
        head_query, head_keys, head_values, head_picks = packed_rows
        far_keys = head_keys.reshape(-1, SEL_BLOCK, HEAD_DIM)[head_picks].reshape(query_blocks, FAR_PICKS * SEL_BLOCK, HEAD_DIM)
        far_values = head_values.reshape(-1, SEL_BLOCK, HEAD_DIM)[head_picks].reshape(query_blocks, FAR_PICKS * SEL_BLOCK, HEAD_DIM)
        all_keys = jnp.concatenate([head_keys.reshape(query_blocks, Q_BLOCK, HEAD_DIM), far_keys], axis=1)
        all_values = jnp.concatenate([head_values.reshape(query_blocks, Q_BLOCK, HEAD_DIM), far_values], axis=1)
        far_pos = (head_picks[:, :, None] * SEL_BLOCK + jnp.arange(SEL_BLOCK, dtype=jnp.int32)[None, None, :]).reshape(query_blocks, -1)
        key_pos = jnp.concatenate([block_pos, far_pos], axis=1)
        allowed_keys = key_pos[:, None, None, :] <= block_pos[:, :, None, None]
        scores = jnp.einsum('nqgd,nmd->nqgm', head_query.astype(jnp.float32), all_keys.astype(jnp.float32)) * scale
        probs = jax.nn.softmax(jnp.where(allowed_keys, scores, masked_score), axis=-1)
        return jnp.einsum('nqgm,nmd->nqgd', probs.astype(jnp.bfloat16).astype(jnp.float32), all_values.astype(jnp.float32))
    q_sel = q_turn.reshape(query_blocks, Q_BLOCK, KV_HEADS, group_size, HEAD_DIM).transpose(2, 0, 1, 3, 4)
    out_sel = lax.map(select_head, (q_sel, sel_key.transpose(1, 0, 2), selected_value.transpose(1, 0, 2), chosen.astype(jnp.int32)))
    out_sel = out_sel.transpose(1, 2, 0, 3, 4).reshape(length, HEADS, HEAD_DIM)
    mixed = (gate_cmp[..., None] * out_cmp + gate_sel[..., None] * out_sel).reshape(length, HEADS * HEAD_DIM).astype(jnp.bfloat16)
    return jnp.dot(mixed, out_weight, preferred_element_type=jnp.float32).astype(jnp.bfloat16)
```

```python
import functools

import numpy as np

import jax
import jax.numpy as jnp
from jax import lax
from jax.experimental import pallas as pl
from jax.experimental.pallas import tpu as pltpu
from jax.sharding import PartitionSpec as P

HEAD_DIM = 64
CMP_BLOCK = 32
SEL_BLOCK = 64
Q_BLOCK = 128
LANES = 2 * HEAD_DIM
PLANES = 4
TILE = 256
MESH = pl.DeviceIdType.MESH

ROPE_BASE = 10000.0
norm_eps = 1e-06
MASKED = -1e30

f32 = jnp.float32
bf16 = jnp.bfloat16


def low_lanes(shape):
    return lax.broadcasted_iota(jnp.int32, shape, len(shape) - 1) < HEAD_DIM


def nt_dot(a, b):
    return lax.dot_general(a, b, (((1,), (1,)), ((), ())), preferred_element_type=f32)


def swap(x):
    return pltpu.roll(x, HEAD_DIM, 1)


def turn(x, cosine, sine):
    half = HEAD_DIM // 2
    lane = lax.broadcasted_iota(jnp.int32, x.shape, 1)
    first = lax.rem(lane, HEAD_DIM) < half
    partner = jnp.where(first, pltpu.roll(x, LANES - half, 1), pltpu.roll(x, half, 1))
    return x * cosine + partner * sine


def gate_lanes(gate, first, shape):
    return jnp.where(low_lanes(shape), gate[:, first : first + 1], gate[:, first + 1 : first + 2])


def with_ones(keys):
    return jnp.where(low_lanes(keys.shape), jnp.ones_like(keys), keys)


def settle(out, rows):
    low = low_lanes((rows, LANES))
    value = jnp.where(low, swap(out[:rows]), out[rows:])
    total = jnp.where(low, out[:rows], swap(out[rows:]))
    return value, total


def layer_kernel(planes, pieces, *refs):
    (
        pick,
        gain_ref,
        ke_ref,
        ko_ref,
        ve_ref,
        vo_ref,
        tok_hbm,
        query_hbm,
        branch_hbm,
        ki_hbm,
        vi_hbm,
        wo_hbm,
        fine_hbm,
        coarse_hbm,
    ) = refs[:14]
    piece_hbm, refs = refs[14 : 14 + pieces], refs[14 + pieces :]
    out_ref, refs = refs[0], refs[1:]
    (
        own,
        sel,
        stage_x,
        stage_t,
        tok,
        normed,
        w_kv,
        w_q,
        w_gate,
        wo,
        fine,
        coarse,
        ki,
        vi,
        qp,
        qt,
        ck,
        cv,
        gate,
        sums,
        oc,
        mix,
        got,
        acc,
        tok_sem,
        local_sem,
        own_send,
        col_send,
        col_recv,
        x_send,
        t_send,
        sel_recv,
        sum_send,
        sum_recv,
        mix_send,
        mix_recv,
    ) = refs[:36]
    col = refs[36:]

    kv_local = own.shape[0]
    span = own.shape[1]
    owners, ranks = sums.shape[0], got.shape[0]
    rows, width = tok.shape
    across = owners // planes
    last = planes - 1
    q_blocks = rows // Q_BLOCK
    all_blocks = owners * q_blocks
    blocks = rows // CMP_BLOCK
    tiles = rows // TILE
    rank_rows = rows // ranks
    group = rank_rows // Q_BLOCK
    heads = branch_hbm.shape[1]
    heads_local = 2 * kv_local
    kv_width = kv_local * HEAD_DIM
    scale = HEAD_DIM ** (-0.5)
    me, rank = lax.axis_index("kv"), lax.axis_index("tp")
    z, x = me // across, me % across

    barrier = pltpu.get_barrier_semaphore()
    for d in range(1, owners):
        pl.semaphore_signal(barrier, inc=1, device_id={"kv": (me + d) % owners}, device_id_type=MESH)
    for d in range(1, ranks):
        pl.semaphore_signal(barrier, inc=1, device_id={"tp": (rank + d) % ranks}, device_id_type=MESH)

    def rows_at(i):
        return pl.ds(pl.multiple_of(i * TILE, TILE), TILE)

    def tok_copy(i):
        return pltpu.make_async_copy(tok_hbm.at[rows_at(i)], tok.at[rows_at(i)], tok_sem.at[i])

    early = [(fine_hbm, fine), (coarse_hbm, coarse)]
    first = 0
    for ref in piece_hbm:
        early.append((ref, w_kv.at[:, pl.ds(first, ref.shape[1])]))
        first += ref.shape[1]
    late = [(ki_hbm, ki), (vi_hbm, vi), (query_hbm, w_q)]
    late += [(branch_hbm.at[b], w_gate.at[pl.ds(b * heads, heads)]) for b in range(2)]
    final = [(wo_hbm, wo)]
    copies = [
        pltpu.make_async_copy(a, b, local_sem.at[n]) for n, (a, b) in enumerate(early + late + final)
    ]
    tok_copy(0).start()
    for copy in copies[: len(early)]:
        copy.start()
    for i in range(1, tiles):
        tok_copy(i).start()
    for copy in copies[len(early) :]:
        copy.start()

    w_gate[2 * heads :, :] = jnp.zeros((w_gate.shape[0] - 2 * heads, width), bf16)
    moves = [(dz, dx) for dz in range(planes) for dx in range(across) if (dz, dx) != (0, 0)]

    def slot(dz, dx):
        return dz * across + dx - 1

    def present(dz, dx):
        return (x >= dx) if dz == 0 else (z >= dz)

    for dz, dx in moves:

        def clear(dz=dz, dx=dx):
            for k in range(kv_local):
                sel[slot(dz, dx), k] = jnp.zeros(sel.shape[2:], bf16)

        pl.when(jnp.logical_not(present(dz, dx)))(clear)


    def remote(src, dst, send, recv, target):
        return pltpu.make_async_remote_copy(
            src_ref=src,
            dst_ref=dst,
            send_sem=send,
            recv_sem=recv,
            device_id={"kv": target},
            device_id_type=MESH,
        )

    above = lax.rem(me + across, owners)

    def own_copy(k, at):
        return remote(own.at[k, at], col[k].at[at], own_send.at[k], col_recv.at[k, 0], above)

    def col_of(dz, k):
        return col[(dz - 1) * kv_local + k]

    def up_copy(dz, k):
        return remote(
            col_of(dz, k), col_of(dz + 1, k), col_send.at[k, dz], col_recv.at[k, dz], above
        )

    def side_copy(dz, dx, k):
        return remote(
            stage_x.at[dz, dx - 1, k],
            sel.at[slot(dz, dx), k],
            x_send.at[dz, dx - 1, k],
            sel_recv.at[slot(dz, dx), k, 0],
            z * across + (x + dx) % across,
        )

    def top_copy(dz, dx, k, step):
        at = pl.ds((rank + 1 + step) % ranks * group, group)
        return remote(
            stage_t.at[dz - 1, dx, k, at],
            sel.at[slot(dz + 1, dx), k, at],
            t_send.at[dz - 1, dx, k, step],
            sel_recv.at[slot(dz + 1, dx), k, step],
            lax.rem((z + 1) * across + (x + dx) % across, owners),
        )

    def gather(src, dst, source, k, device):
        base = (source * kv_local + k) * all_blocks + device * q_blocks

        def one(j, carry):
            dst[j] = src[jnp.maximum(pick[base + j], 0)]
            return carry

        lax.fori_loop(0, q_blocks, one, 0, unroll=4)

    def relay(dz, k):
        whole = (z >= dz) & ((z < last) | (dz == 1))

        def go():
            remote(col_of(dz, k), col_of(dz, k), own_send.at[k], col_recv.at[k, dz - 1], above).wait_recv()
            source = me - dz * across
            if dz + 1 < last:
                pl.when(z + 1 < last)(lambda: up_copy(dz, k).start())
            if dz + 1 <= last:

                def to_top():
                    for dx in range(across):
                        gather(
                            col_of(dz, k),
                            stage_t.at[dz - 1, dx, k],
                            source,
                            k,
                            (z + 1) * across + (x + dx) % across,
                        )
                    half = (ranks // 2) if dz + 1 == last and kv_local > 1 else ranks
                    sends = [(s, k) for s in range(half)]
                    if half < ranks and k == kv_local - 1:
                        sends += [(s, n) for s in range(half, ranks) for n in range(kv_local)]
                    for s, n in sends:
                        for dx in range(across):
                            top_copy(dz, dx, n, s).start()

                pl.when(z + 1 == last)(to_top)
            for dx in range(1, across):
                there = z * across + (x + dx) % across
                gather(col_of(dz, k), stage_x.at[dz, dx - 1, k], source, k, there)
                side_copy(dz, dx, k).start()
            gather(col_of(dz, k), sel.at[slot(dz, 0), k], source, k, me)

        pl.when(whole)(go)


    def norm_tile(i):
        t = tok[rows_at(i), :].astype(f32)
        inv = lax.rsqrt(jnp.mean(t * t, axis=-1, keepdims=True) + norm_eps)
        normed[rows_at(i), :] = (t * inv * gain_ref[...].astype(f32)).astype(bf16)

    def tables(i):
        row = pl.ds(me * tiles + i, 1)
        cos_c, sin_c = coarse[0, row, :], coarse[1, row, :]
        return fine[0] * cos_c - fine[1] * sin_c, fine[1] * cos_c + fine[0] * sin_c

    def project_kv(i):
        at = rows_at(i)
        y = jnp.dot(normed[at, :], w_kv[...], preferred_element_type=f32)
        cosine, sine = tables(i)
        here = pl.ds(i * (TILE // SEL_BLOCK), TILE // SEL_BLOCK)
        if kv_local == 1:
            pair = y[:, :LANES]
            packed = [jnp.where(low_lanes(pair.shape), turn(pair, cosine, sine), pair)]
        else:
            packed = []
            for k in range(0, kv_local, 2):
                key = turn(y[:, k * HEAD_DIM : k * HEAD_DIM + LANES], cosine, sine)
                value = y[:, kv_width + k * HEAD_DIM : kv_width + k * HEAD_DIM + LANES]
                low = low_lanes(key.shape)
                packed.append(jnp.where(low, key, swap(value)))
                packed.append(jnp.where(low, swap(key), value))
        for k in range(kv_local):
            own[k, here] = packed[k].astype(bf16).reshape(TILE // SEL_BLOCK, SEL_BLOCK, LANES)
        ck[at, :] = y[:, 2 * kv_width : 3 * kv_width].astype(bf16).astype(f32)
        cv[at, :] = y[:, 3 * kv_width : 4 * kv_width].astype(bf16).astype(f32)

    def send_tile(i):
        here = pl.ds(i * (TILE // SEL_BLOCK), TILE // SEL_BLOCK)
        if planes > 1:
            pl.when(z < last)(lambda: own_copy(0, here).start())

    tok_copy(0).wait()
    norm_tile(0)
    for copy in copies[: len(early)]:
        copy.wait()
    pl.semaphore_wait(barrier, owners + ranks - 2)

    def first_pass(i, carry):
        pl.when(i > 0)(lambda: send_tile(i - 1))
        tok_copy(i + 1).wait()
        norm_tile(i + 1)
        project_kv(i)
        return carry

    lax.fori_loop(0, tiles - 1, first_pass, 0)
    if tiles > 1:
        send_tile(tiles - 2)
    project_kv(tiles - 1)

    for copy in copies[len(early) : len(early) + len(late)]:
        copy.wait()
    send_tile(tiles - 1)


    def summarize(x_ref, e_ref, i_ref, o_ref):
        embed = jnp.concatenate([e_ref[k].astype(f32) for k in range(kv_local)], axis=1)
        parts = [
            x_ref[pl.ds(c, blocks, stride=CMP_BLOCK), :] + embed[c : c + 1] for c in range(CMP_BLOCK)
        ]
        result = []
        for k in range(kv_local):
            if kv_local == 1:
                flat = jnp.concatenate([p.astype(bf16) for p in parts], axis=1)
            else:
                g, odd = k // 2 * LANES, k % 2
                low = low_lanes((blocks, LANES))
                cut = []
                for c in range(0, CMP_BLOCK, 2):
                    a, b = parts[c][:, g : g + LANES], parts[c + 1][:, g : g + LANES]
                    both = jnp.where(low, swap(a), b) if odd else jnp.where(low, a, swap(b))
                    cut.append(both.astype(bf16))
                flat = jnp.concatenate(cut, axis=1)
            hidden = jax.nn.gelu(nt_dot(flat, i_ref[k])).astype(bf16)
            result.append(jnp.dot(hidden, o_ref[k], preferred_element_type=f32))
        return result

    sk = summarize(ck, ke_ref, ki, ko_ref)
    sv = summarize(cv, ve_ref, vi, vo_ref)
    for k in range(kv_local):
        sums[me, k] = jnp.concatenate([sk[k], sv[k]], axis=1).astype(bf16)

    def sum_copy(d, source):
        return remote(
            sums.at[source], sums.at[source], sum_send.at[d], sum_recv.at[d], (me + d) % owners
        )

    for dx in range(1, across):
        for k in range(kv_local):
            gather(own.at[k], stage_x.at[0, dx - 1, k], me, k, z * across + (x + dx) % across)
    for d in range(1, owners):
        sum_copy(d, me).start()
    everything = pl.ds(0, span)
    for k in range(1, kv_local):
        if planes > 1:
            pl.when(z < last)(lambda k=k: own_copy(k, everything).start())
    for dx in range(1, across):
        for k in range(kv_local):
            pl.when(x + dx < across)(lambda dx=dx, k=k: side_copy(0, dx, k).start())


    def second_pass(i, carry):
        at = rows_at(i)
        n = normed[at, :]
        y = jnp.dot(n, w_q[...], preferred_element_type=f32)
        cosine, sine = tables(i)
        for k in range(kv_local):
            v = y[:, k * LANES : (k + 1) * LANES] * scale
            low = low_lanes(v.shape)
            for ref, q in ((qp, v), (qt, turn(v, cosine, sine))):
                ref[k, 0, at, :] = jnp.where(low, q, 0.0).astype(bf16)
                ref[k, 1, at, :] = jnp.where(low, swap(q), 0.0).astype(bf16)
        g = jax.nn.sigmoid(nt_dot(n, w_gate[...]))
        gate[at, :] = pltpu.roll(g, lax.rem(LANES - rank * heads_local, LANES), 1)
        return carry

    lax.fori_loop(0, tiles, second_pass, 0)
    relays = [(dz, k) for dz in range(1, max(2, last)) for k in range(kv_local)] if planes > 1 else []
    if relays:
        relay(*relays[0])


    for d in range(1, owners):
        sum_copy(d, (me + owners - d) % owners).wait_recv()

    def compress(i, carry):
        at = rows_at(i)
        row = lax.broadcasted_iota(jnp.int32, (2 * TILE, 1), 0)
        pos = me * rows + i * TILE + jnp.where(row >= TILE, row - TILE, row)
        lane = lax.broadcasted_iota(jnp.int32, (1, owners * blocks), 1)
        allowed = (lane + 1) * CMP_BLOCK - 1 <= pos
        some = pos[:TILE] >= CMP_BLOCK - 1
        for k in range(kv_local):
            keys = jnp.concatenate([sums[s, k] for s in range(owners)], axis=0)
            q = jnp.concatenate([qp[k, 0, at, :], qp[k, 1, at, :]], axis=0)
            s = jnp.where(allowed, nt_dot(q, keys), MASKED)
            top = jnp.max(s, axis=-1, keepdims=True)
            e = jnp.exp(s - top).astype(bf16)
            o = jnp.dot(e, with_ones(keys), preferred_element_type=f32)
            value, total = settle(o, TILE)
            o = jnp.where(some, value / total, 0.0)
            oc[k, at, :] = o * gate_lanes(gate[at, :], 2 * k, o.shape)
        return carry

    bounds = [tiles * n // max(1, len(relays) - 1) for n in range(max(1, len(relays) - 1) + 1)]
    for n in range(len(bounds) - 1):
        lax.fori_loop(bounds[n], bounds[n + 1], compress, 0)
        if n + 1 < len(relays):
            relay(*relays[n + 1])


    def is_top(dz):
        return (z == last) & (dz >= 2)

    def wait_side(dz, dx, k):
        pl.when(present(dz, dx) & jnp.logical_not(is_top(dz)))(lambda: side_copy(dz, dx, k).wait_recv())

    for dz, dx in moves:
        if dx:
            for k in range(kv_local):
                wait_side(dz, dx, k)

    def mix_copy(step):
        target = (rank + 1 + step) % ranks
        at = pl.ds(pl.multiple_of(target * rank_rows, rank_rows), rank_rows)
        return pltpu.make_async_remote_copy(
            src_ref=mix.at[at],
            dst_ref=got.at[rank],
            send_sem=mix_send.at[step],
            recv_sem=mix_recv.at[step],
            device_id={"tp": target},
            device_id_type=MESH,
        )

    def add_rank(step):
        source = (rank + ranks - 1 - step) % ranks
        mix_copy(step).wait_recv()
        weight = pl.ds(pl.multiple_of(source * kv_local * LANES, LANES), kv_local * LANES)

        def part(i, carry):
            at = pl.ds(pl.multiple_of(i * Q_BLOCK, Q_BLOCK), Q_BLOCK)
            more = jnp.dot(got[source, at, :], wo[weight, :], preferred_element_type=f32)
            acc[at, :] = acc[at, :] + more
            return carry

        lax.fori_loop(0, group, part, 0)

    acc[...] = jnp.zeros_like(acc)
    copies[-1].wait()

    def choose(step, carry):
        pl.when(step > 0)(lambda: mix_copy(step - 1).start())
        target = (rank + 1 + step) % ranks
        pl.when(step > 1)(lambda: add_rank(step - 2))
        for dz, dx in moves:
            if dz >= 2:

                def wait_top(dz=dz, dx=dx):
                    for k in range(kv_local):
                        top_copy(dz - 1, dx, k, step).wait_recv()

                pl.when(is_top(dz))(wait_top)

        def block(u, carry):
            j = target * group + u
            at = pl.ds(pl.multiple_of(j * Q_BLOCK, Q_BLOCK), Q_BLOCK)
            here = me * q_blocks + j
            low = low_lanes((1, LANES))
            row = lax.broadcasted_iota(jnp.int32, (2 * Q_BLOCK, Q_BLOCK), 0)
            row = jnp.where(row >= Q_BLOCK, row - Q_BLOCK, row)
            lane = lax.broadcasted_iota(jnp.int32, row.shape, 1)
            for k in range(kv_local):
                parts = [own[k, j * (Q_BLOCK // SEL_BLOCK) + b] for b in range(Q_BLOCK // SEL_BLOCK)]
                mine = pick[(me * kv_local + k) * all_blocks + here]
                parts.append(own[k, jnp.maximum(mine, 0)])
                usable = [(mine >= 0) & (mine < j * (Q_BLOCK // SEL_BLOCK))]
                for dz, dx in moves:
                    parts.append(sel[slot(dz, dx), k, j])
                    source = lax.rem(me - dz * across - x + (x + across - dx) % across + owners, owners)
                    found = pick[(source * kv_local + k) * all_blocks + here] >= 0
                    usable.append(found & present(dz, dx))
                bias = [jnp.where(u, 0.0, MASKED).astype(f32) for u in usable]
                bias = jnp.concatenate(
                    [jnp.where(low, bias[n], bias[n + 1]) for n in range(0, len(bias), 2)], axis=1
                )
                keys = jnp.concatenate(parts, axis=0)
                q = jnp.concatenate([qt[k, 0, at, :], qt[k, 1, at, :]], axis=0)
                s = nt_dot(q, keys)
                near = jnp.where(lane > row, MASKED, s[:, :Q_BLOCK])
                s = jnp.concatenate([near, s[:, Q_BLOCK:] + bias], axis=1)
                top = jnp.max(s, axis=-1, keepdims=True)
                e = jnp.exp(s - top).astype(bf16)
                o = jnp.dot(e, with_ones(keys), preferred_element_type=f32)
                value, total = settle(o, Q_BLOCK)
                o = value / total
                g = gate_lanes(gate[at, :], heads + 2 * k, o.shape)
                mix[at, k * LANES : (k + 1) * LANES] = (oc[k, at, :] + o * g).astype(bf16)
            return carry

        lax.fori_loop(0, group, block, 0)
        return carry

    lax.fori_loop(0, ranks, choose, 0)


    if ranks > 1:
        add_rank(ranks - 2)
    mine = pl.ds(pl.multiple_of(rank * kv_local * LANES, LANES), kv_local * LANES)

    def finish(i, carry):
        at = pl.ds(pl.multiple_of(i * Q_BLOCK, Q_BLOCK), Q_BLOCK)
        from_mix = pl.ds(pl.multiple_of(rank * rank_rows + i * Q_BLOCK, Q_BLOCK), Q_BLOCK)
        more = jnp.dot(mix[from_mix, :], wo[mine, :], preferred_element_type=f32)
        out_ref[at, :] = (acc[at, :] + more).astype(bf16)
        return carry

    lax.fori_loop(0, group, finish, 0)


    for k in range(kv_local):
        if planes > 1:
            pl.when(z < last)(lambda k=k: own_copy(k, everything).wait_send())
        for dx in range(1, across):
            pl.when(x + dx < across)(lambda dx=dx, k=k: side_copy(0, dx, k).wait_send())
    for dz, k in relays:
        whole = (z >= dz) & ((z < last) | (dz == 1))
        if dz + 1 < last:
            pl.when(whole & (z + 1 < last))(lambda dz=dz, k=k: up_copy(dz, k).wait_send())
        if dz + 1 <= last:

            def sent_top(dz=dz, k=k):
                for s in range(ranks):
                    for dx in range(across):
                        top_copy(dz, dx, k, s).wait_send()

            pl.when(whole & (z + 1 == last))(sent_top)

        def sent_side(dz=dz, k=k):
            for dx in range(1, across):
                side_copy(dz, dx, k).wait_send()

        pl.when(whole)(sent_side)
    for d in range(1, owners):
        sum_copy(d, me).wait_send()
    for step in range(ranks - 1):
        mix_copy(step).wait_send()


def position_tables(rows, owners):
    half = HEAD_DIM // 2
    lane = np.arange(LANES)
    inverse = ROPE_BASE ** (-(lane % half).astype(np.float64) / half)
    sign = np.where(lane % HEAD_DIM < half, -1.0, 1.0)

    def both(positions):
        phase = positions[:, None].astype(np.float64) * inverse[None, :]
        return np.stack([np.cos(phase), np.sin(phase) * sign]).astype(np.float32)

    return both(np.arange(TILE)), both(np.arange(0, owners * rows, TILE))


def per_device(
    tokens,
    norm_gain,
    query_weight,
    cmp_key_weight,
    cmp_value_weight,
    sel_key_weight,
    sel_value_weight,
    branch_weight,
    key_embed,
    key_inner,
    key_outer,
    value_embed,
    value_inner,
    value_outer,
    out_weight,
    chosen,
):
    rows, width = tokens.shape
    kv_local = key_embed.shape[0]
    owners, ranks = lax.axis_size("kv"), lax.axis_size("tp")
    planes = PLANES if owners % PLANES == 0 else 1
    across = owners // planes
    span = rows // SEL_BLOCK
    q_blocks = rows // Q_BLOCK
    blocks = rows // CMP_BLOCK
    rank_rows = rows // ranks
    kv_width = kv_local * HEAD_DIM

    chosen = chosen.transpose(0, 2, 1)
    source = jnp.arange(owners, dtype=jnp.int32)[:, None, None, None]
    hit = chosen[None] // span == source
    picks = jnp.max(jnp.where(hit, chosen[None] % span, -1), axis=2).reshape(-1)

    weights = [sel_key_weight, sel_value_weight, cmp_key_weight, cmp_value_weight]
    if kv_width % LANES:
        weights = [jnp.concatenate(weights, axis=1)]
    fine, coarse = position_tables(rows, owners)
    operands = (
        picks,
        norm_gain.reshape(1, width),
        key_embed,
        key_outer,
        value_embed,
        value_outer,
        tokens,
        query_weight,
        branch_weight.transpose(0, 2, 1),
        key_inner.transpose(0, 2, 1),
        value_inner.transpose(0, 2, 1),
        out_weight,
        jnp.asarray(fine),
        jnp.asarray(coarse),
        *weights,
    )
    vmem = pl.BlockSpec(memory_space=pltpu.VMEM)
    hbm = pl.BlockSpec(memory_space=pl.ANY)
    dma = pltpu.SemaphoreType.DMA
    picked = (q_blocks, SEL_BLOCK, LANES)
    whole = (span, SEL_BLOCK, LANES)
    n_local = 2 + len(weights) + 5 + 1
    down = max(planes - 2, 1)
    return pl.pallas_call(
        functools.partial(layer_kernel, planes, len(weights)),
        in_specs=[pl.BlockSpec(memory_space=pltpu.SMEM)] + [vmem] * 5 + [hbm] * (8 + len(weights)),
        out_specs=vmem,
        out_shape=jax.ShapeDtypeStruct((rank_rows, out_weight.shape[1]), bf16),
        scratch_shapes=[
            pltpu.VMEM((kv_local, *whole), bf16),
            pltpu.VMEM((max(owners - 1, 1), kv_local, *picked), bf16),
            pltpu.VMEM((max(planes - 1, 1), max(across - 1, 1), kv_local, *picked), bf16),
            pltpu.VMEM((down, across, kv_local, *picked), bf16),
            pltpu.VMEM(tokens.shape, bf16),
            pltpu.VMEM(tokens.shape, bf16),
            pltpu.VMEM((width, 4 * kv_width), bf16),
            pltpu.VMEM(query_weight.shape, bf16),
            pltpu.VMEM((LANES, width), bf16),
            pltpu.VMEM(out_weight.shape, bf16),
            pltpu.VMEM(fine.shape, f32),
            pltpu.VMEM(coarse.shape, f32),
            pltpu.VMEM((kv_local, HEAD_DIM, key_inner.shape[1]), bf16),
            pltpu.VMEM((kv_local, HEAD_DIM, key_inner.shape[1]), bf16),
            pltpu.VMEM((kv_local, 2, rows, LANES), bf16),
            pltpu.VMEM((kv_local, 2, rows, LANES), bf16),
            pltpu.VMEM((rows, kv_width), f32),
            pltpu.VMEM((rows, kv_width), f32),
            pltpu.VMEM((rows, LANES), f32),
            pltpu.VMEM((owners, kv_local, blocks, LANES), bf16),
            pltpu.VMEM((kv_local, rows, LANES), f32),
            pltpu.VMEM((rows, kv_local * LANES), bf16),
            pltpu.VMEM((ranks, rank_rows, kv_local * LANES), bf16),
            pltpu.VMEM((rank_rows, out_weight.shape[1]), f32),
            dma((rows // TILE,)),
            dma((n_local,)),
            dma((kv_local,)),
            dma((kv_local, planes)),
            dma((kv_local, planes)),
            dma((max(planes - 1, 1), max(across - 1, 1), kv_local)),
            dma((down, across, kv_local, ranks)),
            dma((max(owners - 1, 1), kv_local, ranks)),
            dma((owners,)),
            dma((owners,)),
            dma((ranks,)),
            dma((ranks,)),
        ]
        + [pltpu.VMEM(whole, bf16)] * (kv_local * max(planes - 1, 1)),
        compiler_params=pltpu.CompilerParams(
            collective_id=0, has_side_effects=True, vmem_limit_bytes=62 * 1024 * 1024
        ),
        cost_estimate=pl.CostEstimate(flops=int(3e10), bytes_accessed=int(2e7), transcendentals=0),
        name="layer",
    )(*operands)


def solution(mesh):
    placed = (
        P("kv", None),
        P(),
        P(None, "tp"),
        P(None, "tp"),
        P(None, "tp"),
        P(None, "tp"),
        P(None, "tp"),
        P(),
        P("tp", None, None),
        P("tp", None, None),
        P("tp", None, None),
        P("tp", None, None),
        P("tp", None, None),
        P("tp", None, None),
        P(),
        P("tp", None, None),
    )
    return jax.shard_map(
        per_device, mesh=mesh, in_specs=placed, out_specs=P(("kv", "tp"), None), check_vma=False
    )
```

```python
import functools

import numpy as np

import jax
import jax.numpy as jnp
from jax import lax
from jax.experimental import pallas as pl
from jax.experimental.pallas import tpu as pltpu
from jax.sharding import PartitionSpec as P

HEAD_DIM = 64
CMP_BLOCK = 32
SEL_BLOCK = 64
Q_BLOCK = 128
LANES = 2 * HEAD_DIM
PLANES = 4
TILE = 256
ONES = 16
MESH = pl.DeviceIdType.MESH

ROPE_BASE = 10000.0
norm_eps = 1e-06
MASKED = -1e30

f32 = jnp.float32
bf16 = jnp.bfloat16


def low_lanes(shape):
    return lax.broadcasted_iota(jnp.int32, shape, len(shape) - 1) < HEAD_DIM


def nt_dot(a, b):
    return lax.dot_general(a, b, (((1,), (1,)), ((), ())), preferred_element_type=f32)


def swap(x):
    return pltpu.roll(x, HEAD_DIM, 1)


def turn(x, cosine, sine):
    half = HEAD_DIM // 2
    lane = lax.broadcasted_iota(jnp.int32, x.shape, 1)
    first = lax.rem(lane, HEAD_DIM) < half
    partner = jnp.where(first, pltpu.roll(x, LANES - half, 1), pltpu.roll(x, half, 1))
    return x * cosine + partner * sine


def pack_pair(keys, turned):
    rows = turned.shape[0]
    low = low_lanes((rows, LANES))
    return (
        jnp.where(low, keys[:rows], swap(turned)).astype(bf16),
        jnp.where(low, keys[rows:], turned).astype(bf16),
    )


def values_of(parts):
    low = low_lanes(parts[0].shape)
    pairs = [jnp.where(low, swap(parts[n]), parts[n + 1]) for n in range(0, len(parts), 2)]
    values = jnp.concatenate(pairs, axis=1)
    return jnp.concatenate([values, jnp.ones((ONES, values.shape[1]), values.dtype)], axis=0)


def layer_kernel(planes, pieces, *refs):
    (
        chosen_hbm,
        gain_hbm,
        ke_hbm,
        ko_hbm,
        ve_hbm,
        vo_hbm,
        tok_hbm,
        query_hbm,
        branch_hbm,
        ki_hbm,
        vi_hbm,
        wo_hbm,
        fine_hbm,
        coarse_hbm,
    ) = refs[:14]
    piece_hbm, refs = refs[14 : 14 + pieces], refs[14 + pieces :]
    out_ref, refs = refs[0], refs[1:]
    (
        pick,
        found,
        chosen_ref,
        gain_ref,
        gain_row,
        ke_ref,
        ko_ref,
        ve_ref,
        vo_ref,
        own,
        sel,
        part_out,
        part_top,
        stage_x,
        stage_t,
        tok,
        normed,
        w_kv,
        w_q,
        w_gate,
        w_own,
        wo,
        fine,
        coarse,
        ki,
        vi,
        qp,
        qt,
        vsum,
        ck,
        cv,
        gate,
        sums,
        oc,
        mix,
        got,
        acc,
        tok_sem,
        local_sem,
        own_send,
        col_send,
        col_recv,
        x_send,
        t_send,
        sel_recv,
        sum_send,
        sum_recv,
        mix_send,
        mix_recv,
    ) = refs[:49]
    col = refs[49:]

    kv_local = own.shape[0]
    span = own.shape[1]
    owners, ranks = sums.shape[0], got.shape[0]
    rows, width = normed.shape
    across = owners // planes
    last = planes - 1
    q_blocks = rows // Q_BLOCK
    all_blocks = owners * q_blocks
    blocks = rows // CMP_BLOCK
    tiles = rows // TILE
    ring = tok.shape[0]
    rank_rows = rows // ranks
    group = rank_rows // Q_BLOCK
    heads = branch_hbm.shape[1]
    heads_local = 2 * kv_local
    kv_width = kv_local * HEAD_DIM
    scale = HEAD_DIM ** (-0.5)
    me, rank = lax.axis_index("kv"), lax.axis_index("tp")
    z, x = me // across, me % across

    barrier = pltpu.get_barrier_semaphore()
    for d in range(1, owners):
        pl.semaphore_signal(barrier, inc=1, device_id={"kv": (me + d) % owners}, device_id_type=MESH)
    for d in range(1, ranks):
        pl.semaphore_signal(barrier, inc=1, device_id={"tp": (rank + d) % ranks}, device_id_type=MESH)

    def rows_at(i):
        return pl.ds(pl.multiple_of(i * TILE, TILE), TILE)

    def tok_copy(i):
        return pltpu.make_async_copy(tok_hbm.at[rows_at(i)], tok.at[lax.rem(i, ring)], tok_sem.at[i])

    early = [(gain_hbm, gain_ref), (fine_hbm, fine), (coarse_hbm, coarse)]
    first = 0
    for ref in piece_hbm:
        early.append((ref, w_kv.at[:, pl.ds(first, ref.shape[1])]))
        first += ref.shape[1]
    late = [(chosen_hbm, chosen_ref), (ki_hbm, ki), (vi_hbm, vi), (query_hbm, w_q)]
    late += [(ke_hbm, ke_ref), (ko_hbm, ko_ref), (ve_hbm, ve_ref), (vo_hbm, vo_ref)]
    late += [(branch_hbm.at[b], w_gate.at[pl.ds(b * heads, heads)]) for b in range(2)]
    final = [(wo_hbm, wo), (found, pick)]
    copies = [
        pltpu.make_async_copy(a, b, local_sem.at[n]) for n, (a, b) in enumerate(early + late + final)
    ]
    to_smem = copies.pop()
    tok_copy(0).start()
    for copy in copies[: len(early)]:
        copy.start()
    for i in range(1, min(ring, tiles)):
        tok_copy(i).start()
    for copy in copies[len(early) :]:
        copy.start()

    moves = [(dz, dx) for dz in range(planes) for dx in range(across) if (dz, dx) != (0, 0)]

    def slot(dz, dx):
        return dz * across + dx - 1

    def present(dz, dx):
        return (x >= dx) if dz == 0 else (z >= dz)

    for dz, dx in moves:

        def clear(dz=dz, dx=dx):
            for k in range(kv_local):
                sel[slot(dz, dx), k] = jnp.zeros(sel.shape[2:], bf16)

        pl.when(jnp.logical_not(present(dz, dx)))(clear)
    for d in range(1, owners):

        def clear_sums(d=d):
            for k in range(kv_local):
                sums[me + d, k] = jnp.zeros(sums.shape[2:], bf16)

        pl.when(me + d < owners)(clear_sums)


    def remote(src, dst, send, recv, target):
        return pltpu.make_async_remote_copy(
            src_ref=src,
            dst_ref=dst,
            send_sem=send,
            recv_sem=recv,
            device_id={"kv": target},
            device_id_type=MESH,
        )

    above = lax.rem(me + across, owners)

    def own_copy(k, at):
        return remote(own.at[k, at], col[k].at[at], own_send.at[k], col_recv.at[k, 0], above)

    def col_of(dz, k):
        return col[(dz - 1) * kv_local + k]

    def up_copy(dz, k):
        return remote(
            col_of(dz, k), col_of(dz + 1, k), col_send.at[k, dz], col_recv.at[k, dz], above
        )

    def side_copy(dz, dx, k):
        return remote(
            stage_x.at[dz, dx - 1, k],
            sel.at[slot(dz, dx), k],
            x_send.at[dz, dx - 1, k],
            sel_recv.at[slot(dz, dx), k, 0],
            z * across + (x + dx) % across,
        )

    def top_copy(dz, dx, k, step):
        at = pl.ds((rank + 1 + step) % ranks * group, group)
        return remote(
            stage_t.at[dz - 1, dx, k, at],
            sel.at[slot(dz + 1, dx), k, at],
            t_send.at[dz - 1, dx, k, step],
            sel_recv.at[slot(dz + 1, dx), k, step],
            lax.rem((z + 1) * across + (x + dx) % across, owners),
        )

    def gather(src, dst, source, k, device):
        row, base = source * kv_local + k, device * q_blocks

        def one(j, carry):
            dst[j] = src[jnp.maximum(pick[row, base + j], 0)]
            return carry

        lax.fori_loop(0, q_blocks, one, 0, unroll=4)

    def relay(dz, k):
        whole = (z >= dz) & ((z < last) | (dz == 1))

        def go():
            remote(col_of(dz, k), col_of(dz, k), own_send.at[k], col_recv.at[k, dz - 1], above).wait_recv()
            source = me - dz * across
            if dz + 1 < last:
                pl.when(z + 1 < last)(lambda: up_copy(dz, k).start())
            if dz + 1 <= last:

                def to_top():
                    for dx in range(across):
                        gather(
                            col_of(dz, k),
                            stage_t.at[dz - 1, dx, k],
                            source,
                            k,
                            (z + 1) * across + (x + dx) % across,
                        )
                    half = (ranks // 2) if dz + 1 == last and kv_local > 1 else ranks
                    sends = [(s, k) for s in range(half)]
                    if half < ranks and k == kv_local - 1:
                        sends += [(s, n) for s in range(half, ranks) for n in range(kv_local)]
                    for s, n in sends:
                        for dx in range(across):
                            top_copy(dz, dx, n, s).start()

                pl.when(z + 1 == last)(to_top)
            for dx in range(1, across):
                there = z * across + (x + dx) % across
                gather(col_of(dz, k), stage_x.at[dz, dx - 1, k], source, k, there)
                side_copy(dz, dx, k).start()
            gather(col_of(dz, k), sel.at[slot(dz, 0), k], source, k, me)

        pl.when(whole)(go)


    def norm_tile(i):
        t = tok[lax.rem(i, ring)].astype(f32)
        inv = lax.rsqrt(jnp.mean(t * t, axis=-1, keepdims=True) + norm_eps)
        normed[rows_at(i), :] = (t * inv * gain_row[...]).astype(bf16)
        pl.when(i + ring < tiles)(lambda: tok_copy(i + ring).start())

    def tables(i):
        row = pl.ds(me * tiles + i, 1)
        cos_c, sin_c = coarse[0, row, :], coarse[1, row, :]
        return fine[0] * cos_c - fine[1] * sin_c, fine[1] * cos_c + fine[0] * sin_c

    def project_kv(i):
        at = rows_at(i)
        y = jnp.dot(normed[at, :], w_kv[...], preferred_element_type=f32)
        cosine, sine = tables(i)
        for k in range(kv_local):
            if kv_local == 1:
                value = y[:, :LANES]
                key = turn(value, cosine, sine)
                keys, first = key, HEAD_DIM
            elif k % 2 == 0:
                key = turn(y[:, k * HEAD_DIM : k * HEAD_DIM + LANES], cosine, sine)
                value = y[:, kv_width + k * HEAD_DIM : kv_width + k * HEAD_DIM + LANES]
                keys, first = key, 0
            else:
                keys, first = swap(key), HEAD_DIM
            for t in range(TILE // (2 * SEL_BLOCK)):
                two = slice(t * 2 * SEL_BLOCK, (t + 1) * 2 * SEL_BLOCK)
                turned = value[two].T[first : first + HEAD_DIM]
                a, b = pack_pair(keys[two], turned)
                own[k, i * (TILE // SEL_BLOCK) + 2 * t] = a
                own[k, i * (TILE // SEL_BLOCK) + 2 * t + 1] = b
        ck[at, :] = y[:, 2 * kv_width : 3 * kv_width].astype(bf16).astype(f32)
        cv[at, :] = y[:, 3 * kv_width : 4 * kv_width].astype(bf16).astype(f32)

    def send_tile(i):
        here = pl.ds(i * (TILE // SEL_BLOCK), TILE // SEL_BLOCK)
        if planes > 1:
            pl.when(z < last)(lambda: own_copy(0, here).start())

    copies[0].wait()
    for c in range(gain_ref.shape[0]):
        gain_row[:, c * LANES : (c + 1) * LANES] = gain_ref[c : c + 1, :].astype(f32)
    tok_copy(0).wait()
    norm_tile(0)
    for copy in copies[1 : len(early)]:
        copy.wait()
    pl.semaphore_wait(barrier, owners + ranks - 2)

    def first_pass(i, carry):
        pl.when(i > 0)(lambda: send_tile(i - 1))
        tok_copy(i + 1).wait()
        norm_tile(i + 1)
        project_kv(i)
        return carry

    lax.fori_loop(0, tiles - 1, first_pass, 0)
    if tiles > 1:
        send_tile(tiles - 2)
    project_kv(tiles - 1)

    for copy in copies[len(early) : len(early) + len(late)]:
        copy.wait()
    send_tile(tiles - 1)


    for s in range(owners):
        for k in range(kv_local):
            place = chosen_ref[k] - s * span
            place = jnp.where((place >= 0) & (place < span), place, -1)
            found[s * kv_local + k : s * kv_local + k + 1, :] = jnp.max(place, axis=0, keepdims=True)
    to_smem.start()


    def summarize(x_ref, e_ref, i_ref, o_ref):
        embed = jnp.concatenate([e_ref[k].astype(f32) for k in range(kv_local)], axis=1)
        parts = [
            x_ref[pl.ds(c, blocks, stride=CMP_BLOCK), :] + embed[c : c + 1] for c in range(CMP_BLOCK)
        ]
        result = []
        for k in range(kv_local):
            if kv_local == 1:
                flat = jnp.concatenate([p.astype(bf16) for p in parts], axis=1)
            else:
                g, odd = k // 2 * LANES, k % 2
                low = low_lanes((blocks, LANES))
                cut = []
                for c in range(0, CMP_BLOCK, 2):
                    a, b = parts[c][:, g : g + LANES], parts[c + 1][:, g : g + LANES]
                    both = jnp.where(low, swap(a), b) if odd else jnp.where(low, a, swap(b))
                    cut.append(both.astype(bf16))
                flat = jnp.concatenate(cut, axis=1)
            hidden = jax.nn.gelu(nt_dot(flat, i_ref[k])).astype(bf16)
            result.append(jnp.dot(hidden, o_ref[k], preferred_element_type=f32))
        return result

    sk = summarize(ck, ke_ref, ki, ko_ref)
    sv = summarize(cv, ve_ref, vi, vo_ref)
    for k in range(kv_local):
        sums[me, k] = jnp.concatenate([sk[k], sv[k].T], axis=1).astype(bf16)

    def sum_up(dz, source):
        there = lax.rem(me + dz * across, owners)
        return remote(sums.at[source], sums.at[source], sum_send.at[0, dz], sum_recv.at[0, dz], there)

    def sum_side(dz, dx, source):
        there = z * across + (x + dx) % across
        return remote(sums.at[source], sums.at[source], sum_send.at[dx, dz], sum_recv.at[dx, dz], there)

    for dz in range(1, planes):
        pl.when(z + dz <= last)(lambda dz=dz: sum_up(dz, me).start())
    for dx in range(1, across):
        pl.when(x + dx < across)(lambda dx=dx: sum_side(0, dx, me).start())
    to_smem.wait()
    for dx in range(1, across):
        for k in range(kv_local):
            gather(own.at[k], stage_x.at[0, dx - 1, k], me, k, z * across + (x + dx) % across)
    everything = pl.ds(0, span)
    for k in range(1, kv_local):
        if planes > 1:
            pl.when(z < last)(lambda k=k: own_copy(k, everything).start())
    for dx in range(1, across):
        pl.when(x + dx < across)(lambda dx=dx: side_copy(0, dx, 0).start())


    mine = lax.broadcasted_iota(jnp.int32, (w_own.shape[0], w_gate.shape[0]), 0)
    branch = jnp.where(mine >= heads_local, 1, 0)
    wanted = branch * heads + rank * heads_local + mine - branch * heads_local
    wanted = jnp.where(mine < 2 * heads_local, wanted, -1)
    source = lax.broadcasted_iota(jnp.int32, mine.shape, 1)
    chooser = jnp.where(source == wanted, 1.0, 0.0).astype(bf16)
    w_own[...] = jnp.dot(chooser, w_gate[...], preferred_element_type=f32).astype(bf16)

    def second_pass(i, carry):
        at = rows_at(i)
        n = normed[at, :]
        y = jnp.dot(n, w_q[...], preferred_element_type=f32)
        cosine, sine = tables(i)
        for k in range(kv_local):
            v = y[:, k * LANES : (k + 1) * LANES] * scale
            low = low_lanes(v.shape)
            for ref, q in ((qp, v), (qt, turn(v, cosine, sine))):
                ref[k, 0, at, :] = jnp.where(low, q, 0.0).astype(bf16)
                ref[k, 1, at, :] = jnp.where(low, swap(q), 0.0).astype(bf16)
        gate[:, at] = jax.nn.sigmoid(nt_dot(w_own[...], n))
        return carry

    lax.fori_loop(0, tiles // 2, second_pass, 0)
    for dz in range(1, planes):

        def pass_on(dz=dz):
            below = me - dz * across
            sum_up(dz, below).wait_recv()
            for dx in range(1, across):
                sum_side(dz, dx, below).start()

        pl.when(z >= dz)(pass_on)
    lax.fori_loop(tiles // 2, tiles, second_pass, 0)
    relays = [(dz, k) for dz in range(1, max(2, last)) for k in range(kv_local)] if planes > 1 else []


    if relays:
        relay(*relays[0])
    for dx in range(1, across):
        for k in range(1, kv_local):
            pl.when(x + dx < across)(lambda dx=dx, k=k: side_copy(0, dx, k).start())
    for dz in range(planes):
        for dx in range(1, across):
            there = lax.rem((z - dz + planes) * across + (x + across - dx) % across, owners)
            pl.when(present(dz, dx))(
                lambda dz=dz, dx=dx, there=there: sum_side(dz, dx, there).wait_recv()
            )

    def gate_row(branch, head, at):
        return gate[branch * heads_local + head : branch * heads_local + head + 1, at]

    for k in range(kv_local):
        vsum[k] = values_of([sums[s, k] for s in range(owners)])

    def compress(i, carry):
        at = rows_at(i)
        lane = lax.broadcasted_iota(jnp.int32, (1, 2 * TILE), 1)
        pos = me * rows + i * TILE + jnp.where(lane >= TILE, lane - TILE, lane)
        block = lax.broadcasted_iota(jnp.int32, (owners * blocks, 1), 0)
        allowed = (block + 1) * CMP_BLOCK - 1 <= pos
        for k in range(kv_local):
            keys = jnp.concatenate([sums[s, k] for s in range(owners)], axis=0)
            q = jnp.concatenate([qp[k, 0, at, :], qp[k, 1, at, :]], axis=0)
            s = jnp.where(allowed, nt_dot(keys, q), MASKED)
            top = jnp.max(s, axis=0, keepdims=True)
            e = jnp.exp(s - top).astype(bf16)
            o = jnp.dot(vsum[k], e, preferred_element_type=f32)
            o = jnp.where(pos >= CMP_BLOCK - 1, o[:HEAD_DIM] / o[HEAD_DIM : HEAD_DIM + 1], 0.0)
            for u in range(2):
                part = o[:, u * TILE : (u + 1) * TILE] * gate_row(0, 2 * k + u, at)
                oc[k, u * HEAD_DIM : (u + 1) * HEAD_DIM, at] = part
        return carry

    bounds = [tiles * n // kv_local for n in range(kv_local + 1)]
    for k in range(kv_local):
        if k > 0 and planes > 1:
            relay(1, k)
        lax.fori_loop(bounds[k], bounds[k + 1], compress, 0)


    def is_top(dz):
        return (z == last) & (dz >= 2)

    def wait_side(dz, dx, k):
        pl.when(present(dz, dx) & jnp.logical_not(is_top(dz)))(lambda: side_copy(dz, dx, k).wait_recv())

    def bias_of(usable):
        return [jnp.where(u, 0.0, MASKED).astype(f32) for u in usable]

    def add_bias(s, bias):
        cut = [s[n * SEL_BLOCK : (n + 1) * SEL_BLOCK] + b for n, b in enumerate(bias)]
        return jnp.concatenate(cut, axis=0)

    def far_parts(some_moves, k, j):
        parts, usable = [], []
        for dz, dx in some_moves:
            parts.append(sel[slot(dz, dx), k, j])
            source = lax.rem(me - dz * across - x + (x + across - dx) % across + owners, owners)
            usable.append((pick[source * kv_local + k, me * q_blocks + j] >= 0) & present(dz, dx))
        return parts, usable

    near_moves = [m for m in moves if m[0] < 2]
    far_moves = [m for m in moves if m[0] >= 2]
    own_blocks = Q_BLOCK // SEL_BLOCK

    def queries(k, j):
        at = pl.ds(pl.multiple_of(j * Q_BLOCK, Q_BLOCK), Q_BLOCK)
        return jnp.concatenate([qt[k, 0, at, :], qt[k, 1, at, :]], axis=0)

    unroll = group if group < 4 else 4

    def near(k, some, carry):
        row = lax.broadcasted_iota(jnp.int32, (Q_BLOCK, 2 * Q_BLOCK), 0)
        lane = lax.broadcasted_iota(jnp.int32, row.shape, 1)
        lane = jnp.where(lane >= Q_BLOCK, lane - Q_BLOCK, lane)
        for u in range(unroll):
            j = some * unroll + u
            parts = [own[k, j * own_blocks + b] for b in range(own_blocks)]
            mine = pick[me * kv_local + k, me * q_blocks + j]
            parts.append(own[k, jnp.maximum(mine, 0)])
            more, usable = far_parts(near_moves, k, j)
            bias = bias_of([(mine >= 0) & (mine < j * own_blocks)] + usable)
            parts = parts + more
            s = nt_dot(jnp.concatenate(parts, axis=0), queries(k, j))
            close = jnp.where(row > lane, MASKED, s[:Q_BLOCK])
            s = jnp.concatenate([close, add_bias(s[Q_BLOCK:], bias)], axis=0)
            top = jnp.max(s, axis=0, keepdims=True)
            e = jnp.exp(s - top).astype(bf16)
            part_out[k, j] = jnp.dot(values_of(parts), e, preferred_element_type=f32)
            part_top[k, j] = top
        return carry

    for k in range(kv_local):
        for dz, dx in near_moves:
            if dx:
                wait_side(dz, dx, k)
        lax.fori_loop(0, q_blocks // unroll, functools.partial(near, k), 0)
        for dz in range(2, last):
            relay(dz, k)
    for dz, dx in far_moves:
        if dx:
            for k in range(kv_local):
                wait_side(dz, dx, k)

    def mix_copy(step):
        target = (rank + 1 + step) % ranks
        at = pl.ds(pl.multiple_of(target * rank_rows, rank_rows), rank_rows)
        return pltpu.make_async_remote_copy(
            src_ref=mix.at[at],
            dst_ref=got.at[rank],
            send_sem=mix_send.at[step],
            recv_sem=mix_recv.at[step],
            device_id={"tp": target},
            device_id_type=MESH,
        )

    def add_rank(step):
        source = (rank + ranks - 1 - step) % ranks
        mix_copy(step).wait_recv()
        weight = pl.ds(pl.multiple_of(source * kv_local * LANES, LANES), kv_local * LANES)

        def part(i, carry):
            at = pl.ds(pl.multiple_of(i * Q_BLOCK, Q_BLOCK), Q_BLOCK)
            more = jnp.dot(got[source, at, :], wo[weight, :], preferred_element_type=f32)
            acc[at, :] = acc[at, :] + more
            return carry

        lax.fori_loop(0, group, part, 0)

    acc[...] = jnp.zeros_like(acc)
    copies[-1].wait()

    def choose(step, carry):
        pl.when(step > 0)(lambda: mix_copy(step - 1).start())
        target = (rank + 1 + step) % ranks
        pl.when(step > 1)(lambda: add_rank(step - 2))
        for dz, dx in moves:
            if dz >= 2:

                def wait_top(dz=dz, dx=dx):
                    for k in range(kv_local):
                        top_copy(dz - 1, dx, k, step).wait_recv()

                pl.when(is_top(dz))(wait_top)

        def block(some, carry):
            for u, k in [(u, k) for u in range(unroll) for k in range(kv_local)]:
                j = target * group + some * unroll + u
                at = pl.ds(pl.multiple_of(j * Q_BLOCK, Q_BLOCK), Q_BLOCK)
                out, top = part_out[k, j], part_top[k, j]
                if far_moves:
                    parts, usable = far_parts(far_moves, k, j)
                    s = add_bias(nt_dot(jnp.concatenate(parts, axis=0), queries(k, j)), bias_of(usable))
                    both = jnp.maximum(top, jnp.max(s, axis=0, keepdims=True))
                    e = jnp.exp(s - both).astype(bf16)
                    out = out * jnp.exp(top - both)
                    out = out + jnp.dot(values_of(parts), e, preferred_element_type=f32)
                o = out[:HEAD_DIM] / out[HEAD_DIM : HEAD_DIM + 1]
                o = [o[:, n * Q_BLOCK : (n + 1) * Q_BLOCK] * gate_row(1, 2 * k + n, at) for n in range(2)]
                turned = oc[k, :, at] + jnp.concatenate(o, axis=0)
                mix[at, k * LANES : (k + 1) * LANES] = turned.T.astype(bf16)
            return carry

        lax.fori_loop(0, group // unroll, block, 0)
        return carry

    lax.fori_loop(0, ranks, choose, 0)


    previous = (rank + 1) % ranks
    if ranks > 1:
        mix_copy(ranks - 2).wait_recv()

    def weight_of(r):
        return wo[pl.ds(pl.multiple_of(r * kv_local * LANES, LANES), kv_local * LANES), :]

    def finish(i, carry):
        at = pl.ds(pl.multiple_of(i * Q_BLOCK, Q_BLOCK), Q_BLOCK)
        from_mix = pl.ds(pl.multiple_of(rank * rank_rows + i * Q_BLOCK, Q_BLOCK), Q_BLOCK)
        more = jnp.dot(mix[from_mix, :], weight_of(rank), preferred_element_type=f32)
        if ranks > 1:
            more += jnp.dot(got[previous, at, :], weight_of(previous), preferred_element_type=f32)
        out_ref[at, :] = (acc[at, :] + more).astype(bf16)
        return carry

    lax.fori_loop(0, group, finish, 0)


    for k in range(kv_local):
        if planes > 1:
            pl.when(z < last)(lambda k=k: own_copy(k, everything).wait_send())
        for dx in range(1, across):
            pl.when(x + dx < across)(lambda dx=dx, k=k: side_copy(0, dx, k).wait_send())
    for dz, k in relays:
        whole = (z >= dz) & ((z < last) | (dz == 1))
        if dz + 1 < last:
            pl.when(whole & (z + 1 < last))(lambda dz=dz, k=k: up_copy(dz, k).wait_send())
        if dz + 1 <= last:

            def sent_top(dz=dz, k=k):
                for s in range(ranks):
                    for dx in range(across):
                        top_copy(dz, dx, k, s).wait_send()

            pl.when(whole & (z + 1 == last))(sent_top)

        def sent_side(dz=dz, k=k):
            for dx in range(1, across):
                side_copy(dz, dx, k).wait_send()

        pl.when(whole)(sent_side)
    for dz in range(1, planes):
        pl.when(z + dz <= last)(lambda dz=dz: sum_up(dz, me).wait_send())
    for dx in range(1, across):
        pl.when(x + dx < across)(lambda dx=dx: sum_side(0, dx, me).wait_send())
        for dz in range(1, planes):
            pl.when(z >= dz)(lambda dz=dz, dx=dx: sum_side(dz, dx, me - dz * across).wait_send())
    for step in range(ranks - 1):
        mix_copy(step).wait_send()


def position_tables(rows, owners):
    half = HEAD_DIM // 2
    lane = np.arange(LANES)
    inverse = ROPE_BASE ** (-(lane % half).astype(np.float64) / half)
    sign = np.where(lane % HEAD_DIM < half, -1.0, 1.0)

    def both(positions):
        phase = positions[:, None].astype(np.float64) * inverse[None, :]
        return np.stack([np.cos(phase), np.sin(phase) * sign]).astype(np.float32)

    return both(np.arange(TILE)), both(np.arange(0, owners * rows, TILE))


def per_device(
    tokens,
    norm_gain,
    query_weight,
    cmp_key_weight,
    cmp_value_weight,
    sel_key_weight,
    sel_value_weight,
    branch_weight,
    key_embed,
    key_inner,
    key_outer,
    value_embed,
    value_inner,
    value_outer,
    out_weight,
    chosen,
):
    rows, width = tokens.shape
    kv_local = key_embed.shape[0]
    owners, ranks = lax.axis_size("kv"), lax.axis_size("tp")
    planes = PLANES if owners % PLANES == 0 else 1
    across = owners // planes
    span = rows // SEL_BLOCK
    q_blocks = rows // Q_BLOCK
    blocks = rows // CMP_BLOCK
    rank_rows = rows // ranks
    kv_width = kv_local * HEAD_DIM

    weights = [sel_key_weight, sel_value_weight, cmp_key_weight, cmp_value_weight]
    if kv_width % LANES:
        weights = [jnp.concatenate(weights, axis=1)]
    fine, coarse = position_tables(rows, owners)
    operands = (
        chosen.transpose(0, 2, 1),
        norm_gain.reshape(width // LANES, LANES),
        key_embed,
        key_outer,
        value_embed,
        value_outer,
        tokens,
        query_weight,
        branch_weight.transpose(0, 2, 1),
        key_inner.transpose(0, 2, 1),
        value_inner.transpose(0, 2, 1),
        out_weight,
        jnp.asarray(fine),
        jnp.asarray(coarse),
        *weights,
    )
    vmem = pl.BlockSpec(memory_space=pltpu.VMEM)
    hbm = pl.BlockSpec(memory_space=pl.ANY)
    dma = pltpu.SemaphoreType.DMA
    picked = (q_blocks, SEL_BLOCK, LANES)
    whole = (span, SEL_BLOCK, LANES)
    n_local = 3 + len(weights) + 8 + 2 + 2
    picks = (owners * kv_local, chosen.shape[1])
    down = max(planes - 2, 1)
    return pl.pallas_call(
        functools.partial(layer_kernel, planes, len(weights)),
        in_specs=[hbm] * len(operands),
        out_specs=vmem,
        out_shape=jax.ShapeDtypeStruct((rank_rows, out_weight.shape[1]), bf16),
        scratch_shapes=[
            pltpu.SMEM(picks, jnp.int32),
            pltpu.VMEM(picks, jnp.int32),
            pltpu.VMEM((kv_local, chosen.shape[2], chosen.shape[1]), jnp.int32),
            pltpu.VMEM((width // LANES, LANES), bf16),
            pltpu.VMEM((1, width), f32),
            pltpu.VMEM(key_embed.shape, bf16),
            pltpu.VMEM(key_outer.shape, bf16),
            pltpu.VMEM(value_embed.shape, bf16),
            pltpu.VMEM(value_outer.shape, bf16),
            pltpu.VMEM((kv_local, *whole), bf16),
            pltpu.VMEM((max(owners - 1, 1), kv_local, *picked), bf16),
            pltpu.VMEM((kv_local, q_blocks, HEAD_DIM + ONES, 2 * Q_BLOCK), f32),
            pltpu.VMEM((kv_local, q_blocks, 1, 2 * Q_BLOCK), f32),
            pltpu.VMEM((max(planes - 1, 1), max(across - 1, 1), kv_local, *picked), bf16),
            pltpu.VMEM((down, across, kv_local, *picked), bf16),
            pltpu.VMEM((min(3, rows // TILE), TILE, width), bf16),
            pltpu.VMEM(tokens.shape, bf16),
            pltpu.VMEM((width, 4 * kv_width), bf16),
            pltpu.VMEM(query_weight.shape, bf16),
            pltpu.VMEM((2 * branch_weight.shape[2], width), bf16),
            pltpu.VMEM((16, width), bf16),
            pltpu.VMEM(out_weight.shape, bf16),
            pltpu.VMEM(fine.shape, f32),
            pltpu.VMEM(coarse.shape, f32),
            pltpu.VMEM((kv_local, HEAD_DIM, key_inner.shape[1]), bf16),
            pltpu.VMEM((kv_local, HEAD_DIM, key_inner.shape[1]), bf16),
            pltpu.VMEM((kv_local, 2, rows, LANES), bf16),
            pltpu.VMEM((kv_local, 2, rows, LANES), bf16),
            pltpu.VMEM((kv_local, HEAD_DIM + ONES, owners * blocks), bf16),
            pltpu.VMEM((rows, kv_width), f32),
            pltpu.VMEM((rows, kv_width), f32),
            pltpu.VMEM((16, rows), f32),
            pltpu.VMEM((owners, kv_local, blocks, LANES), bf16),
            pltpu.VMEM((kv_local, LANES, rows), f32),
            pltpu.VMEM((rows, kv_local * LANES), bf16),
            pltpu.VMEM((ranks, rank_rows, kv_local * LANES), bf16),
            pltpu.VMEM((rank_rows, out_weight.shape[1]), f32),
            dma((rows // TILE,)),
            dma((n_local,)),
            dma((kv_local,)),
            dma((kv_local, planes)),
            dma((kv_local, planes)),
            dma((max(planes - 1, 1), max(across - 1, 1), kv_local)),
            dma((down, across, kv_local, ranks)),
            dma((max(owners - 1, 1), kv_local, ranks)),
            dma((across, planes)),
            dma((across, planes)),
            dma((ranks,)),
            dma((ranks,)),
        ]
        + [pltpu.VMEM(whole, bf16)] * (kv_local * max(planes - 1, 1)),
        compiler_params=pltpu.CompilerParams(
            collective_id=0, has_side_effects=True, vmem_limit_bytes=60 * 1024 * 1024
        ),
        cost_estimate=pl.CostEstimate(flops=int(3e10), bytes_accessed=int(2e7), transcendentals=0),
        name="layer",
    )(*operands)


def solution(mesh):
    placed = (
        P("kv", None),
        P(),
        P(None, "tp"),
        P(None, "tp"),
        P(None, "tp"),
        P(None, "tp"),
        P(None, "tp"),
        P(),
        P("tp", None, None),
        P("tp", None, None),
        P("tp", None, None),
        P("tp", None, None),
        P("tp", None, None),
        P("tp", None, None),
        P(),
        P("tp", None, None),
    )
    return jax.shard_map(
        per_device, mesh=mesh, in_specs=placed, out_specs=P(("kv", "tp"), None), check_vma=False
    )
```

```python
import functools

import numpy as np

import jax
import jax.numpy as jnp
from jax import lax
from jax.experimental import pallas as pl
from jax.experimental.pallas import tpu as pltpu
from jax.sharding import PartitionSpec as P

HEAD_DIM = 64
CMP_BLOCK = 32
SEL_BLOCK = 64
Q_BLOCK = 128
LANES = 2 * HEAD_DIM
PLANES = 4
TILE = 256
ONES = 16
MESH = pl.DeviceIdType.MESH

ROPE_BASE = 10000.0
norm_eps = 1e-06
MASKED = -1e30

f32 = jnp.float32
bf16 = jnp.bfloat16


def low_lanes(shape):
    return lax.broadcasted_iota(jnp.int32, shape, len(shape) - 1) < HEAD_DIM


def nt_dot(a, b):
    return lax.dot_general(a, b, (((1,), (1,)), ((), ())), preferred_element_type=f32)


def swap(x):
    return pltpu.roll(x, HEAD_DIM, 1)


def turn(x, cosine, sine):
    half = HEAD_DIM // 2
    lane = lax.broadcasted_iota(jnp.int32, x.shape, 1)
    first = lax.rem(lane, HEAD_DIM) < half
    partner = jnp.where(first, pltpu.roll(x, LANES - half, 1), pltpu.roll(x, half, 1))
    return x * cosine + partner * sine


def pack_pair(keys, turned):
    rows = turned.shape[0]
    low = low_lanes((rows, LANES))
    return (
        jnp.where(low, keys[:rows], swap(turned)).astype(bf16),
        jnp.where(low, keys[rows:], turned).astype(bf16),
    )


def values_of(parts):
    low = low_lanes(parts[0].shape)
    pairs = [jnp.where(low, swap(parts[n]), parts[n + 1]) for n in range(0, len(parts), 2)]
    values = jnp.concatenate(pairs, axis=1)
    return jnp.concatenate([values, jnp.ones((ONES, values.shape[1]), values.dtype)], axis=0)


def layer_kernel(planes, pieces, *refs):
    (
        chosen_hbm,
        gain_hbm,
        ke_hbm,
        ko_hbm,
        ve_hbm,
        vo_hbm,
        tok_hbm,
        query_hbm,
        branch_hbm,
        ki_hbm,
        vi_hbm,
        wo_hbm,
        fine_hbm,
        coarse_hbm,
    ) = refs[:14]
    piece_hbm, refs = refs[14 : 14 + pieces], refs[14 + pieces :]
    out_ref, refs = refs[0], refs[1:]
    (
        pick,
        found,
        chosen_ref,
        gain_ref,
        gain_row,
        ke_ref,
        ko_ref,
        ve_ref,
        vo_ref,
        own,
        sel,
        part_out,
        part_top,
        stage_x,
        stage_t,
        tok,
        normed,
        w_kv,
        w_q,
        w_gate,
        w_own,
        wo,
        fine,
        coarse,
        ki,
        vi,
        qp,
        qt,
        vsum,
        ck,
        cv,
        gate,
        sums,
        oc,
        mix,
        got,
        acc,
        tok_sem,
        local_sem,
        own_send,
        col_send,
        col_recv,
        x_send,
        t_send,
        near_recv,
        far_recv,
        sum_send,
        sum_recv,
        mix_send,
        mix_recv,
    ) = refs[:50]
    col = refs[50:]

    kv_local = own.shape[0]
    span = own.shape[1]
    owners, ranks = sums.shape[0], got.shape[0]
    rows, width = normed.shape
    across = owners // planes
    last = planes - 1
    q_blocks = rows // Q_BLOCK
    all_blocks = owners * q_blocks
    blocks = rows // CMP_BLOCK
    tiles = rows // TILE
    ring = tok.shape[0]
    rank_rows = rows // ranks
    group = rank_rows // Q_BLOCK
    heads = branch_hbm.shape[1]
    heads_local = 2 * kv_local
    kv_width = kv_local * HEAD_DIM
    scale = HEAD_DIM ** (-0.5)
    me, rank = lax.axis_index("kv"), lax.axis_index("tp")
    z, x = me // across, me % across

    barrier = pltpu.get_barrier_semaphore()
    for d in range(1, owners):
        pl.semaphore_signal(barrier, inc=1, device_id={"kv": (me + d) % owners}, device_id_type=MESH)
    for d in range(1, ranks):
        pl.semaphore_signal(barrier, inc=1, device_id={"tp": (rank + d) % ranks}, device_id_type=MESH)

    def rows_at(i):
        return pl.ds(pl.multiple_of(i * TILE, TILE), TILE)

    def tok_copy(i):
        return pltpu.make_async_copy(tok_hbm.at[rows_at(i)], tok.at[lax.rem(i, ring)], tok_sem.at[lax.rem(i, ring)])

    early = [(gain_hbm, gain_ref), (fine_hbm, fine), (coarse_hbm, coarse)]
    first = 0
    for ref in piece_hbm:
        early.append((ref, w_kv.at[:, pl.ds(first, ref.shape[1])]))
        first += ref.shape[1]
    late = [(chosen_hbm, chosen_ref), (ki_hbm, ki), (vi_hbm, vi), (query_hbm, w_q)]
    late += [(ke_hbm, ke_ref), (ko_hbm, ko_ref), (ve_hbm, ve_ref), (vo_hbm, vo_ref)]
    late += [(branch_hbm.at[b], w_gate.at[pl.ds(b * heads, heads)]) for b in range(2)]
    final = [(wo_hbm, wo), (found, pick)]
    copies = [
        pltpu.make_async_copy(a, b, local_sem.at[n]) for n, (a, b) in enumerate(early + late + final)
    ]
    to_smem = copies.pop()
    tok_copy(0).start()
    for copy in copies[: len(early)]:
        copy.start()
    for i in range(1, min(ring, tiles)):
        tok_copy(i).start()
    for copy in copies[len(early) :]:
        copy.start()

    for ref in (qp, qt):
        ref[:, :, HEAD_DIM:, :] = jnp.zeros((kv_local, 2, HEAD_DIM, rows), bf16)
    moves = [(dz, dx) for dz in range(planes) for dx in range(across) if (dz, dx) != (0, 0)]

    def slot(dz, dx):
        return dz * across + dx - 1

    def present(dz, dx):
        return (x >= dx) if dz == 0 else (z >= dz)

    for dz, dx in moves:

        def clear(dz=dz, dx=dx):
            for k in range(kv_local):
                sel[slot(dz, dx), k] = jnp.zeros(sel.shape[2:], bf16)

        pl.when(jnp.logical_not(present(dz, dx)))(clear)
    for d in range(1, owners):

        def clear_sums(d=d):
            for k in range(kv_local):
                sums[me + d, k] = jnp.zeros(sums.shape[2:], bf16)

        pl.when(me + d < owners)(clear_sums)


    def remote(src, dst, send, recv, target):
        return pltpu.make_async_remote_copy(
            src_ref=src,
            dst_ref=dst,
            send_sem=send,
            recv_sem=recv,
            device_id={"kv": target},
            device_id_type=MESH,
        )

    above = lax.rem(me + across, owners)

    def own_copy(k, at):
        return remote(own.at[k, at], col[k].at[at], own_send.at[k], col_recv.at[k, 0], above)

    def col_of(dz, k):
        return col[(dz - 1) * kv_local + k]

    def up_copy(dz, k):
        return remote(
            col_of(dz, k), col_of(dz + 1, k), col_send.at[k, dz - 1], col_recv.at[k, dz], above
        )

    def side_copy(dz, dx, k):
        return remote(
            stage_x.at[dz, dx - 1, k],
            sel.at[slot(dz, dx), k],
            x_send.at[dz if dz else planes + dx - 1],
            near_recv.at[slot(dz, dx), k],
            z * across + (x + dx) % across,
        )

    def rank_at(step):
        if ranks % 2:
            return (rank + 1 + step) % ranks
        chip = (rank // 2 + 1 + step // 2) % (ranks // 2)
        return chip * 2 + (rank + step + 1) % 2

    def rank_from(step):
        if ranks % 2:
            return (rank + 2 * ranks - 1 - step) % ranks
        chip = (rank // 2 + ranks - 1 - step // 2) % (ranks // 2)
        return chip * 2 + (rank + step + 1) % 2

    parts_last = [1] * (kv_local - 1) + [2 if group % 2 == 0 else 1]

    def pieces_of(k):
        return range(ranks - 1 + parts_last[k])

    def piece_at(piece, k):
        if isinstance(piece, int) and piece >= ranks - 1:
            size = group // parts_last[k]
            return pl.ds(rank * group + (piece - (ranks - 1)) * size, size)
        return pl.ds(rank_at(piece) * group, group)

    def far_side_copy(dz, dx, k, piece):
        at = piece_at(piece, k)
        return remote(
            stage_x.at[dz, dx - 1, k, at],
            sel.at[slot(dz, dx), k, at],
            x_send.at[dz],
            far_recv.at[k, piece],
            z * across + (x + dx) % across,
        )

    def top_copy(dz, dx, k, piece):
        at = piece_at(piece, k)
        return remote(
            stage_t.at[dz - 1, dx, k, at],
            sel.at[slot(dz + 1, dx), k, at],
            t_send.at[dz - 1],
            far_recv.at[k, piece],
            lax.rem((z + 1) * across + (x + dx) % across, owners),
        )

    def gather(src, dst, source, k, device):
        row, base = source * kv_local + k, device * q_blocks

        def one(j, carry):
            dst[j] = src[jnp.maximum(pick[row, base + j], 0)]
            return carry

        lax.fori_loop(0, q_blocks, one, 0, unroll=4)

    def relay(dz, k):
        whole = (z >= dz) & ((z < last) | (dz == 1))

        def go():
            remote(col_of(dz, k), col_of(dz, k), own_send.at[k], col_recv.at[k, dz - 1], above).wait_recv()
            source = me - dz * across
            if dz + 1 < last:
                pl.when(z + 1 < last)(lambda: up_copy(dz, k).start())
            if dz + 1 <= last:

                def to_top():
                    for dx in range(across):
                        gather(
                            col_of(dz, k),
                            stage_t.at[dz - 1, dx, k],
                            source,
                            k,
                            (z + 1) * across + (x + dx) % across,
                        )
                    sends = [(s, k) for s in pieces_of(k)]
                    for s, n in sends:
                        for dx in range(across):
                            top_copy(dz, dx, n, s).start()

                pl.when(z + 1 == last)(to_top)
            for dx in range(1, across):
                there = z * across + (x + dx) % across
                gather(col_of(dz, k), stage_x.at[dz, dx - 1, k], source, k, there)
                if dz < 2:
                    side_copy(dz, dx, k).start()
                else:
                    for piece in pieces_of(k):
                        far_side_copy(dz, dx, k, piece).start()
            gather(col_of(dz, k), sel.at[slot(dz, 0), k], source, k, me)

        pl.when(whole)(go)


    def norm_tile(i):
        t = tok[lax.rem(i, ring)].astype(f32)
        inv = lax.rsqrt(jnp.mean(t * t, axis=-1, keepdims=True) + norm_eps)
        normed[rows_at(i), :] = (t * inv * gain_row[...]).astype(bf16)
        pl.when(i + ring < tiles)(lambda: tok_copy(i + ring).start())

    def tables(i):
        row = pl.ds(me * tiles + i, 1)
        cos_c, sin_c = coarse[0, row, :], coarse[1, row, :]
        return fine[0] * cos_c - fine[1] * sin_c, fine[1] * cos_c + fine[0] * sin_c

    def project_kv(i):
        at = rows_at(i)
        y = jnp.dot(normed[at, :], w_kv[...], preferred_element_type=f32)
        cosine, sine = tables(i)
        for k in range(kv_local):
            if kv_local == 1:
                value = y[:, :LANES]
                key = turn(value, cosine, sine)
                keys, first = key, HEAD_DIM
            elif k % 2 == 0:
                key = turn(y[:, k * HEAD_DIM : k * HEAD_DIM + LANES], cosine, sine)
                value = y[:, kv_width + k * HEAD_DIM : kv_width + k * HEAD_DIM + LANES]
                keys, first = key, 0
            else:
                keys, first = swap(key), HEAD_DIM
            for t in range(TILE // (2 * SEL_BLOCK)):
                two = slice(t * 2 * SEL_BLOCK, (t + 1) * 2 * SEL_BLOCK)
                turned = value[two].T[first : first + HEAD_DIM]
                a, b = pack_pair(keys[two], turned)
                own[k, i * (TILE // SEL_BLOCK) + 2 * t] = a
                own[k, i * (TILE // SEL_BLOCK) + 2 * t + 1] = b
        ck[at, :] = y[:, 2 * kv_width : 3 * kv_width].astype(bf16).astype(f32)
        cv[at, :] = y[:, 3 * kv_width : 4 * kv_width].astype(bf16).astype(f32)

    def send_tile(i):
        here = pl.ds(i * (TILE // SEL_BLOCK), TILE // SEL_BLOCK)
        if planes > 1:
            pl.when(z < last)(lambda: own_copy(0, here).start())

    copies[0].wait()
    for c in range(gain_ref.shape[0]):
        gain_row[:, c * LANES : (c + 1) * LANES] = gain_ref[c : c + 1, :].astype(f32)
    tok_copy(0).wait()
    norm_tile(0)
    for copy in copies[1 : len(early)]:
        copy.wait()
    pl.semaphore_wait(barrier, owners + ranks - 2)

    def first_pass(i, carry):
        pl.when(i > 0)(lambda: send_tile(i - 1))
        tok_copy(i + 1).wait()
        norm_tile(i + 1)
        project_kv(i)
        return carry

    lax.fori_loop(0, tiles - 1, first_pass, 0)
    if tiles > 1:
        send_tile(tiles - 2)
    project_kv(tiles - 1)

    for copy in copies[len(early) : len(early) + len(late)]:
        copy.wait()
    send_tile(tiles - 1)


    for s in range(owners):
        for k in range(kv_local):
            place = chosen_ref[k] - s * span
            place = jnp.where((place >= 0) & (place < span), place, -1)
            found[s * kv_local + k : s * kv_local + k + 1, :] = jnp.max(place, axis=0, keepdims=True)
    to_smem.start()

    quarter = span // 4
    for k in range(1, kv_local):
        if planes > 1:
            pl.when(z < last)(lambda k=k: own_copy(k, pl.ds(0, quarter)).start())


    def summarize(x_ref, e_ref, i_ref, o_ref):
        embed = jnp.concatenate([e_ref[k].astype(f32) for k in range(kv_local)], axis=1)
        parts = [
            x_ref[pl.ds(c, blocks, stride=CMP_BLOCK), :] + embed[c : c + 1] for c in range(CMP_BLOCK)
        ]
        result = []
        for k in range(kv_local):
            if kv_local == 1:
                flat = jnp.concatenate([p.astype(bf16) for p in parts], axis=1)
            else:
                g, odd = k // 2 * LANES, k % 2
                low = low_lanes((blocks, LANES))
                cut = []
                for c in range(0, CMP_BLOCK, 2):
                    a, b = parts[c][:, g : g + LANES], parts[c + 1][:, g : g + LANES]
                    both = jnp.where(low, swap(a), b) if odd else jnp.where(low, a, swap(b))
                    cut.append(both.astype(bf16))
                flat = jnp.concatenate(cut, axis=1)
            hidden = jax.nn.gelu(nt_dot(flat, i_ref[k])).astype(bf16)
            result.append(jnp.dot(hidden, o_ref[k], preferred_element_type=f32))
        return result

    sk = summarize(ck, ke_ref, ki, ko_ref)
    sv = summarize(cv, ve_ref, vi, vo_ref)
    for k in range(kv_local):
        sums[me, k] = jnp.concatenate([sk[k], sv[k].T], axis=1).astype(bf16)

    def sum_up(dz, source):
        there = lax.rem(me + dz * across, owners)
        return remote(sums.at[source], sums.at[source], sum_send.at[0, dz], sum_recv.at[0, dz], there)

    def sum_side(dz, dx, source):
        there = z * across + (x + dx) % across
        return remote(sums.at[source], sums.at[source], sum_send.at[dx, dz], sum_recv.at[dx, dz], there)

    for dz in range(1, planes):
        pl.when(z + dz <= last)(lambda dz=dz: sum_up(dz, me).start())
    for dx in range(1, across):
        pl.when(x + dx < across)(lambda dx=dx: sum_side(0, dx, me).start())
    to_smem.wait()
    for dx in range(1, across):
        for k in range(kv_local):
            gather(own.at[k], stage_x.at[0, dx - 1, k], me, k, z * across + (x + dx) % across)
    everything = pl.ds(0, span)
    for k in range(1, kv_local):
        if planes > 1:
            pl.when(z < last)(lambda k=k: own_copy(k, pl.ds(quarter, span - quarter)).start())
    for dx in range(1, across):
        pl.when(x + dx < across)(lambda dx=dx: side_copy(0, dx, 0).start())


    mine = lax.broadcasted_iota(jnp.int32, (w_own.shape[0], w_gate.shape[0]), 0)
    branch = jnp.where(mine >= heads_local, 1, 0)
    wanted = branch * heads + rank * heads_local + mine - branch * heads_local
    wanted = jnp.where(mine < 2 * heads_local, wanted, -1)
    source = lax.broadcasted_iota(jnp.int32, mine.shape, 1)
    chooser = jnp.where(source == wanted, 1.0, 0.0).astype(bf16)
    w_own[...] = jnp.dot(chooser, w_gate[...], preferred_element_type=f32).astype(bf16)

    def second_pass(i, carry):
        at = rows_at(i)
        n = normed[at, :]
        y = jnp.dot(n, w_q[...], preferred_element_type=f32)
        cosine, sine = tables(i)
        for k in range(kv_local):
            v = y[:, k * LANES : (k + 1) * LANES] * scale
            for ref, q in ((qp, v), (qt, turn(v, cosine, sine))):
                turned = q.T.astype(bf16)
                for u in range(2):
                    ref[k, u, :HEAD_DIM, at] = turned[u * HEAD_DIM : (u + 1) * HEAD_DIM]
        gate[:, at] = jax.nn.sigmoid(nt_dot(w_own[...], n))
        return carry

    lax.fori_loop(0, tiles // 2, second_pass, 0)
    for dz in range(1, planes):

        def pass_on(dz=dz):
            below = me - dz * across
            sum_up(dz, below).wait_recv()
            for dx in range(1, across):
                sum_side(dz, dx, below).start()

        pl.when(z >= dz)(pass_on)
    lax.fori_loop(tiles // 2, tiles, second_pass, 0)
    relays = [(dz, k) for dz in range(1, max(2, last)) for k in range(kv_local)] if planes > 1 else []


    if relays:
        relay(*relays[0])
    for dx in range(1, across):
        for k in range(1, kv_local):
            pl.when(x + dx < across)(lambda dx=dx, k=k: side_copy(0, dx, k).start())
    for dz in range(planes):
        for dx in range(1, across):
            there = lax.rem((z - dz + planes) * across + (x + across - dx) % across, owners)
            pl.when(present(dz, dx))(
                lambda dz=dz, dx=dx, there=there: sum_side(dz, dx, there).wait_recv()
            )

    def gate_row(branch, head, at):
        return gate[branch * heads_local + head : branch * heads_local + head + 1, at]

    for k in range(kv_local):
        vsum[k] = values_of([sums[s, k] for s in range(owners)])

    def compress(i, carry):
        at = rows_at(i)
        lane = lax.broadcasted_iota(jnp.int32, (1, 2 * TILE), 1)
        pos = me * rows + i * TILE + jnp.where(lane >= TILE, lane - TILE, lane)
        block = lax.broadcasted_iota(jnp.int32, (owners * blocks, 1), 0)
        allowed = (block + 1) * CMP_BLOCK - 1 <= pos
        for k in range(kv_local):
            keys = jnp.concatenate([sums[s, k] for s in range(owners)], axis=0)
            q = jnp.concatenate([qp[k, 0, :, at], qp[k, 1, :, at]], axis=1)
            s = jnp.where(allowed, jnp.dot(keys, q, preferred_element_type=f32), MASKED)
            top = jnp.max(s, axis=0, keepdims=True)
            e = jnp.exp(s - top).astype(bf16)
            o = jnp.dot(vsum[k], e, preferred_element_type=f32)
            o = jnp.where(pos >= CMP_BLOCK - 1, o[:HEAD_DIM] / o[HEAD_DIM : HEAD_DIM + 1], 0.0)
            for u in range(2):
                part = o[:, u * TILE : (u + 1) * TILE] * gate_row(0, 2 * k + u, at)
                oc[k, u * HEAD_DIM : (u + 1) * HEAD_DIM, at] = part
        return carry

    bounds = [tiles * n // kv_local for n in range(kv_local + 1)]
    for k in range(kv_local):
        if k > 0 and planes > 1:
            relay(1, k)
        lax.fori_loop(bounds[k], bounds[k + 1], compress, 0)


    def is_top(dz):
        return (z == last) & (dz >= 2)

    def wait_side(dz, dx, k):
        pl.when(present(dz, dx))(lambda: side_copy(dz, dx, k).wait_recv())

    def bias_of(usable):
        return [jnp.where(u, 0.0, MASKED).astype(f32) for u in usable]

    def add_bias(s, bias):
        cut = [s[n * SEL_BLOCK : (n + 1) * SEL_BLOCK] + b for n, b in enumerate(bias)]
        return jnp.concatenate(cut, axis=0)

    def far_parts(some_moves, k, j):
        parts, usable = [], []
        for dz, dx in some_moves:
            parts.append(sel[slot(dz, dx), k, j])
            source = lax.rem(me - dz * across - x + (x + across - dx) % across + owners, owners)
            usable.append((pick[source * kv_local + k, me * q_blocks + j] >= 0) & present(dz, dx))
        return parts, usable

    near_moves = [m for m in moves if m[0] < 2]
    far_moves = [m for m in moves if m[0] >= 2]
    own_blocks = Q_BLOCK // SEL_BLOCK

    def queries(k, j):
        at = pl.ds(pl.multiple_of(j * Q_BLOCK, Q_BLOCK), Q_BLOCK)
        return jnp.concatenate([qt[k, 0, :, at], qt[k, 1, :, at]], axis=1)

    def scores(parts, k, j):
        keys = jnp.concatenate(parts, axis=0)
        return jnp.dot(keys, queries(k, j), preferred_element_type=f32)

    unroll = group if group < 4 else 4

    def near(k, some, carry):
        row = lax.broadcasted_iota(jnp.int32, (Q_BLOCK, 2 * Q_BLOCK), 0)
        lane = lax.broadcasted_iota(jnp.int32, row.shape, 1)
        lane = jnp.where(lane >= Q_BLOCK, lane - Q_BLOCK, lane)
        js = [some * unroll + u for u in range(unroll)]
        all_parts, ss = [], []
        for j in js:
            parts = [own[k, j * own_blocks + b] for b in range(own_blocks)]
            mine = pick[me * kv_local + k, me * q_blocks + j]
            parts.append(own[k, jnp.maximum(mine, 0)])
            more, usable = far_parts(near_moves, k, j)
            bias = bias_of([(mine >= 0) & (mine < j * own_blocks)] + usable)
            all_parts.append(parts + more)
            s = scores(all_parts[-1], k, j)
            close = jnp.where(row > lane, MASKED, s[:Q_BLOCK])
            ss.append(jnp.concatenate([close, add_bias(s[Q_BLOCK:], bias)], axis=0))
        tops = [jnp.max(s, axis=0, keepdims=True) for s in ss]
        es = [jnp.exp(s - top).astype(bf16) for s, top in zip(ss, tops)]
        for j, parts, e, top in zip(js, all_parts, es, tops):
            part_out[k, j] = jnp.dot(values_of(parts), e, preferred_element_type=f32)
            part_top[k, j] = top
        return carry

    for k in range(kv_local):
        for dz, dx in near_moves:
            if dx:
                wait_side(dz, dx, k)
        lax.fori_loop(0, q_blocks // unroll, functools.partial(near, k), 0)
        for dz in range(2, last):
            relay(dz, k)

    def wait_far(piece, k):
        if not far_moves:
            return
        at = piece_at(piece, k)

        def wait(first, count):
            region = sel.at[pl.ds(first, count), k, at]
            remote(region, region, x_send.at[0], far_recv.at[k, piece], above).wait_recv()

        pl.when(z == last)(lambda: wait(slot(2, 0), (planes - 2) * across))
        if across > 1:
            for dz in range(2, last):
                pl.when(z == dz)(lambda: wait(slot(2, 1), across - 1))

    def mix_copy(k, step):
        target = rank_at(step)
        at = pl.ds(pl.multiple_of(target * rank_rows, rank_rows), rank_rows)
        return pltpu.make_async_remote_copy(
            src_ref=mix.at[k, at],
            dst_ref=got.at[rank, k],
            send_sem=mix_send.at[k],
            recv_sem=mix_recv.at[k],
            device_id={"tp": target},
            device_id_type=MESH,
        )

    def outputs(k, u):
        at = pl.ds(pl.multiple_of(u * Q_BLOCK, Q_BLOCK), Q_BLOCK)
        from_mix = pl.ds(pl.multiple_of(rank * rank_rows + u * Q_BLOCK, Q_BLOCK), Q_BLOCK)
        shares, weights = [], []
        for step in range(ranks):
            source = rank_from(step) if step < ranks - 1 else rank
            shares.append(got[source, k, at, :] if step < ranks - 1 else mix[k, from_mix, :])
            weights.append(wo[pl.ds(pl.multiple_of((source * kv_local + k) * LANES, LANES), LANES), :])
        shares, weights = jnp.concatenate(shares, axis=1), jnp.concatenate(weights, axis=0)
        return at, jnp.dot(shares, weights, preferred_element_type=f32)

    def every_mix(k):
        return pltpu.make_async_remote_copy(
            src_ref=got.at[pl.ds(0, ranks - 1), k],
            dst_ref=got.at[pl.ds(0, ranks - 1), k],
            send_sem=mix_send.at[k],
            recv_sem=mix_recv.at[k],
            device_id={"tp": rank_at(0)},
            device_id_type=MESH,
        )

    def add_head(k):
        every_mix(k).wait_recv()

        def part(u, carry):
            at, more = outputs(k, u)
            acc[at, :] = more if k == 0 else acc[at, :] + more
            return carry

        lax.fori_loop(0, group, part, 0)

    copies[-1].wait()

    def late(k, blocks_of):
        ats = [pl.ds(pl.multiple_of(j * Q_BLOCK, Q_BLOCK), Q_BLOCK) for j in blocks_of]
        outs = [part_out[k, j] for j in blocks_of]
        if far_moves:
            fars = [far_parts(far_moves, k, j) for j in blocks_of]
            ss = [scores(parts, k, j) for (parts, _), j in zip(fars, blocks_of)]
            ss = [add_bias(s, bias_of(usable)) for s, (_, usable) in zip(ss, fars)]
            old = [part_top[k, j] for j in blocks_of]
            new = [jnp.maximum(t, jnp.max(s, axis=0, keepdims=True)) for t, s in zip(old, ss)]
            es = [jnp.exp(s - t).astype(bf16) for s, t in zip(ss, new)]
            more = [
                jnp.dot(values_of(parts), e, preferred_element_type=f32) for (parts, _), e in zip(fars, es)
            ]
            outs = [o * jnp.exp(a - b) + m for o, a, b, m in zip(outs, old, new, more)]
        for at, out in zip(ats, outs):
            o = out[:HEAD_DIM] / out[HEAD_DIM : HEAD_DIM + 1]
            o = [o[:, n * Q_BLOCK : (n + 1) * Q_BLOCK] * gate_row(1, 2 * k + n, at) for n in range(2)]
            turned = oc[k, :, at] + jnp.concatenate(o, axis=0)
            mix[k, at, :] = turned.T.astype(bf16)

    def choose(k, step, carry):
        pl.when((step > 0) & (step < ranks - 2))(lambda: mix_copy(k, step - 1).start())
        wait_far(step, k)
        late(k, [rank_at(step) * group + u for u in range(group)])
        return carry

    for k in range(kv_local):
        lax.fori_loop(0, ranks - 2, functools.partial(choose, k), 0)
        if ranks > 2:
            mix_copy(k, ranks - 3).start()
        if k > 0:
            add_head(k - 1)
        lax.fori_loop(ranks - 2, ranks - 1, functools.partial(choose, k), 0)
        mix_copy(k, ranks - 2).start()
        size = group // parts_last[k]
        for n in range(parts_last[k]):
            wait_far(ranks - 1 + n, k)
            mine = [n * size + u for u in range(size)]
            late(k, [rank * group + u for u in mine])
            if k == kv_local - 1:
                if n == 0:
                    every_mix(k).wait_recv()
                for u in mine:
                    at, more = outputs(k, u)
                    out_ref[at, :] = (more if k == 0 else acc[at, :] + more).astype(bf16)


    for k in range(kv_local):
        if planes > 1:
            pl.when(z < last)(lambda k=k: own_copy(k, everything).wait_send())

    def sent(region, send):
        return remote(region, region, send, sum_recv.at[0, 0], above)

    for dx in range(1, across):
        pl.when(x + dx < across)(
            lambda dx=dx: sent(stage_x.at[0, dx - 1], x_send.at[planes + dx - 1]).wait_send()
        )
    for dz, k in relays:
        whole = (z >= dz) & ((z < last) | (dz == 1))
        if dz + 1 < last:
            pl.when(whole & (z + 1 < last))(lambda dz=dz, k=k: up_copy(dz, k).wait_send())
        if k == 0 and dz + 1 <= last:
            pl.when(whole & (z + 1 == last))(
                lambda dz=dz: sent(stage_t.at[dz - 1], t_send.at[dz - 1]).wait_send()
            )
        if k == 0 and across > 1:
            pl.when(whole)(lambda dz=dz: sent(stage_x.at[dz], x_send.at[dz]).wait_send())
    for dz in range(1, planes):
        pl.when(z + dz <= last)(lambda dz=dz: sum_up(dz, me).wait_send())
    for dx in range(1, across):
        pl.when(x + dx < across)(lambda dx=dx: sum_side(0, dx, me).wait_send())
        for dz in range(1, planes):
            pl.when(z >= dz)(lambda dz=dz, dx=dx: sum_side(dz, dx, me - dz * across).wait_send())
    for k in range(kv_local):
        every_mix(k).wait_send()


def position_tables(rows, owners):
    half = HEAD_DIM // 2
    lane = np.arange(LANES)
    inverse = ROPE_BASE ** (-(lane % half).astype(np.float64) / half)
    sign = np.where(lane % HEAD_DIM < half, -1.0, 1.0)

    def both(positions):
        phase = positions[:, None].astype(np.float64) * inverse[None, :]
        return np.stack([np.cos(phase), np.sin(phase) * sign]).astype(np.float32)

    return both(np.arange(TILE)), both(np.arange(0, owners * rows, TILE))


def per_device(
    tokens,
    norm_gain,
    query_weight,
    cmp_key_weight,
    cmp_value_weight,
    sel_key_weight,
    sel_value_weight,
    branch_weight,
    key_embed,
    key_inner,
    key_outer,
    value_embed,
    value_inner,
    value_outer,
    out_weight,
    chosen,
):
    rows, width = tokens.shape
    kv_local = key_embed.shape[0]
    owners, ranks = lax.axis_size("kv"), lax.axis_size("tp")
    planes = PLANES if owners % PLANES == 0 else 1
    across = owners // planes
    span = rows // SEL_BLOCK
    q_blocks = rows // Q_BLOCK
    blocks = rows // CMP_BLOCK
    rank_rows = rows // ranks
    kv_width = kv_local * HEAD_DIM

    weights = [sel_key_weight, sel_value_weight, cmp_key_weight, cmp_value_weight]
    if kv_width % LANES:
        weights = [jnp.concatenate(weights, axis=1)]
    fine, coarse = position_tables(rows, owners)
    operands = (
        chosen.transpose(0, 2, 1),
        norm_gain.reshape(width // LANES, LANES),
        key_embed,
        key_outer,
        value_embed,
        value_outer,
        tokens,
        query_weight,
        branch_weight.transpose(0, 2, 1),
        key_inner.transpose(0, 2, 1),
        value_inner.transpose(0, 2, 1),
        out_weight,
        jnp.asarray(fine),
        jnp.asarray(coarse),
        *weights,
    )
    vmem = pl.BlockSpec(memory_space=pltpu.VMEM)
    hbm = pl.BlockSpec(memory_space=pl.ANY)
    dma = pltpu.SemaphoreType.DMA
    picked = (q_blocks, SEL_BLOCK, LANES)
    whole = (span, SEL_BLOCK, LANES)
    n_local = 3 + len(weights) + 8 + 2 + 2
    picks = (owners * kv_local, chosen.shape[1])
    down = max(planes - 2, 1)
    n_pieces = ranks + 1
    return pl.pallas_call(
        functools.partial(layer_kernel, planes, len(weights)),
        in_specs=[hbm] * len(operands),
        out_specs=vmem,
        out_shape=pltpu.VMEM((rank_rows, out_weight.shape[1]), bf16),
        scratch_shapes=[
            pltpu.SMEM(picks, jnp.int32),
            pltpu.VMEM(picks, jnp.int32),
            pltpu.VMEM((kv_local, chosen.shape[2], chosen.shape[1]), jnp.int32),
            pltpu.VMEM((width // LANES, LANES), bf16),
            pltpu.VMEM((1, width), f32),
            pltpu.VMEM(key_embed.shape, bf16),
            pltpu.VMEM(key_outer.shape, bf16),
            pltpu.VMEM(value_embed.shape, bf16),
            pltpu.VMEM(value_outer.shape, bf16),
            pltpu.VMEM((kv_local, *whole), bf16),
            pltpu.VMEM((max(owners - 1, 1), kv_local, *picked), bf16),
            pltpu.VMEM((kv_local, q_blocks, HEAD_DIM + ONES, 2 * Q_BLOCK), f32),
            pltpu.VMEM((kv_local, q_blocks, 1, 2 * Q_BLOCK), f32),
            pltpu.VMEM((max(planes - 1, 1), max(across - 1, 1), kv_local, *picked), bf16),
            pltpu.VMEM((down, across, kv_local, *picked), bf16),
            pltpu.VMEM((min(3, rows // TILE), TILE, width), bf16),
            pltpu.VMEM(tokens.shape, bf16),
            pltpu.VMEM((width, 4 * kv_width), bf16),
            pltpu.VMEM(query_weight.shape, bf16),
            pltpu.VMEM((2 * branch_weight.shape[2], width), bf16),
            pltpu.VMEM((16, width), bf16),
            pltpu.VMEM(out_weight.shape, bf16),
            pltpu.VMEM(fine.shape, f32),
            pltpu.VMEM(coarse.shape, f32),
            pltpu.VMEM((kv_local, HEAD_DIM, key_inner.shape[1]), bf16),
            pltpu.VMEM((kv_local, HEAD_DIM, key_inner.shape[1]), bf16),
            pltpu.VMEM((kv_local, 2, LANES, rows), bf16),
            pltpu.VMEM((kv_local, 2, LANES, rows), bf16),
            pltpu.VMEM((kv_local, HEAD_DIM + ONES, owners * blocks), bf16),
            pltpu.VMEM((rows, kv_width), f32),
            pltpu.VMEM((rows, kv_width), f32),
            pltpu.VMEM((16, rows), f32),
            pltpu.VMEM((owners, kv_local, blocks, LANES), bf16),
            pltpu.VMEM((kv_local, LANES, rows), f32),
            pltpu.VMEM((kv_local, rows, LANES), bf16),
            pltpu.VMEM((ranks, kv_local, rank_rows, LANES), bf16),
            pltpu.VMEM((rank_rows, out_weight.shape[1]), f32),
            dma((min(3, rows // TILE),)),
            dma((n_local,)),
            dma((kv_local,)),
            dma((kv_local, down)),
            dma((kv_local, max(planes - 1, 1))),
            dma((planes + across,)),
            dma((down,)),
            dma((max(2 * across - 1, 1), kv_local)),
            dma((kv_local, n_pieces)),
            dma((across, planes)),
            dma((across, planes)),
            dma((kv_local,)),
            dma((kv_local,)),
        ]
        + [pltpu.VMEM(whole, bf16)] * (kv_local * max(planes - 1, 1)),
        compiler_params=pltpu.CompilerParams(
            collective_id=0, has_side_effects=True, vmem_limit_bytes=56 * 1024 * 1024
        ),
        cost_estimate=pl.CostEstimate(flops=int(3e10), bytes_accessed=int(2e7), transcendentals=0),
        name="layer",
    )(*operands)


def solution(mesh):
    placed = (
        P("kv", None),
        P(),
        P(None, "tp"),
        P(None, "tp"),
        P(None, "tp"),
        P(None, "tp"),
        P(None, "tp"),
        P(),
        P("tp", None, None),
        P("tp", None, None),
        P("tp", None, None),
        P("tp", None, None),
        P("tp", None, None),
        P("tp", None, None),
        P(),
        P("tp", None, None),
    )
    return jax.shard_map(
        per_device, mesh=mesh, in_specs=placed, out_specs=P(("kv", "tp"), None), check_vma=False
    )
```

```python
import functools

import numpy as np

import jax
import jax.numpy as jnp
from jax import lax
from jax.experimental import pallas as pl
from jax.experimental.pallas import tpu as pltpu
from jax.sharding import PartitionSpec as P

HEAD_DIM = 64
CMP_BLOCK = 32
SEL_BLOCK = 64
Q_BLOCK = 128
LANES = 2 * HEAD_DIM
PLANES = 4
TILE = 256
ONES = 16
MESH = pl.DeviceIdType.MESH

ROPE_BASE = 10000.0
norm_eps = 1e-06
MASKED = -1e30

f32 = jnp.float32
bf16 = jnp.bfloat16


def low_lanes(shape):
    return lax.broadcasted_iota(jnp.int32, shape, len(shape) - 1) < HEAD_DIM


def nt_dot(a, b):
    return lax.dot_general(a, b, (((1,), (1,)), ((), ())), preferred_element_type=f32)


def swap(x):
    return pltpu.roll(x, HEAD_DIM, 1)


def turn(x, cosine, sine):
    half = HEAD_DIM // 2
    lane = lax.broadcasted_iota(jnp.int32, x.shape, 1)
    first = lax.rem(lane, HEAD_DIM) < half
    partner = jnp.where(first, pltpu.roll(x, LANES - half, 1), pltpu.roll(x, half, 1))
    return x * cosine + partner * sine


def pack_pair(keys, turned):
    rows = turned.shape[0]
    low = low_lanes((rows, LANES))
    return (
        jnp.where(low, keys[:rows], swap(turned)).astype(bf16),
        jnp.where(low, keys[rows:], turned).astype(bf16),
    )


def values_of(parts):
    low = low_lanes(parts[0].shape)
    pairs = [jnp.where(low, swap(parts[n]), parts[n + 1]) for n in range(0, len(parts), 2)]
    values = jnp.concatenate(pairs, axis=1)
    return jnp.concatenate([values, jnp.ones((ONES, values.shape[1]), values.dtype)], axis=0)


def layer_kernel(planes, pieces, *refs):
    (
        chosen_hbm,
        gain_hbm,
        ke_hbm,
        ko_hbm,
        ve_hbm,
        vo_hbm,
        tok_hbm,
        query_hbm,
        branch_hbm,
        ki_hbm,
        vi_hbm,
        wo_hbm,
        fine_hbm,
        coarse_hbm,
    ) = refs[:14]
    piece_hbm, refs = refs[14 : 14 + pieces], refs[14 + pieces :]
    out_ref, refs = refs[0], refs[1:]
    (
        pick,
        found,
        chosen_ref,
        gain_ref,
        gain_row,
        ke_ref,
        ko_ref,
        ve_ref,
        vo_ref,
        own,
        sel,
        part_out,
        part_top,
        stage_x,
        stage_t,
        tok,
        normed,
        w_kv,
        w_q,
        w_gate,
        w_own,
        wo,
        fine,
        coarse,
        ki,
        vi,
        qp,
        qt,
        vsum,
        ck,
        cv,
        gate,
        sums,
        oc,
        mix,
        got,
        acc,
        tok_sem,
        local_sem,
        own_send,
        col_send,
        col_recv,
        x_send,
        t_send,
        near_recv,
        far_recv,
        sum_send,
        sum_recv,
        mix_send,
        mix_recv,
    ) = refs[:50]
    col = refs[50:]

    kv_local = own.shape[0]
    span = own.shape[1]
    owners, ranks = sums.shape[0], got.shape[0]
    rows, width = normed.shape
    across = owners // planes
    last = planes - 1
    q_blocks = rows // Q_BLOCK
    all_blocks = owners * q_blocks
    blocks = rows // CMP_BLOCK
    tiles = rows // TILE
    ring = tok.shape[0]
    rank_rows = rows // ranks
    group = rank_rows // Q_BLOCK
    heads = branch_hbm.shape[1]
    heads_local = 2 * kv_local
    kv_width = kv_local * HEAD_DIM
    scale = HEAD_DIM ** (-0.5)
    me, rank = lax.axis_index("kv"), lax.axis_index("tp")
    z, x = me // across, me % across

    barrier = pltpu.get_barrier_semaphore()
    for d in range(1, owners):
        pl.semaphore_signal(barrier, inc=1, device_id={"kv": (me + d) % owners}, device_id_type=MESH)
    for d in range(1, ranks):
        pl.semaphore_signal(barrier, inc=1, device_id={"tp": (rank + d) % ranks}, device_id_type=MESH)

    def rows_at(i):
        return pl.ds(pl.multiple_of(i * TILE, TILE), TILE)

    def tok_copy(i):
        return pltpu.make_async_copy(tok_hbm.at[rows_at(i)], tok.at[lax.rem(i, ring)], tok_sem.at[lax.rem(i, ring)])

    early = [(gain_hbm, gain_ref), (fine_hbm, fine), (coarse_hbm, coarse)]
    first = 0
    for ref in piece_hbm:
        early.append((ref, w_kv.at[:, pl.ds(first, ref.shape[1])]))
        first += ref.shape[1]
    late = [(chosen_hbm, chosen_ref), (ki_hbm, ki), (vi_hbm, vi), (query_hbm, w_q)]
    late += [(ke_hbm, ke_ref), (ko_hbm, ko_ref), (ve_hbm, ve_ref), (vo_hbm, vo_ref)]
    late += [(branch_hbm.at[b], w_gate.at[pl.ds(b * heads, heads)]) for b in range(2)]
    final = [(wo_hbm, wo), (found, pick)]
    copies = [
        pltpu.make_async_copy(a, b, local_sem.at[n]) for n, (a, b) in enumerate(early + late + final)
    ]
    to_smem = copies.pop()
    tok_copy(0).start()
    for copy in copies[: len(early)]:
        copy.start()
    if tiles > 1:
        tok_copy(1).start()

    for ref in (qp, qt):
        ref[:, :, HEAD_DIM:, :] = jnp.zeros((kv_local, 2, HEAD_DIM, rows), bf16)
    moves = [(dz, dx) for dz in range(planes) for dx in range(across) if (dz, dx) != (0, 0)]

    def slot(dz, dx):
        return dz * across + dx - 1

    def present(dz, dx):
        return (x >= dx) if dz == 0 else (z >= dz)

    for dz, dx in moves:

        def clear(dz=dz, dx=dx):
            for k in range(kv_local):
                sel[slot(dz, dx), k] = jnp.zeros(sel.shape[2:], bf16)

        pl.when(jnp.logical_not(present(dz, dx)))(clear)
    for d in range(1, owners):

        def clear_sums(d=d):
            for k in range(kv_local):
                sums[me + d, k] = jnp.zeros(sums.shape[2:], bf16)

        pl.when(me + d < owners)(clear_sums)


    def remote(src, dst, send, recv, target):
        return pltpu.make_async_remote_copy(
            src_ref=src,
            dst_ref=dst,
            send_sem=send,
            recv_sem=recv,
            device_id={"kv": target},
            device_id_type=MESH,
        )

    above = lax.rem(me + across, owners)

    def own_copy(k, at):
        return remote(own.at[k, at], col[k].at[at], own_send.at[k], col_recv.at[k, 0], above)

    def col_of(dz, k):
        return col[(dz - 1) * kv_local + k]

    def up_copy(dz, k):
        return remote(
            col_of(dz, k), col_of(dz + 1, k), col_send.at[k, dz - 1], col_recv.at[k, dz], above
        )

    def side_copy(dz, dx, k):
        return remote(
            stage_x.at[dz, dx - 1, k],
            sel.at[slot(dz, dx), k],
            x_send.at[dz if dz else planes + dx - 1],
            near_recv.at[slot(dz, dx), k],
            z * across + (x + dx) % across,
        )

    def rank_at(step):
        if ranks % 2:
            return (rank + 1 + step) % ranks
        chip = (rank // 2 + 1 + step // 2) % (ranks // 2)
        return chip * 2 + (rank + step + 1) % 2

    def rank_from(step):
        if ranks % 2:
            return (rank + 2 * ranks - 1 - step) % ranks
        chip = (rank // 2 + ranks - 1 - step // 2) % (ranks // 2)
        return chip * 2 + (rank + step + 1) % 2

    parts_last = [1] * (kv_local - 1) + [2 if group % 2 == 0 else 1]

    def pieces_of(k):
        return range(ranks - 1 + parts_last[k])

    def piece_at(piece, k):
        if isinstance(piece, int) and piece >= ranks - 1:
            size = group // parts_last[k]
            return pl.ds(rank * group + (piece - (ranks - 1)) * size, size)
        return pl.ds(rank_at(piece) * group, group)

    def far_side_copy(dz, dx, k, piece):
        at = piece_at(piece, k)
        return remote(
            stage_x.at[dz, dx - 1, k, at],
            sel.at[slot(dz, dx), k, at],
            x_send.at[dz],
            far_recv.at[k, piece],
            z * across + (x + dx) % across,
        )

    def top_copy(dz, dx, k, piece):
        at = piece_at(piece, k)
        return remote(
            stage_t.at[dz - 1, dx, k, at],
            sel.at[slot(dz + 1, dx), k, at],
            t_send.at[dz - 1],
            far_recv.at[k, piece],
            lax.rem((z + 1) * across + (x + dx) % across, owners),
        )

    def gather(src, dst, source, k, device):
        row, base = source * kv_local + k, device * q_blocks

        def one(j, carry):
            dst[j] = src[jnp.maximum(pick[row, base + j], 0)]
            return carry

        lax.fori_loop(0, q_blocks, one, 0, unroll=4)

    def relay(dz, k):
        whole = (z >= dz) & ((z < last) | (dz == 1))

        def go():
            remote(col_of(dz, k), col_of(dz, k), own_send.at[k], col_recv.at[k, dz - 1], above).wait_recv()
            source = me - dz * across
            if dz + 1 < last:
                pl.when(z + 1 < last)(lambda: up_copy(dz, k).start())
            if dz + 1 <= last:

                def to_top():
                    for dx in range(across):
                        gather(
                            col_of(dz, k),
                            stage_t.at[dz - 1, dx, k],
                            source,
                            k,
                            (z + 1) * across + (x + dx) % across,
                        )
                    sends = [(s, k) for s in pieces_of(k)]
                    for s, n in sends:
                        for dx in range(across):
                            top_copy(dz, dx, n, s).start()

                pl.when(z + 1 == last)(to_top)
            for dx in range(1, across):
                there = z * across + (x + dx) % across
                gather(col_of(dz, k), stage_x.at[dz, dx - 1, k], source, k, there)
                if dz < 2:
                    side_copy(dz, dx, k).start()
                else:
                    for piece in pieces_of(k):
                        far_side_copy(dz, dx, k, piece).start()
            gather(col_of(dz, k), sel.at[slot(dz, 0), k], source, k, me)

        pl.when(whole)(go)


    def norm_tile(i):
        t = tok[lax.rem(i, ring)].astype(f32)
        inv = lax.rsqrt(jnp.mean(t * t, axis=-1, keepdims=True) + norm_eps)
        normed[rows_at(i), :] = (t * inv * gain_row[...]).astype(bf16)
        pl.when(i + ring < tiles)(lambda: tok_copy(i + ring).start())

    def tables(i):
        row = pl.ds(me * tiles + i, 1)
        cos_c, sin_c = coarse[0, row, :], coarse[1, row, :]
        return fine[0] * cos_c - fine[1] * sin_c, fine[1] * cos_c + fine[0] * sin_c

    def project_kv(i):
        at = rows_at(i)
        y = jnp.dot(normed[at, :], w_kv[...], preferred_element_type=f32)
        cosine, sine = tables(i)
        for k in range(kv_local):
            if kv_local == 1:
                value = y[:, :LANES]
                key = turn(value, cosine, sine)
                keys, first = key, HEAD_DIM
            elif k % 2 == 0:
                key = turn(y[:, k * HEAD_DIM : k * HEAD_DIM + LANES], cosine, sine)
                value = y[:, kv_width + k * HEAD_DIM : kv_width + k * HEAD_DIM + LANES]
                keys, first = key, 0
            else:
                keys, first = swap(key), HEAD_DIM
            for t in range(TILE // (2 * SEL_BLOCK)):
                two = slice(t * 2 * SEL_BLOCK, (t + 1) * 2 * SEL_BLOCK)
                turned = value[two].T[first : first + HEAD_DIM]
                a, b = pack_pair(keys[two], turned)
                own[k, i * (TILE // SEL_BLOCK) + 2 * t] = a
                own[k, i * (TILE // SEL_BLOCK) + 2 * t + 1] = b
        ck[at, :] = y[:, 2 * kv_width : 3 * kv_width].astype(bf16).astype(f32)
        cv[at, :] = y[:, 3 * kv_width : 4 * kv_width].astype(bf16).astype(f32)

    def send_tile(i):
        here = pl.ds(i * (TILE // SEL_BLOCK), TILE // SEL_BLOCK)
        if planes > 1:
            pl.when(z < last)(lambda: own_copy(0, here).start())

    copies[0].wait()
    for c in range(gain_ref.shape[0]):
        gain_row[:, c * LANES : (c + 1) * LANES] = gain_ref[c : c + 1, :].astype(f32)
    tok_copy(0).wait()
    norm_tile(0)
    for copy in copies[1 : len(early)]:
        copy.wait()
    for i in range(2, min(ring, tiles)):
        tok_copy(i).start()
    for copy in copies[len(early) :]:
        copy.start()
    pl.semaphore_wait(barrier, owners + ranks - 2)

    def first_pass(i, carry):
        pl.when(i > 0)(lambda: send_tile(i - 1))
        tok_copy(i + 1).wait()
        norm_tile(i + 1)
        project_kv(i)
        return carry

    lax.fori_loop(0, tiles - 1, first_pass, 0)
    if tiles > 1:
        send_tile(tiles - 2)
    project_kv(tiles - 1)

    for copy in copies[len(early) : len(early) + len(late)]:
        copy.wait()
    send_tile(tiles - 1)


    for s in range(owners):
        for k in range(kv_local):
            place = chosen_ref[k] - s * span
            place = jnp.where((place >= 0) & (place < span), place, -1)
            found[s * kv_local + k : s * kv_local + k + 1, :] = jnp.max(place, axis=0, keepdims=True)
    to_smem.start()

    quarter = span // 4
    for k in range(1, kv_local):
        if planes > 1:
            pl.when(z < last)(lambda k=k: own_copy(k, pl.ds(0, quarter)).start())


    def summarize(x_ref, e_ref, i_ref, o_ref):
        embed = jnp.concatenate([e_ref[k].astype(f32) for k in range(kv_local)], axis=1)
        parts = [
            x_ref[pl.ds(c, blocks, stride=CMP_BLOCK), :] + embed[c : c + 1] for c in range(CMP_BLOCK)
        ]
        result = []
        for k in range(kv_local):
            if kv_local == 1:
                flat = jnp.concatenate([p.astype(bf16) for p in parts], axis=1)
            else:
                g, odd = k // 2 * LANES, k % 2
                low = low_lanes((blocks, LANES))
                cut = []
                for c in range(0, CMP_BLOCK, 2):
                    a, b = parts[c][:, g : g + LANES], parts[c + 1][:, g : g + LANES]
                    both = jnp.where(low, swap(a), b) if odd else jnp.where(low, a, swap(b))
                    cut.append(both.astype(bf16))
                flat = jnp.concatenate(cut, axis=1)
            hidden = jax.nn.gelu(nt_dot(flat, i_ref[k])).astype(bf16)
            result.append(jnp.dot(hidden, o_ref[k], preferred_element_type=f32))
        return result

    sk = summarize(ck, ke_ref, ki, ko_ref)
    sv = summarize(cv, ve_ref, vi, vo_ref)
    for k in range(kv_local):
        sums[me, k] = jnp.concatenate([sk[k], sv[k].T], axis=1).astype(bf16)

    def sum_up(dz, source):
        there = lax.rem(me + dz * across, owners)
        return remote(sums.at[source], sums.at[source], sum_send.at[0, dz], sum_recv.at[0, dz], there)

    def sum_side(dz, dx, source):
        there = z * across + (x + dx) % across
        return remote(sums.at[source], sums.at[source], sum_send.at[dx, dz], sum_recv.at[dx, dz], there)

    for dz in range(1, planes):
        pl.when(z + dz <= last)(lambda dz=dz: sum_up(dz, me).start())
    for dx in range(1, across):
        pl.when(x + dx < across)(lambda dx=dx: sum_side(0, dx, me).start())
    to_smem.wait()
    for dx in range(1, across):
        for k in range(kv_local):
            gather(own.at[k], stage_x.at[0, dx - 1, k], me, k, z * across + (x + dx) % across)
    everything = pl.ds(0, span)
    for k in range(1, kv_local):
        if planes > 1:
            pl.when(z < last)(lambda k=k: own_copy(k, pl.ds(quarter, span - quarter)).start())
    for dx in range(1, across):
        pl.when(x + dx < across)(lambda dx=dx: side_copy(0, dx, 0).start())


    mine = lax.broadcasted_iota(jnp.int32, (w_own.shape[0], w_gate.shape[0]), 0)
    branch = jnp.where(mine >= heads_local, 1, 0)
    wanted = branch * heads + rank * heads_local + mine - branch * heads_local
    wanted = jnp.where(mine < 2 * heads_local, wanted, -1)
    source = lax.broadcasted_iota(jnp.int32, mine.shape, 1)
    chooser = jnp.where(source == wanted, 1.0, 0.0).astype(bf16)
    w_own[...] = jnp.dot(chooser, w_gate[...], preferred_element_type=f32).astype(bf16)

    def second_pass(i, carry):
        at = rows_at(i)
        n = normed[at, :]
        y = jnp.dot(n, w_q[...], preferred_element_type=f32)
        cosine, sine = tables(i)
        for k in range(kv_local):
            v = y[:, k * LANES : (k + 1) * LANES] * scale
            for ref, q in ((qp, v), (qt, turn(v, cosine, sine))):
                turned = q.T.astype(bf16)
                for u in range(2):
                    ref[k, u, :HEAD_DIM, at] = turned[u * HEAD_DIM : (u + 1) * HEAD_DIM]
        gate[:, at] = jax.nn.sigmoid(nt_dot(w_own[...], n))
        return carry

    lax.fori_loop(0, tiles // 2, second_pass, 0)
    for dz in range(1, planes):

        def pass_on(dz=dz):
            below = me - dz * across
            sum_up(dz, below).wait_recv()
            for dx in range(1, across):
                sum_side(dz, dx, below).start()

        pl.when(z >= dz)(pass_on)
    lax.fori_loop(tiles // 2, tiles, second_pass, 0)
    relays = [(dz, k) for dz in range(1, max(2, last)) for k in range(kv_local)] if planes > 1 else []


    if relays:
        relay(*relays[0])
    for dx in range(1, across):
        for k in range(1, kv_local):
            pl.when(x + dx < across)(lambda dx=dx, k=k: side_copy(0, dx, k).start())
    for dz in range(planes):
        for dx in range(1, across):
            there = lax.rem((z - dz + planes) * across + (x + across - dx) % across, owners)
            pl.when(present(dz, dx))(
                lambda dz=dz, dx=dx, there=there: sum_side(dz, dx, there).wait_recv()
            )

    def gate_row(branch, head, at):
        return gate[branch * heads_local + head : branch * heads_local + head + 1, at]

    for k in range(kv_local):
        vsum[k] = values_of([sums[s, k] for s in range(owners)])

    def compress(i, carry):
        at = rows_at(i)
        lane = lax.broadcasted_iota(jnp.int32, (1, 2 * TILE), 1)
        pos = me * rows + i * TILE + jnp.where(lane >= TILE, lane - TILE, lane)
        block = lax.broadcasted_iota(jnp.int32, (owners * blocks, 1), 0)
        allowed = (block + 1) * CMP_BLOCK - 1 <= pos
        for k in range(kv_local):
            keys = jnp.concatenate([sums[s, k] for s in range(owners)], axis=0)
            q = jnp.concatenate([qp[k, 0, :, at], qp[k, 1, :, at]], axis=1)
            s = jnp.where(allowed, jnp.dot(keys, q, preferred_element_type=f32), MASKED)
            top = jnp.max(s, axis=0, keepdims=True)
            e = jnp.exp(s - top).astype(bf16)
            o = jnp.dot(vsum[k], e, preferred_element_type=f32)
            o = jnp.where(pos >= CMP_BLOCK - 1, o[:HEAD_DIM] / o[HEAD_DIM : HEAD_DIM + 1], 0.0)
            for u in range(2):
                part = o[:, u * TILE : (u + 1) * TILE] * gate_row(0, 2 * k + u, at)
                oc[k, u * HEAD_DIM : (u + 1) * HEAD_DIM, at] = part
        return carry

    bounds = [tiles * n // kv_local for n in range(kv_local + 1)]
    for k in range(kv_local):
        if k > 0 and planes > 1:
            relay(1, k)
        lax.fori_loop(bounds[k], bounds[k + 1], compress, 0)


    def is_top(dz):
        return (z == last) & (dz >= 2)

    def wait_side(dz, dx, k):
        pl.when(present(dz, dx))(lambda: side_copy(dz, dx, k).wait_recv())

    def bias_of(usable):
        return [jnp.where(u, 0.0, MASKED).astype(f32) for u in usable]

    def add_bias(s, bias):
        cut = [s[n * SEL_BLOCK : (n + 1) * SEL_BLOCK] + b for n, b in enumerate(bias)]
        return jnp.concatenate(cut, axis=0)

    def far_parts(some_moves, k, j):
        parts, usable = [], []
        for dz, dx in some_moves:
            parts.append(sel[slot(dz, dx), k, j])
            source = lax.rem(me - dz * across - x + (x + across - dx) % across + owners, owners)
            usable.append((pick[source * kv_local + k, me * q_blocks + j] >= 0) & present(dz, dx))
        return parts, usable

    near_moves = [m for m in moves if m[0] < 2]
    far_moves = [m for m in moves if m[0] >= 2]
    own_blocks = Q_BLOCK // SEL_BLOCK

    def queries(k, j):
        at = pl.ds(pl.multiple_of(j * Q_BLOCK, Q_BLOCK), Q_BLOCK)
        return jnp.concatenate([qt[k, 0, :, at], qt[k, 1, :, at]], axis=1)

    def scores(parts, k, j):
        keys = jnp.concatenate(parts, axis=0)
        return jnp.dot(keys, queries(k, j), preferred_element_type=f32)

    unroll = group if group < 4 else 4

    def near(k, some, carry):
        row = lax.broadcasted_iota(jnp.int32, (Q_BLOCK, 2 * Q_BLOCK), 0)
        lane = lax.broadcasted_iota(jnp.int32, row.shape, 1)
        lane = jnp.where(lane >= Q_BLOCK, lane - Q_BLOCK, lane)
        js = [some * unroll + u for u in range(unroll)]
        all_parts, ss = [], []
        for j in js:
            parts = [own[k, j * own_blocks + b] for b in range(own_blocks)]
            mine = pick[me * kv_local + k, me * q_blocks + j]
            parts.append(own[k, jnp.maximum(mine, 0)])
            more, usable = far_parts(near_moves, k, j)
            bias = bias_of([(mine >= 0) & (mine < j * own_blocks)] + usable)
            all_parts.append(parts + more)
            s = scores(all_parts[-1], k, j)
            close = jnp.where(row > lane, MASKED, s[:Q_BLOCK])
            ss.append(jnp.concatenate([close, add_bias(s[Q_BLOCK:], bias)], axis=0))
        tops = [jnp.max(s, axis=0, keepdims=True) for s in ss]
        es = [jnp.exp(s - top).astype(bf16) for s, top in zip(ss, tops)]
        for j, parts, e, top in zip(js, all_parts, es, tops):
            part_out[k, j] = jnp.dot(values_of(parts), e, preferred_element_type=f32)
            part_top[k, j] = top
        return carry

    for k in range(kv_local):
        for dz, dx in near_moves:
            if dx:
                wait_side(dz, dx, k)
        lax.fori_loop(0, q_blocks // unroll, functools.partial(near, k), 0)
        for dz in range(2, last):
            relay(dz, k)

    def wait_far(piece, k):
        if not far_moves:
            return
        at = piece_at(piece, k)

        def wait(first, count):
            region = sel.at[pl.ds(first, count), k, at]
            remote(region, region, x_send.at[0], far_recv.at[k, piece], above).wait_recv()

        pl.when(z == last)(lambda: wait(slot(2, 0), (planes - 2) * across))
        if across > 1:
            for dz in range(2, last):
                pl.when(z == dz)(lambda: wait(slot(2, 1), across - 1))

    def mix_copy(k, step):
        target = rank_at(step)
        at = pl.ds(pl.multiple_of(target * rank_rows, rank_rows), rank_rows)
        return pltpu.make_async_remote_copy(
            src_ref=mix.at[k, at],
            dst_ref=got.at[rank, k],
            send_sem=mix_send.at[k],
            recv_sem=mix_recv.at[k],
            device_id={"tp": target},
            device_id_type=MESH,
        )

    def outputs(k, u, size):
        at = pl.ds(pl.multiple_of(u * Q_BLOCK, Q_BLOCK), size * Q_BLOCK)
        from_mix = pl.ds(pl.multiple_of(rank * rank_rows + u * Q_BLOCK, Q_BLOCK), size * Q_BLOCK)
        shares, weights = [], []
        for step in range(ranks):
            source = rank_from(step) if step < ranks - 1 else rank
            shares.append(got[source, k, at, :] if step < ranks - 1 else mix[k, from_mix, :])
            weights.append(wo[pl.ds(pl.multiple_of((source * kv_local + k) * LANES, LANES), LANES), :])
        shares, weights = jnp.concatenate(shares, axis=1), jnp.concatenate(weights, axis=0)
        return at, jnp.dot(shares, weights, preferred_element_type=f32)

    def every_mix(k):
        return pltpu.make_async_remote_copy(
            src_ref=got.at[pl.ds(0, ranks - 1), k],
            dst_ref=got.at[pl.ds(0, ranks - 1), k],
            send_sem=mix_send.at[k],
            recv_sem=mix_recv.at[k],
            device_id={"tp": rank_at(0)},
            device_id_type=MESH,
        )

    def add_head(k):
        every_mix(k).wait_recv()

        two = 2 if group % 2 == 0 else 1

        def part(n, carry):
            at, more = outputs(k, n * two, two)
            acc[at, :] = more if k == 0 else acc[at, :] + more
            return carry

        lax.fori_loop(0, group // two, part, 0)

    copies[-1].wait()

    def late(k, blocks_of):
        ats = [pl.ds(pl.multiple_of(j * Q_BLOCK, Q_BLOCK), Q_BLOCK) for j in blocks_of]
        outs = [part_out[k, j] for j in blocks_of]
        if far_moves:
            fars = [far_parts(far_moves, k, j) for j in blocks_of]
            ss = [scores(parts, k, j) for (parts, _), j in zip(fars, blocks_of)]
            ss = [add_bias(s, bias_of(usable)) for s, (_, usable) in zip(ss, fars)]
            old = [part_top[k, j] for j in blocks_of]
            new = [jnp.maximum(t, jnp.max(s, axis=0, keepdims=True)) for t, s in zip(old, ss)]
            es = [jnp.exp(s - t).astype(bf16) for s, t in zip(ss, new)]
            more = [
                jnp.dot(values_of(parts), e, preferred_element_type=f32) for (parts, _), e in zip(fars, es)
            ]
            outs = [o * jnp.exp(a - b) + m for o, a, b, m in zip(outs, old, new, more)]
        for at, out in zip(ats, outs):
            o = out[:HEAD_DIM] / out[HEAD_DIM : HEAD_DIM + 1]
            o = [o[:, n * Q_BLOCK : (n + 1) * Q_BLOCK] * gate_row(1, 2 * k + n, at) for n in range(2)]
            turned = oc[k, :, at] + jnp.concatenate(o, axis=0)
            mix[k, at, :] = turned.T.astype(bf16)

    def choose(k, step, carry):
        pl.when((step > 0) & (step < ranks - 2))(lambda: mix_copy(k, step - 1).start())
        wait_far(step, k)
        late(k, [rank_at(step) * group + u for u in range(group)])
        return carry

    for k in range(kv_local):
        lax.fori_loop(0, ranks - 2, functools.partial(choose, k), 0)
        if ranks > 2:
            mix_copy(k, ranks - 3).start()
        if k > 0:
            add_head(k - 1)
        lax.fori_loop(ranks - 2, ranks - 1, functools.partial(choose, k), 0)
        mix_copy(k, ranks - 2).start()
        size = group // parts_last[k]
        for n in range(parts_last[k]):
            wait_far(ranks - 1 + n, k)
            mine = [n * size + u for u in range(size)]
            late(k, [rank * group + u for u in mine])
            if k == kv_local - 1:
                if n == 0:
                    every_mix(k).wait_recv()
                at, more = outputs(k, n * size, size)
                out_ref[at, :] = (more if k == 0 else acc[at, :] + more).astype(bf16)


    for k in range(kv_local):
        if planes > 1:
            pl.when(z < last)(lambda k=k: own_copy(k, everything).wait_send())

    def sent(region, send):
        return remote(region, region, send, sum_recv.at[0, 0], above)

    for dx in range(1, across):
        pl.when(x + dx < across)(
            lambda dx=dx: sent(stage_x.at[0, dx - 1], x_send.at[planes + dx - 1]).wait_send()
        )
    for dz, k in relays:
        whole = (z >= dz) & ((z < last) | (dz == 1))
        if dz + 1 < last:
            pl.when(whole & (z + 1 < last))(lambda dz=dz, k=k: up_copy(dz, k).wait_send())
        if k == 0 and dz + 1 <= last:
            pl.when(whole & (z + 1 == last))(
                lambda dz=dz: sent(stage_t.at[dz - 1], t_send.at[dz - 1]).wait_send()
            )
        if k == 0 and across > 1:
            pl.when(whole)(lambda dz=dz: sent(stage_x.at[dz], x_send.at[dz]).wait_send())
    for dz in range(1, planes):
        pl.when(z + dz <= last)(lambda dz=dz: sum_up(dz, me).wait_send())
    for dx in range(1, across):
        pl.when(x + dx < across)(lambda dx=dx: sum_side(0, dx, me).wait_send())
        for dz in range(1, planes):
            pl.when(z >= dz)(lambda dz=dz, dx=dx: sum_side(dz, dx, me - dz * across).wait_send())
    for k in range(kv_local):
        every_mix(k).wait_send()


def position_tables(rows, owners):
    half = HEAD_DIM // 2
    lane = np.arange(LANES)
    inverse = ROPE_BASE ** (-(lane % half).astype(np.float64) / half)
    sign = np.where(lane % HEAD_DIM < half, -1.0, 1.0)

    def both(positions):
        phase = positions[:, None].astype(np.float64) * inverse[None, :]
        return np.stack([np.cos(phase), np.sin(phase) * sign]).astype(np.float32)

    return both(np.arange(TILE)), both(np.arange(0, owners * rows, TILE))


def per_device(
    tokens,
    norm_gain,
    query_weight,
    cmp_key_weight,
    cmp_value_weight,
    sel_key_weight,
    sel_value_weight,
    branch_weight,
    key_embed,
    key_inner,
    key_outer,
    value_embed,
    value_inner,
    value_outer,
    out_weight,
    chosen,
):
    rows, width = tokens.shape
    kv_local = key_embed.shape[0]
    owners, ranks = lax.axis_size("kv"), lax.axis_size("tp")
    planes = PLANES if owners % PLANES == 0 else 1
    across = owners // planes
    span = rows // SEL_BLOCK
    q_blocks = rows // Q_BLOCK
    blocks = rows // CMP_BLOCK
    rank_rows = rows // ranks
    kv_width = kv_local * HEAD_DIM

    weights = [sel_key_weight, sel_value_weight, cmp_key_weight, cmp_value_weight]
    if kv_width % LANES:
        weights = [jnp.concatenate(weights, axis=1)]
    fine, coarse = position_tables(rows, owners)
    operands = (
        chosen.transpose(0, 2, 1),
        norm_gain.reshape(width // LANES, LANES),
        key_embed,
        key_outer,
        value_embed,
        value_outer,
        tokens,
        query_weight,
        branch_weight.transpose(0, 2, 1),
        key_inner.transpose(0, 2, 1),
        value_inner.transpose(0, 2, 1),
        out_weight,
        jnp.asarray(fine),
        jnp.asarray(coarse),
        *weights,
    )
    vmem = pl.BlockSpec(memory_space=pltpu.VMEM)
    hbm = pl.BlockSpec(memory_space=pl.ANY)
    dma = pltpu.SemaphoreType.DMA
    picked = (q_blocks, SEL_BLOCK, LANES)
    whole = (span, SEL_BLOCK, LANES)
    n_local = 3 + len(weights) + 8 + 2 + 2
    picks = (owners * kv_local, chosen.shape[1])
    down = max(planes - 2, 1)
    n_pieces = ranks + 1
    return pl.pallas_call(
        functools.partial(layer_kernel, planes, len(weights)),
        in_specs=[hbm] * len(operands),
        out_specs=vmem,
        out_shape=pltpu.VMEM((rank_rows, out_weight.shape[1]), bf16),
        scratch_shapes=[
            pltpu.SMEM(picks, jnp.int32),
            pltpu.VMEM(picks, jnp.int32),
            pltpu.VMEM((kv_local, chosen.shape[2], chosen.shape[1]), jnp.int32),
            pltpu.VMEM((width // LANES, LANES), bf16),
            pltpu.VMEM((1, width), f32),
            pltpu.VMEM(key_embed.shape, bf16),
            pltpu.VMEM(key_outer.shape, bf16),
            pltpu.VMEM(value_embed.shape, bf16),
            pltpu.VMEM(value_outer.shape, bf16),
            pltpu.VMEM((kv_local, *whole), bf16),
            pltpu.VMEM((max(owners - 1, 1), kv_local, *picked), bf16),
            pltpu.VMEM((kv_local, q_blocks, HEAD_DIM + ONES, 2 * Q_BLOCK), f32),
            pltpu.VMEM((kv_local, q_blocks, 1, 2 * Q_BLOCK), f32),
            pltpu.VMEM((max(planes - 1, 1), max(across - 1, 1), kv_local, *picked), bf16),
            pltpu.VMEM((down, across, kv_local, *picked), bf16),
            pltpu.VMEM((min(3, rows // TILE), TILE, width), bf16),
            pltpu.VMEM(tokens.shape, bf16),
            pltpu.VMEM((width, 4 * kv_width), bf16),
            pltpu.VMEM(query_weight.shape, bf16),
            pltpu.VMEM((2 * branch_weight.shape[2], width), bf16),
            pltpu.VMEM((16, width), bf16),
            pltpu.VMEM(out_weight.shape, bf16),
            pltpu.VMEM(fine.shape, f32),
            pltpu.VMEM(coarse.shape, f32),
            pltpu.VMEM((kv_local, HEAD_DIM, key_inner.shape[1]), bf16),
            pltpu.VMEM((kv_local, HEAD_DIM, key_inner.shape[1]), bf16),
            pltpu.VMEM((kv_local, 2, LANES, rows), bf16),
            pltpu.VMEM((kv_local, 2, LANES, rows), bf16),
            pltpu.VMEM((kv_local, HEAD_DIM + ONES, owners * blocks), bf16),
            pltpu.VMEM((rows, kv_width), f32),
            pltpu.VMEM((rows, kv_width), f32),
            pltpu.VMEM((16, rows), f32),
            pltpu.VMEM((owners, kv_local, blocks, LANES), bf16),
            pltpu.VMEM((kv_local, LANES, rows), f32),
            pltpu.VMEM((kv_local, rows, LANES), bf16),
            pltpu.VMEM((ranks, kv_local, rank_rows, LANES), bf16),
            pltpu.VMEM((rank_rows, out_weight.shape[1]), f32),
            dma((min(3, rows // TILE),)),
            dma((n_local,)),
            dma((kv_local,)),
            dma((kv_local, down)),
            dma((kv_local, max(planes - 1, 1))),
            dma((planes + across,)),
            dma((down,)),
            dma((max(2 * across - 1, 1), kv_local)),
            dma((kv_local, n_pieces)),
            dma((across, planes)),
            dma((across, planes)),
            dma((kv_local,)),
            dma((kv_local,)),
        ]
        + [pltpu.VMEM(whole, bf16)] * (kv_local * max(planes - 1, 1)),
        compiler_params=pltpu.CompilerParams(
            collective_id=0, has_side_effects=True, vmem_limit_bytes=56 * 1024 * 1024
        ),
        cost_estimate=pl.CostEstimate(flops=int(3e10), bytes_accessed=int(2e7), transcendentals=0),
        name="layer",
    )(*operands)


def solution(mesh):
    placed = (
        P("kv", None),
        P(),
        P(None, "tp"),
        P(None, "tp"),
        P(None, "tp"),
        P(None, "tp"),
        P(None, "tp"),
        P(),
        P("tp", None, None),
        P("tp", None, None),
        P("tp", None, None),
        P("tp", None, None),
        P("tp", None, None),
        P("tp", None, None),
        P(),
        P("tp", None, None),
    )
    return jax.shard_map(
        per_device, mesh=mesh, in_specs=placed, out_specs=P(("kv", "tp"), None), check_vma=False
    )
```

```python
import functools

import numpy as np

import jax
import jax.numpy as jnp
from jax import lax
from jax.experimental import pallas as pl
from jax.experimental.pallas import tpu as pltpu
from jax.sharding import PartitionSpec as P

HEAD_DIM = 64
CMP_BLOCK = 32
SEL_BLOCK = 64
Q_BLOCK = 128
LANES = 2 * HEAD_DIM
PLANES = 4
TILE = 256
ONES = 16
MESH = pl.DeviceIdType.MESH

ROPE_BASE = 10000.0
norm_eps = 1e-06
MASKED = -1e30

f32 = jnp.float32
bf16 = jnp.bfloat16


def low_lanes(shape):
    return lax.broadcasted_iota(jnp.int32, shape, len(shape) - 1) < HEAD_DIM


def nt_dot(a, b):
    return lax.dot_general(a, b, (((1,), (1,)), ((), ())), preferred_element_type=f32)


def swap(x):
    return pltpu.roll(x, HEAD_DIM, 1)


def turn(x, cosine, sine):
    half = HEAD_DIM // 2
    lane = lax.broadcasted_iota(jnp.int32, x.shape, 1)
    first = lax.rem(lane, HEAD_DIM) < half
    partner = jnp.where(first, pltpu.roll(x, LANES - half, 1), pltpu.roll(x, half, 1))
    return x * cosine + partner * sine


def pack_pair(keys, turned):
    rows = turned.shape[0]
    low = low_lanes((rows, LANES))
    return (
        jnp.where(low, keys[:rows], swap(turned)).astype(bf16),
        jnp.where(low, keys[rows:], turned).astype(bf16),
    )


def values_of(parts):
    low = low_lanes(parts[0].shape)
    pairs = [jnp.where(low, swap(parts[n]), parts[n + 1]) for n in range(0, len(parts), 2)]
    values = jnp.concatenate(pairs, axis=1)
    return jnp.concatenate([values, jnp.ones((ONES, values.shape[1]), values.dtype)], axis=0)


def layer_kernel(planes, pieces, *refs):
    (
        chosen_hbm,
        gain_hbm,
        ke_hbm,
        ko_hbm,
        ve_hbm,
        vo_hbm,
        tok_hbm,
        query_hbm,
        branch_hbm,
        ki_hbm,
        vi_hbm,
        wo_hbm,
        fine_hbm,
        coarse_hbm,
    ) = refs[:14]
    piece_hbm, refs = refs[14 : 14 + pieces], refs[14 + pieces :]
    out_ref, refs = refs[0], refs[1:]
    (
        pick,
        found,
        chosen_ref,
        gain_ref,
        gain_row,
        ke_ref,
        ko_ref,
        ve_ref,
        vo_ref,
        own,
        sel,
        part_out,
        part_top,
        stage_x,
        stage_t,
        help_q,
        help_sel,
        help_out,
        help_stat,
        got_out,
        got_stat,
        tok,
        normed,
        w_kv,
        w_q,
        w_gate,
        w_own,
        wo,
        fine,
        coarse,
        ki,
        vi,
        qp,
        qt,
        vsum,
        ck,
        cv,
        gate,
        sums,
        oc,
        mix,
        got,
        acc,
        tok_sem,
        local_sem,
        own_send,
        col_send,
        col_recv,
        x_send,
        t_send,
        near_recv,
        far_recv,
        sum_send,
        sum_recv,
        mix_send,
        mix_recv,
        query_send,
        query_recv,
        help_recv,
        answer_send,
        answer_recv,
    ) = refs[:61]
    col = refs[61:]

    kv_local = own.shape[0]
    span = own.shape[1]
    owners, ranks = sums.shape[0], got.shape[0]
    rows, width = normed.shape
    across = owners // planes
    last = planes - 1
    q_blocks = rows // Q_BLOCK
    all_blocks = owners * q_blocks
    blocks = rows // CMP_BLOCK
    tiles = rows // TILE
    ring = tok.shape[0]
    rank_rows = rows // ranks
    group = rank_rows // Q_BLOCK
    heads = branch_hbm.shape[1]
    heads_local = 2 * kv_local
    kv_width = kv_local * HEAD_DIM
    scale = HEAD_DIM ** (-0.5)
    me, rank = lax.axis_index("kv"), lax.axis_index("tp")
    z, x = me // across, me % across

    barrier = pltpu.get_barrier_semaphore()
    for d in range(1, owners):
        pl.semaphore_signal(barrier, inc=1, device_id={"kv": (me + d) % owners}, device_id_type=MESH)
    for d in range(1, ranks):
        pl.semaphore_signal(barrier, inc=1, device_id={"tp": (rank + d) % ranks}, device_id_type=MESH)

    def rows_at(i):
        return pl.ds(pl.multiple_of(i * TILE, TILE), TILE)

    def tok_copy(i):
        return pltpu.make_async_copy(tok_hbm.at[rows_at(i)], tok.at[lax.rem(i, ring)], tok_sem.at[lax.rem(i, ring)])

    early = [(gain_hbm, gain_ref), (fine_hbm, fine), (coarse_hbm, coarse)]
    first = 0
    for ref in piece_hbm:
        early.append((ref, w_kv.at[:, pl.ds(first, ref.shape[1])]))
        first += ref.shape[1]
    late = [(chosen_hbm, chosen_ref), (ki_hbm, ki), (vi_hbm, vi), (query_hbm, w_q)]
    late += [(ke_hbm, ke_ref), (ko_hbm, ko_ref), (ve_hbm, ve_ref), (vo_hbm, vo_ref)]
    late += [(branch_hbm.at[b], w_gate.at[pl.ds(b * heads, heads)]) for b in range(2)]
    final = [(wo_hbm, wo), (found, pick)]
    copies = [
        pltpu.make_async_copy(a, b, local_sem.at[n]) for n, (a, b) in enumerate(early + late + final)
    ]
    to_smem = copies.pop()
    tok_copy(0).start()
    for copy in copies[: len(early)]:
        copy.start()
    if tiles > 1:
        tok_copy(1).start()

    for ref in (qp, qt):
        ref[:, :, HEAD_DIM:, :] = jnp.zeros((kv_local, 2, HEAD_DIM, rows), bf16)
    moves = [(dz, dx) for dz in range(planes) for dx in range(across) if (dz, dx) != (0, 0)]

    def slot(dz, dx):
        return dz * across + dx - 1

    def present(dz, dx):
        return (x >= dx) if dz == 0 else (z >= dz)

    for dz, dx in moves:

        def clear(dz=dz, dx=dx):
            for k in range(kv_local):
                sel[slot(dz, dx), k] = jnp.zeros(sel.shape[2:], bf16)

        pl.when(jnp.logical_not(present(dz, dx)))(clear)
    for d in range(1, owners):

        def clear_sums(d=d):
            for k in range(kv_local):
                sums[me + d, k] = jnp.zeros(sums.shape[2:], bf16)

        pl.when(me + d < owners)(clear_sums)


    def remote(src, dst, send, recv, target):
        return pltpu.make_async_remote_copy(
            src_ref=src,
            dst_ref=dst,
            send_sem=send,
            recv_sem=recv,
            device_id={"kv": target},
            device_id_type=MESH,
        )

    above = lax.rem(me + across, owners)

    def own_copy(k, at):
        return remote(own.at[k, at], col[k].at[at], own_send.at[k], col_recv.at[k, 0], above)

    def col_of(dz, k):
        return col[(dz - 1) * kv_local + k]

    def up_copy(dz, k):
        return remote(
            col_of(dz, k), col_of(dz + 1, k), col_send.at[k, dz - 1], col_recv.at[k, dz], above
        )

    def side_copy(dz, dx, k):
        return remote(
            stage_x.at[dz, dx - 1, k],
            sel.at[slot(dz, dx), k],
            x_send.at[dz if dz else planes + dx - 1],
            near_recv.at[slot(dz, dx), k],
            z * across + (x + dx) % across,
        )

    def rank_at(step):
        if ranks % 2:
            return (rank + 1 + step) % ranks
        chip = (rank // 2 + 1 + step // 2) % (ranks // 2)
        return chip * 2 + (rank + step + 1) % 2

    def rank_from(step):
        if ranks % 2:
            return (rank + 2 * ranks - 1 - step) % ranks
        chip = (rank // 2 + ranks - 1 - step // 2) % (ranks // 2)
        return chip * 2 + (rank + step + 1) % 2

    own_group = pl.ds(rank * group, group)

    def piece_at(piece):
        return pl.ds(rank_at(piece) * group, group)

    def far_side_copy(dz, dx, k, piece):
        at = piece_at(piece)
        return remote(
            stage_x.at[dz, dx - 1, k, at],
            sel.at[slot(dz, dx), k, at],
            x_send.at[dz],
            far_recv.at[k, piece],
            z * across + (x + dx) % across,
        )

    def top_copy(dz, dx, k, piece):
        at = piece_at(piece)
        return remote(
            stage_t.at[dz - 1, dx, k, at],
            sel.at[slot(dz + 1, dx), k, at],
            t_send.at[dz - 1, 0 if dx == 0 else 1],
            far_recv.at[k, piece],
            lax.rem((z + 1) * across + (x + dx) % across, owners),
        )

    def help_copy(dz, dx, k):
        return remote(
            stage_t.at[dz - 1, dx, k, own_group],
            help_sel.at[dz - 1, dx - 1, k],
            t_send.at[dz - 1, 1],
            help_recv.at[k],
            z * across + (x + dx) % across,
        )

    def help_queries():
        at = pl.ds(pl.multiple_of(rank * rank_rows, rank_rows), rank_rows)
        below = lax.rem(me + owners - across, owners)
        return remote(qt.at[:, :, :, at], help_q, query_send.at[0], query_recv.at[0], below)

    def help_answer(k, n):
        src, dst = ((help_out, got_out), (help_stat, got_stat))[n]
        return remote(src.at[k], dst.at[k], answer_send.at[k, n], answer_recv.at[k, n], above)

    def gather(src, dst, source, k, device):
        row, base = source * kv_local + k, device * q_blocks

        def one(j, carry):
            dst[j] = src[jnp.maximum(pick[row, base + j], 0)]
            return carry

        lax.fori_loop(0, q_blocks, one, 0, unroll=4)

    def relay(dz, k):
        whole = (z >= dz) & ((z < last) | (dz == 1))

        def go():
            remote(col_of(dz, k), col_of(dz, k), own_send.at[k], col_recv.at[k, dz - 1], above).wait_recv()
            source = me - dz * across
            if dz + 1 < last:
                pl.when(z + 1 < last)(lambda: up_copy(dz, k).start())
            if dz + 1 <= last:

                def to_top():
                    for dx in range(across):
                        gather(
                            col_of(dz, k),
                            stage_t.at[dz - 1, dx, k],
                            source,
                            k,
                            (z + 1) * across + (x + dx) % across,
                        )
                    for dx in range(1, across):
                        help_copy(dz, dx, k).start()
                    for s in range(ranks - 1):
                        for dx in range(across):
                            top_copy(dz, dx, k, s).start()

                pl.when(z + 1 == last)(to_top)
            for dx in range(1, across):
                there = z * across + (x + dx) % across
                gather(col_of(dz, k), stage_x.at[dz, dx - 1, k], source, k, there)
                if dz < 2:
                    side_copy(dz, dx, k).start()
                else:
                    for piece in range(ranks):
                        far_side_copy(dz, dx, k, piece).start()
            gather(col_of(dz, k), sel.at[slot(dz, 0), k], source, k, me)

        pl.when(whole)(go)


    def norm_tile(i):
        t = tok[lax.rem(i, ring)].astype(f32)
        inv = lax.rsqrt(jnp.mean(t * t, axis=-1, keepdims=True) + norm_eps)
        normed[rows_at(i), :] = (t * inv * gain_row[...]).astype(bf16)
        pl.when(i + ring < tiles)(lambda: tok_copy(i + ring).start())

    def tables(i):
        row = pl.ds(me * tiles + i, 1)
        cos_c, sin_c = coarse[0, row, :], coarse[1, row, :]
        return fine[0] * cos_c - fine[1] * sin_c, fine[1] * cos_c + fine[0] * sin_c

    def project_kv(i):
        at = rows_at(i)
        y = jnp.dot(normed[at, :], w_kv[...], preferred_element_type=f32)
        cosine, sine = tables(i)
        for k in range(kv_local):
            if kv_local == 1:
                value = y[:, :LANES]
                key = turn(value, cosine, sine)
                keys, first = key, HEAD_DIM
            elif k % 2 == 0:
                key = turn(y[:, k * HEAD_DIM : k * HEAD_DIM + LANES], cosine, sine)
                value = y[:, kv_width + k * HEAD_DIM : kv_width + k * HEAD_DIM + LANES]
                keys, first = key, 0
            else:
                keys, first = swap(key), HEAD_DIM
            for t in range(TILE // (2 * SEL_BLOCK)):
                two = slice(t * 2 * SEL_BLOCK, (t + 1) * 2 * SEL_BLOCK)
                turned = value[two].T[first : first + HEAD_DIM]
                a, b = pack_pair(keys[two], turned)
                own[k, i * (TILE // SEL_BLOCK) + 2 * t] = a
                own[k, i * (TILE // SEL_BLOCK) + 2 * t + 1] = b
        ck[at, :] = y[:, 2 * kv_width : 3 * kv_width].astype(bf16).astype(f32)
        cv[at, :] = y[:, 3 * kv_width : 4 * kv_width].astype(bf16).astype(f32)

    def send_tile(i):
        here = pl.ds(i * (TILE // SEL_BLOCK), TILE // SEL_BLOCK)
        if planes > 1:
            pl.when(z < last)(lambda: own_copy(0, here).start())

    copies[0].wait()
    for c in range(gain_ref.shape[0]):
        gain_row[:, c * LANES : (c + 1) * LANES] = gain_ref[c : c + 1, :].astype(f32)
    tok_copy(0).wait()
    norm_tile(0)
    for copy in copies[1 : len(early)]:
        copy.wait()
    for i in range(2, min(ring, tiles)):
        tok_copy(i).start()
    for copy in copies[len(early) :]:
        copy.start()
    pl.semaphore_wait(barrier, owners + ranks - 2)

    def first_pass(i, carry):
        pl.when(i > 0)(lambda: send_tile(i - 1))
        tok_copy(i + 1).wait()
        norm_tile(i + 1)
        project_kv(i)
        return carry

    lax.fori_loop(0, tiles - 1, first_pass, 0)
    if tiles > 1:
        send_tile(tiles - 2)
    project_kv(tiles - 1)

    for copy in copies[len(early) : len(early) + len(late)]:
        copy.wait()
    send_tile(tiles - 1)


    for s in range(owners):
        for k in range(kv_local):
            place = chosen_ref[k] - s * span
            place = jnp.where((place >= 0) & (place < span), place, -1)
            found[s * kv_local + k : s * kv_local + k + 1, :] = jnp.max(place, axis=0, keepdims=True)
    to_smem.start()

    quarter = span // 4
    for k in range(1, kv_local):
        if planes > 1:
            pl.when(z < last)(lambda k=k: own_copy(k, pl.ds(0, quarter)).start())


    def summarize(x_ref, e_ref, i_ref, o_ref):
        embed = jnp.concatenate([e_ref[k].astype(f32) for k in range(kv_local)], axis=1)
        parts = [
            x_ref[pl.ds(c, blocks, stride=CMP_BLOCK), :] + embed[c : c + 1] for c in range(CMP_BLOCK)
        ]
        result = []
        for k in range(kv_local):
            if kv_local == 1:
                flat = jnp.concatenate([p.astype(bf16) for p in parts], axis=1)
            else:
                g, odd = k // 2 * LANES, k % 2
                low = low_lanes((blocks, LANES))
                cut = []
                for c in range(0, CMP_BLOCK, 2):
                    a, b = parts[c][:, g : g + LANES], parts[c + 1][:, g : g + LANES]
                    both = jnp.where(low, swap(a), b) if odd else jnp.where(low, a, swap(b))
                    cut.append(both.astype(bf16))
                flat = jnp.concatenate(cut, axis=1)
            hidden = jax.nn.gelu(nt_dot(flat, i_ref[k])).astype(bf16)
            result.append(jnp.dot(hidden, o_ref[k], preferred_element_type=f32))
        return result

    sk = summarize(ck, ke_ref, ki, ko_ref)
    sv = summarize(cv, ve_ref, vi, vo_ref)
    for k in range(kv_local):
        sums[me, k] = jnp.concatenate([sk[k], sv[k].T], axis=1).astype(bf16)

    def sum_up(dz, source):
        there = lax.rem(me + dz * across, owners)
        return remote(sums.at[source], sums.at[source], sum_send.at[0, dz], sum_recv.at[0, dz], there)

    def sum_side(dz, dx, source):
        there = z * across + (x + dx) % across
        return remote(sums.at[source], sums.at[source], sum_send.at[dx, dz], sum_recv.at[dx, dz], there)

    for dz in range(1, planes):
        pl.when(z + dz <= last)(lambda dz=dz: sum_up(dz, me).start())
    for dx in range(1, across):
        pl.when(x + dx < across)(lambda dx=dx: sum_side(0, dx, me).start())
    to_smem.wait()
    for dx in range(1, across):
        for k in range(kv_local):
            gather(own.at[k], stage_x.at[0, dx - 1, k], me, k, z * across + (x + dx) % across)
    everything = pl.ds(0, span)
    for k in range(1, kv_local):
        if planes > 1:
            pl.when(z < last)(lambda k=k: own_copy(k, pl.ds(quarter, span - quarter)).start())
    for dx in range(1, across):
        pl.when(x + dx < across)(lambda dx=dx: side_copy(0, dx, 0).start())


    mine = lax.broadcasted_iota(jnp.int32, (w_own.shape[0], w_gate.shape[0]), 0)
    branch = jnp.where(mine >= heads_local, 1, 0)
    wanted = branch * heads + rank * heads_local + mine - branch * heads_local
    wanted = jnp.where(mine < 2 * heads_local, wanted, -1)
    source = lax.broadcasted_iota(jnp.int32, mine.shape, 1)
    chooser = jnp.where(source == wanted, 1.0, 0.0).astype(bf16)
    w_own[...] = jnp.dot(chooser, w_gate[...], preferred_element_type=f32).astype(bf16)

    def second_pass(i, carry):
        at = rows_at(i)
        n = normed[at, :]
        y = jnp.dot(n, w_q[...], preferred_element_type=f32)
        cosine, sine = tables(i)
        for k in range(kv_local):
            v = y[:, k * LANES : (k + 1) * LANES] * scale
            for ref, q in ((qp, v), (qt, turn(v, cosine, sine))):
                turned = q.T.astype(bf16)
                for u in range(2):
                    ref[k, u, :HEAD_DIM, at] = turned[u * HEAD_DIM : (u + 1) * HEAD_DIM]
        gate[:, at] = jax.nn.sigmoid(nt_dot(w_own[...], n))
        return carry

    lax.fori_loop(0, tiles // 2, second_pass, 0)
    for dz in range(1, planes):

        def pass_on(dz=dz):
            below = me - dz * across
            sum_up(dz, below).wait_recv()
            for dx in range(1, across):
                sum_side(dz, dx, below).start()

        pl.when(z >= dz)(pass_on)
    lax.fori_loop(tiles // 2, tiles, second_pass, 0)
    if planes > 2:
        pl.when(z == last)(lambda: help_queries().start())
    relays = [(dz, k) for dz in range(1, max(2, last)) for k in range(kv_local)] if planes > 1 else []


    if relays:
        relay(*relays[0])
    for dx in range(1, across):
        for k in range(1, kv_local):
            pl.when(x + dx < across)(lambda dx=dx, k=k: side_copy(0, dx, k).start())
    for dz in range(planes):
        for dx in range(1, across):
            there = lax.rem((z - dz + planes) * across + (x + across - dx) % across, owners)
            pl.when(present(dz, dx))(
                lambda dz=dz, dx=dx, there=there: sum_side(dz, dx, there).wait_recv()
            )

    def gate_row(branch, head, at):
        return gate[branch * heads_local + head : branch * heads_local + head + 1, at]

    for k in range(kv_local):
        vsum[k] = values_of([sums[s, k] for s in range(owners)])

    def compress(i, carry):
        at = rows_at(i)
        lane = lax.broadcasted_iota(jnp.int32, (1, 2 * TILE), 1)
        pos = me * rows + i * TILE + jnp.where(lane >= TILE, lane - TILE, lane)
        block = lax.broadcasted_iota(jnp.int32, (owners * blocks, 1), 0)
        allowed = (block + 1) * CMP_BLOCK - 1 <= pos
        for k in range(kv_local):
            keys = jnp.concatenate([sums[s, k] for s in range(owners)], axis=0)
            q = jnp.concatenate([qp[k, 0, :, at], qp[k, 1, :, at]], axis=1)
            s = jnp.where(allowed, jnp.dot(keys, q, preferred_element_type=f32), MASKED)
            top = jnp.max(s, axis=0, keepdims=True)
            e = jnp.exp(s - top).astype(bf16)
            o = jnp.dot(vsum[k], e, preferred_element_type=f32)
            o = jnp.where(pos >= CMP_BLOCK - 1, o[:HEAD_DIM] / o[HEAD_DIM : HEAD_DIM + 1], 0.0)
            for u in range(2):
                part = o[:, u * TILE : (u + 1) * TILE] * gate_row(0, 2 * k + u, at)
                oc[k, u * HEAD_DIM : (u + 1) * HEAD_DIM, at] = part
        return carry

    bounds = [tiles * n // kv_local for n in range(kv_local + 1)]
    for k in range(kv_local):
        if k > 0 and planes > 1:
            relay(1, k)
        lax.fori_loop(bounds[k], bounds[k + 1], compress, 0)


    def is_top(dz):
        return (z == last) & (dz >= 2)

    def wait_side(dz, dx, k):
        pl.when(present(dz, dx))(lambda: side_copy(dz, dx, k).wait_recv())

    def bias_of(usable):
        return [jnp.where(u, 0.0, MASKED).astype(f32) for u in usable]

    def add_bias(s, bias):
        cut = [s[n * SEL_BLOCK : (n + 1) * SEL_BLOCK] + b for n, b in enumerate(bias)]
        return jnp.concatenate(cut, axis=0)

    def far_parts(some_moves, k, j):
        parts, usable = [], []
        for dz, dx in some_moves:
            parts.append(sel[slot(dz, dx), k, j])
            source = lax.rem(me - dz * across - x + (x + across - dx) % across + owners, owners)
            usable.append((pick[source * kv_local + k, me * q_blocks + j] >= 0) & present(dz, dx))
        return parts, usable

    near_moves = [m for m in moves if m[0] < 2]
    far_moves = [m for m in moves if m[0] >= 2]
    own_blocks = Q_BLOCK // SEL_BLOCK

    def queries(k, j):
        at = pl.ds(pl.multiple_of(j * Q_BLOCK, Q_BLOCK), Q_BLOCK)
        return jnp.concatenate([qt[k, 0, :, at], qt[k, 1, :, at]], axis=1)

    def scores(parts, k, j):
        keys = jnp.concatenate(parts, axis=0)
        return jnp.dot(keys, queries(k, j), preferred_element_type=f32)

    unroll = group if group < 4 else 4

    def answer(k):
        def go():
            if k == 0:
                help_queries().wait_recv()
            if across > 1:
                everyone = help_sel.at[:, :, k]
                remote(everyone, everyone, t_send.at[0, 0], help_recv.at[k], above).wait_recv()
            fars, ss = [], []
            for u in range(group):
                parts, usable = [], []
                for dz in range(1, planes - 1):
                    for dx in range(across):
                        block = stage_t[dz - 1, 0, k, rank * group + u] if dx == 0 else help_sel[dz - 1, dx - 1, k, u]
                        source = lax.rem((z - dz + planes) * across + (x + across - dx) % across, owners)
                        there = lax.rem(me + across, owners) * q_blocks + rank * group + u
                        parts.append(block)
                        usable.append(pick[source * kv_local + k, there] >= 0)
                cut = slice(u * Q_BLOCK, (u + 1) * Q_BLOCK)
                q = jnp.concatenate([help_q[k, 0, :, cut], help_q[k, 1, :, cut]], axis=1)
                s = jnp.dot(jnp.concatenate(parts, axis=0), q, preferred_element_type=f32)
                fars.append(parts)
                ss.append(add_bias(s, bias_of(usable)))
            tops = [jnp.max(s, axis=0, keepdims=True) for s in ss]
            es = [jnp.exp(s - t).astype(bf16) for s, t in zip(ss, tops)]
            outs = [jnp.dot(values_of(p), e, preferred_element_type=f32) for p, e in zip(fars, es)]
            row = lax.broadcasted_iota(jnp.int32, (8, 2 * Q_BLOCK), 0)
            for u in range(group):
                help_out[k, u] = outs[u][:HEAD_DIM].astype(bf16)
                help_stat[k, u] = jnp.where(row == 0, outs[u][HEAD_DIM : HEAD_DIM + 1], tops[u])
            for n in range(2):
                help_answer(k, n).start()

        pl.when(z == last - 1)(go)

    def near(k, some, carry):
        row = lax.broadcasted_iota(jnp.int32, (Q_BLOCK, 2 * Q_BLOCK), 0)
        lane = lax.broadcasted_iota(jnp.int32, row.shape, 1)
        lane = jnp.where(lane >= Q_BLOCK, lane - Q_BLOCK, lane)
        js = [some * unroll + u for u in range(unroll)]
        all_parts, ss = [], []
        for j in js:
            parts = [own[k, j * own_blocks + b] for b in range(own_blocks)]
            mine = pick[me * kv_local + k, me * q_blocks + j]
            parts.append(own[k, jnp.maximum(mine, 0)])
            more, usable = far_parts(near_moves, k, j)
            bias = bias_of([(mine >= 0) & (mine < j * own_blocks)] + usable)
            all_parts.append(parts + more)
            s = scores(all_parts[-1], k, j)
            close = jnp.where(row > lane, MASKED, s[:Q_BLOCK])
            ss.append(jnp.concatenate([close, add_bias(s[Q_BLOCK:], bias)], axis=0))
        tops = [jnp.max(s, axis=0, keepdims=True) for s in ss]
        es = [jnp.exp(s - top).astype(bf16) for s, top in zip(ss, tops)]
        for j, parts, e, top in zip(js, all_parts, es, tops):
            part_out[k, j] = jnp.dot(values_of(parts), e, preferred_element_type=f32)
            part_top[k, j] = top
        return carry

    for k in range(kv_local):
        for dz, dx in near_moves:
            if dx:
                wait_side(dz, dx, k)
        lax.fori_loop(0, q_blocks // unroll, functools.partial(near, k), 0)
        if k > 0 and far_moves:
            answer(k - 1)
        for dz in range(2, last):
            relay(dz, k)

    def wait_far(piece, k):
        if not far_moves:
            return
        at = piece_at(piece)
        own_piece = isinstance(piece, int) and piece == ranks - 1

        def wait(first, count):
            region = sel.at[pl.ds(first, count), k, at]
            remote(region, region, x_send.at[0], far_recv.at[k, piece], above).wait_recv()

        if not own_piece:
            pl.when(z == last)(lambda: wait(slot(2, 0), (planes - 2) * across))
        if across > 1:
            for dz in range(2, last):
                pl.when(z == dz)(lambda: wait(slot(2, 1), across - 1))

    def mix_copy(k, step):
        target = rank_at(step)
        at = pl.ds(pl.multiple_of(target * rank_rows, rank_rows), rank_rows)
        return pltpu.make_async_remote_copy(
            src_ref=mix.at[k, at],
            dst_ref=got.at[rank, k],
            send_sem=mix_send.at[k],
            recv_sem=mix_recv.at[k],
            device_id={"tp": target},
            device_id_type=MESH,
        )

    def outputs(k, u, size):
        at = pl.ds(pl.multiple_of(u * Q_BLOCK, Q_BLOCK), size * Q_BLOCK)
        from_mix = pl.ds(pl.multiple_of(rank * rank_rows + u * Q_BLOCK, Q_BLOCK), size * Q_BLOCK)
        shares, weights = [], []
        for step in range(ranks):
            source = rank_from(step) if step < ranks - 1 else rank
            shares.append(got[source, k, at, :] if step < ranks - 1 else mix[k, from_mix, :])
            weights.append(wo[pl.ds(pl.multiple_of((source * kv_local + k) * LANES, LANES), LANES), :])
        shares, weights = jnp.concatenate(shares, axis=1), jnp.concatenate(weights, axis=0)
        return at, jnp.dot(shares, weights, preferred_element_type=f32)

    def every_mix(k):
        return pltpu.make_async_remote_copy(
            src_ref=got.at[pl.ds(0, ranks - 1), k],
            dst_ref=got.at[pl.ds(0, ranks - 1), k],
            send_sem=mix_send.at[k],
            recv_sem=mix_recv.at[k],
            device_id={"tp": rank_at(0)},
            device_id_type=MESH,
        )

    def add_head(k):
        every_mix(k).wait_recv()

        two = 2 if group % 2 == 0 else 1

        def part(n, carry):
            at, more = outputs(k, n * two, two)
            acc[at, :] = more if k == 0 else acc[at, :] + more
            return carry

        lax.fori_loop(0, group // two, part, 0)

    copies[-1].wait()

    def late(k, blocks_of):
        ats = [pl.ds(pl.multiple_of(j * Q_BLOCK, Q_BLOCK), Q_BLOCK) for j in blocks_of]
        outs = [part_out[k, j] for j in blocks_of]
        if far_moves:
            fars = [far_parts(far_moves, k, j) for j in blocks_of]
            ss = [scores(parts, k, j) for (parts, _), j in zip(fars, blocks_of)]
            ss = [add_bias(s, bias_of(usable)) for s, (_, usable) in zip(ss, fars)]
            old = [part_top[k, j] for j in blocks_of]
            new = [jnp.maximum(t, jnp.max(s, axis=0, keepdims=True)) for t, s in zip(old, ss)]
            es = [jnp.exp(s - t).astype(bf16) for s, t in zip(ss, new)]
            more = [
                jnp.dot(values_of(parts), e, preferred_element_type=f32) for (parts, _), e in zip(fars, es)
            ]
            outs = [o * jnp.exp(a - b) + m for o, a, b, m in zip(outs, old, new, more)]
        settle(k, ats, [(out[:HEAD_DIM], out[HEAD_DIM : HEAD_DIM + 1]) for out in outs])

    def settle(k, ats, outs):
        for at, (value, total) in zip(ats, outs):
            o = value / total
            o = [o[:, n * Q_BLOCK : (n + 1) * Q_BLOCK] * gate_row(1, 2 * k + n, at) for n in range(2)]
            turned = oc[k, :, at] + jnp.concatenate(o, axis=0)
            mix[k, at, :] = turned.T.astype(bf16)

    def answered(k):
        for n in range(2):
            help_answer(k, n).wait_recv()
        ats, outs = [], []
        for u in range(group):
            j = rank * group + u
            out, top, more, stat = part_out[k, j], part_top[k, j], got_out[k, u].astype(f32), got_stat[k, u]
            both = jnp.maximum(top, stat[1:2])
            a, b = jnp.exp(top - both), jnp.exp(stat[1:2] - both)
            total = out[HEAD_DIM : HEAD_DIM + 1] * a + stat[0:1] * b
            ats.append(pl.ds(pl.multiple_of(j * Q_BLOCK, Q_BLOCK), Q_BLOCK))
            outs.append((out[:HEAD_DIM] * a + more * b, total))
        settle(k, ats, outs)

    def choose(k, step, carry):
        pl.when((step > 0) & (step < ranks - 2))(lambda: mix_copy(k, step - 1).start())
        wait_far(step, k)
        late(k, [rank_at(step) * group + u for u in range(group)])
        return carry

    for k in range(kv_local):
        lax.fori_loop(0, ranks - 2, functools.partial(choose, k), 0)
        if ranks > 2:
            mix_copy(k, ranks - 3).start()
        if k == 0 and far_moves:
            answer(kv_local - 1)
        if k > 0:
            add_head(k - 1)
        lax.fori_loop(ranks - 2, ranks - 1, functools.partial(choose, k), 0)
        mix_copy(k, ranks - 2).start()
        def mine(k=k):
            wait_far(ranks - 1, k)
            late(k, [rank * group + u for u in range(group)])

        if far_moves:
            pl.when(z == last)(functools.partial(answered, k))
            pl.when(z < last)(mine)
        else:
            mine()
    every_mix(kv_local - 1).wait_recv()
    two = 2 if group % 2 == 0 else 1
    for n in range(0, group, two):
        at, more = outputs(kv_local - 1, n, two)
        out_ref[at, :] = (more if kv_local == 1 else acc[at, :] + more).astype(bf16)


    for k in range(kv_local):
        if planes > 1:
            pl.when(z < last)(lambda k=k: own_copy(k, everything).wait_send())

    def sent(region, send):
        return remote(region, region, send, sum_recv.at[0, 0], above)

    for dx in range(1, across):
        pl.when(x + dx < across)(
            lambda dx=dx: sent(stage_x.at[0, dx - 1], x_send.at[planes + dx - 1]).wait_send()
        )
    for dz, k in relays:
        whole = (z >= dz) & ((z < last) | (dz == 1))
        if dz + 1 < last:
            pl.when(whole & (z + 1 < last))(lambda dz=dz, k=k: up_copy(dz, k).wait_send())
        if k == 0 and dz + 1 <= last:

            def sent_top(dz=dz):
                most = pl.ds(0, q_blocks - group)
                sent(stage_t.at[dz - 1, 0, :, most], t_send.at[dz - 1, 0]).wait_send()
                if across > 1:
                    sent(stage_t.at[dz - 1, pl.ds(1, across - 1)], t_send.at[dz - 1, 1]).wait_send()

            pl.when(whole & (z + 1 == last))(sent_top)
        if k == 0 and across > 1:
            pl.when(whole)(lambda dz=dz: sent(stage_x.at[dz], x_send.at[dz]).wait_send())
    for dz in range(1, planes):
        pl.when(z + dz <= last)(lambda dz=dz: sum_up(dz, me).wait_send())
    for dx in range(1, across):
        pl.when(x + dx < across)(lambda dx=dx: sum_side(0, dx, me).wait_send())
        for dz in range(1, planes):
            pl.when(z >= dz)(lambda dz=dz, dx=dx: sum_side(dz, dx, me - dz * across).wait_send())
    for k in range(kv_local):
        every_mix(k).wait_send()
        if far_moves:
            for n in range(2):
                pl.when(z == last - 1)(lambda k=k, n=n: help_answer(k, n).wait_send())
    if far_moves:
        pl.when(z == last)(lambda: help_queries().wait_send())


def position_tables(rows, owners):
    half = HEAD_DIM // 2
    lane = np.arange(LANES)
    inverse = ROPE_BASE ** (-(lane % half).astype(np.float64) / half)
    sign = np.where(lane % HEAD_DIM < half, -1.0, 1.0)

    def both(positions):
        phase = positions[:, None].astype(np.float64) * inverse[None, :]
        return np.stack([np.cos(phase), np.sin(phase) * sign]).astype(np.float32)

    return both(np.arange(TILE)), both(np.arange(0, owners * rows, TILE))


def per_device(
    tokens,
    norm_gain,
    query_weight,
    cmp_key_weight,
    cmp_value_weight,
    sel_key_weight,
    sel_value_weight,
    branch_weight,
    key_embed,
    key_inner,
    key_outer,
    value_embed,
    value_inner,
    value_outer,
    out_weight,
    chosen,
):
    rows, width = tokens.shape
    kv_local = key_embed.shape[0]
    owners, ranks = lax.axis_size("kv"), lax.axis_size("tp")
    planes = PLANES if owners % PLANES == 0 else 1
    across = owners // planes
    span = rows // SEL_BLOCK
    q_blocks = rows // Q_BLOCK
    blocks = rows // CMP_BLOCK
    rank_rows = rows // ranks
    kv_width = kv_local * HEAD_DIM

    weights = [sel_key_weight, sel_value_weight, cmp_key_weight, cmp_value_weight]
    if kv_width % LANES:
        weights = [jnp.concatenate(weights, axis=1)]
    fine, coarse = position_tables(rows, owners)
    operands = (
        chosen.transpose(0, 2, 1),
        norm_gain.reshape(width // LANES, LANES),
        key_embed,
        key_outer,
        value_embed,
        value_outer,
        tokens,
        query_weight,
        branch_weight.transpose(0, 2, 1),
        key_inner.transpose(0, 2, 1),
        value_inner.transpose(0, 2, 1),
        out_weight,
        jnp.asarray(fine),
        jnp.asarray(coarse),
        *weights,
    )
    vmem = pl.BlockSpec(memory_space=pltpu.VMEM)
    hbm = pl.BlockSpec(memory_space=pl.ANY)
    dma = pltpu.SemaphoreType.DMA
    picked = (q_blocks, SEL_BLOCK, LANES)
    whole = (span, SEL_BLOCK, LANES)
    n_local = 3 + len(weights) + 8 + 2 + 2
    picks = (owners * kv_local, chosen.shape[1])
    down = max(planes - 2, 1)
    n_pieces = ranks
    group = rank_rows // Q_BLOCK
    return pl.pallas_call(
        functools.partial(layer_kernel, planes, len(weights)),
        in_specs=[hbm] * len(operands),
        out_specs=vmem,
        out_shape=pltpu.VMEM((rank_rows, out_weight.shape[1]), bf16),
        scratch_shapes=[
            pltpu.SMEM(picks, jnp.int32),
            pltpu.VMEM(picks, jnp.int32),
            pltpu.VMEM((kv_local, chosen.shape[2], chosen.shape[1]), jnp.int32),
            pltpu.VMEM((width // LANES, LANES), bf16),
            pltpu.VMEM((1, width), f32),
            pltpu.VMEM(key_embed.shape, bf16),
            pltpu.VMEM(key_outer.shape, bf16),
            pltpu.VMEM(value_embed.shape, bf16),
            pltpu.VMEM(value_outer.shape, bf16),
            pltpu.VMEM((kv_local, *whole), bf16),
            pltpu.VMEM((max(owners - 1, 1), kv_local, *picked), bf16),
            pltpu.VMEM((kv_local, q_blocks, HEAD_DIM + ONES, 2 * Q_BLOCK), f32),
            pltpu.VMEM((kv_local, q_blocks, 1, 2 * Q_BLOCK), f32),
            pltpu.VMEM((max(planes - 1, 1), max(across - 1, 1), kv_local, *picked), bf16),
            pltpu.VMEM((down, across, kv_local, *picked), bf16),
            pltpu.VMEM((kv_local, 2, LANES, rank_rows), bf16),
            pltpu.VMEM((down, max(across - 1, 1), kv_local, group, SEL_BLOCK, LANES), bf16),
            pltpu.VMEM((kv_local, group, HEAD_DIM, 2 * Q_BLOCK), bf16),
            pltpu.VMEM((kv_local, group, 8, 2 * Q_BLOCK), f32),
            pltpu.VMEM((kv_local, group, HEAD_DIM, 2 * Q_BLOCK), bf16),
            pltpu.VMEM((kv_local, group, 8, 2 * Q_BLOCK), f32),
            pltpu.VMEM((min(3, rows // TILE), TILE, width), bf16),
            pltpu.VMEM(tokens.shape, bf16),
            pltpu.VMEM((width, 4 * kv_width), bf16),
            pltpu.VMEM(query_weight.shape, bf16),
            pltpu.VMEM((2 * branch_weight.shape[2], width), bf16),
            pltpu.VMEM((16, width), bf16),
            pltpu.VMEM(out_weight.shape, bf16),
            pltpu.VMEM(fine.shape, f32),
            pltpu.VMEM(coarse.shape, f32),
            pltpu.VMEM((kv_local, HEAD_DIM, key_inner.shape[1]), bf16),
            pltpu.VMEM((kv_local, HEAD_DIM, key_inner.shape[1]), bf16),
            pltpu.VMEM((kv_local, 2, LANES, rows), bf16),
            pltpu.VMEM((kv_local, 2, LANES, rows), bf16),
            pltpu.VMEM((kv_local, HEAD_DIM + ONES, owners * blocks), bf16),
            pltpu.VMEM((rows, kv_width), f32),
            pltpu.VMEM((rows, kv_width), f32),
            pltpu.VMEM((16, rows), f32),
            pltpu.VMEM((owners, kv_local, blocks, LANES), bf16),
            pltpu.VMEM((kv_local, LANES, rows), f32),
            pltpu.VMEM((kv_local, rows, LANES), bf16),
            pltpu.VMEM((ranks, kv_local, rank_rows, LANES), bf16),
            pltpu.VMEM((rank_rows, out_weight.shape[1]), f32),
            dma((min(3, rows // TILE),)),
            dma((n_local,)),
            dma((kv_local,)),
            dma((kv_local, down)),
            dma((kv_local, max(planes - 1, 1))),
            dma((planes + across,)),
            dma((down, 2)),
            dma((max(2 * across - 1, 1), kv_local)),
            dma((kv_local, n_pieces)),
            dma((across, planes)),
            dma((across, planes)),
            dma((kv_local,)),
            dma((kv_local,)),
            dma((1,)),
            dma((1,)),
            dma((kv_local,)),
            dma((kv_local, 2)),
            dma((kv_local, 2)),
        ]
        + [pltpu.VMEM(whole, bf16)] * (kv_local * max(planes - 1, 1)),
        compiler_params=pltpu.CompilerParams(
            collective_id=0, has_side_effects=True, vmem_limit_bytes=56 * 1024 * 1024
        ),
        cost_estimate=pl.CostEstimate(flops=int(3e10), bytes_accessed=int(2e7), transcendentals=0),
        name="layer",
    )(*operands)


def solution(mesh):
    placed = (
        P("kv", None),
        P(),
        P(None, "tp"),
        P(None, "tp"),
        P(None, "tp"),
        P(None, "tp"),
        P(None, "tp"),
        P(),
        P("tp", None, None),
        P("tp", None, None),
        P("tp", None, None),
        P("tp", None, None),
        P("tp", None, None),
        P("tp", None, None),
        P(),
        P("tp", None, None),
    )
    return jax.shard_map(
        per_device, mesh=mesh, in_specs=placed, out_specs=P(("kv", "tp"), None), check_vma=False
    )
```

```python
import functools

import numpy as np

import jax
import jax.numpy as jnp
from jax import lax
from jax.experimental import pallas as pl
from jax.experimental.pallas import tpu as pltpu
from jax.sharding import PartitionSpec as P

HEAD_DIM = 64
CMP_BLOCK = 32
SEL_BLOCK = 64
Q_BLOCK = 128
LANES = 2 * HEAD_DIM
PLANES = 4
TILE = 256
ONES = 16
MESH = pl.DeviceIdType.MESH

ROPE_BASE = 10000.0
norm_eps = 1e-06
MASKED = -1e30

f32 = jnp.float32
bf16 = jnp.bfloat16


def low_lanes(shape):
    return lax.broadcasted_iota(jnp.int32, shape, len(shape) - 1) < HEAD_DIM


def nt_dot(a, b):
    return lax.dot_general(a, b, (((1,), (1,)), ((), ())), preferred_element_type=f32)


def swap(x):
    return pltpu.roll(x, HEAD_DIM, 1)


def turn(x, cosine, sine):
    half = HEAD_DIM // 2
    lane = lax.broadcasted_iota(jnp.int32, x.shape, 1)
    first = lax.rem(lane, HEAD_DIM) < half
    partner = jnp.where(first, pltpu.roll(x, LANES - half, 1), pltpu.roll(x, half, 1))
    return x * cosine + partner * sine


def pack_pair(keys, turned):
    rows = turned.shape[0]
    low = low_lanes((rows, LANES))
    return (
        jnp.where(low, keys[:rows], swap(turned)).astype(bf16),
        jnp.where(low, keys[rows:], turned).astype(bf16),
    )


def values_of(parts):
    low = low_lanes(parts[0].shape)
    pairs = [jnp.where(low, swap(parts[n]), parts[n + 1]) for n in range(0, len(parts), 2)]
    values = jnp.concatenate(pairs, axis=1)
    return jnp.concatenate([values, jnp.ones((ONES, values.shape[1]), values.dtype)], axis=0)


def layer_kernel(planes, pieces, *refs):
    (
        chosen_hbm,
        gain_hbm,
        ke_hbm,
        ko_hbm,
        ve_hbm,
        vo_hbm,
        tok_hbm,
        query_hbm,
        branch_hbm,
        ki_hbm,
        vi_hbm,
        wo_hbm,
        fine_hbm,
        coarse_hbm,
    ) = refs[:14]
    piece_hbm, refs = refs[14 : 14 + pieces], refs[14 + pieces :]
    out_ref, refs = refs[0], refs[1:]
    (
        pick,
        found,
        chosen_ref,
        gain_ref,
        gain_row,
        ke_ref,
        ko_ref,
        ve_ref,
        vo_ref,
        own,
        sel,
        part_out,
        part_top,
        stage_x,
        stage_t,
        help_q,
        help_sel,
        help_out,
        help_stat,
        got_out,
        got_stat,
        tok,
        normed,
        w_kv,
        w_q,
        w_gate,
        w_own,
        wo,
        fine,
        coarse,
        ki,
        vi,
        qp,
        qt,
        vsum,
        ck,
        cv,
        gate,
        sums,
        oc,
        mix,
        got,
        acc,
        tok_sem,
        local_sem,
        own_send,
        col_send,
        col_recv,
        x_send,
        t_send,
        near_recv,
        far_recv,
        sum_send,
        sum_recv,
        mix_send,
        mix_recv,
        query_send,
        query_recv,
        help_recv,
        answer_send,
        answer_recv,
    ) = refs[:61]
    col = refs[61:]

    kv_local = own.shape[0]
    span = own.shape[1]
    owners, ranks = sums.shape[0], got.shape[0]
    rows, width = normed.shape
    across = owners // planes
    last = planes - 1
    q_blocks = rows // Q_BLOCK
    all_blocks = owners * q_blocks
    blocks = rows // CMP_BLOCK
    tiles = rows // TILE
    ring = tok.shape[0]
    rank_rows = rows // ranks
    group = rank_rows // Q_BLOCK
    heads = branch_hbm.shape[1]
    heads_local = 2 * kv_local
    kv_width = kv_local * HEAD_DIM
    scale = HEAD_DIM ** (-0.5)
    me, rank = lax.axis_index("kv"), lax.axis_index("tp")
    z, x = me // across, me % across

    barrier = pltpu.get_barrier_semaphore()
    for d in range(1, owners):
        pl.semaphore_signal(barrier, inc=1, device_id={"kv": (me + d) % owners}, device_id_type=MESH)
    for d in range(1, ranks):
        pl.semaphore_signal(barrier, inc=1, device_id={"tp": (rank + d) % ranks}, device_id_type=MESH)

    def rows_at(i):
        return pl.ds(pl.multiple_of(i * TILE, TILE), TILE)

    def tok_copy(i):
        return pltpu.make_async_copy(tok_hbm.at[rows_at(i)], tok.at[lax.rem(i, ring)], tok_sem.at[lax.rem(i, ring)])

    early = [(gain_hbm, gain_ref), (fine_hbm, fine), (coarse_hbm, coarse)]
    first = 0
    for ref in piece_hbm:
        early.append((ref, w_kv.at[:, pl.ds(first, ref.shape[1])]))
        first += ref.shape[1]
    late = [(chosen_hbm, chosen_ref), (ki_hbm, ki), (vi_hbm, vi), (query_hbm, w_q)]
    late += [(ke_hbm, ke_ref), (ko_hbm, ko_ref), (ve_hbm, ve_ref), (vo_hbm, vo_ref)]
    late += [(branch_hbm.at[b], w_gate.at[pl.ds(b * heads, heads)]) for b in range(2)]
    final = [(wo_hbm, wo), (found, pick)]
    copies = [
        pltpu.make_async_copy(a, b, local_sem.at[n]) for n, (a, b) in enumerate(early + late + final)
    ]
    to_smem = copies.pop()
    tok_copy(0).start()
    for copy in copies[: len(early)]:
        copy.start()
    if tiles > 1:
        tok_copy(1).start()

    for ref in (qp, qt):
        ref[:, :, HEAD_DIM:, :] = jnp.zeros((kv_local, 2, HEAD_DIM, rows), bf16)
    moves = [(dz, dx) for dz in range(planes) for dx in range(across) if (dz, dx) != (0, 0)]

    def slot(dz, dx):
        return dz * across + dx - 1

    def present(dz, dx):
        return (x >= dx) if dz == 0 else (z >= dz)

    for dz, dx in moves:

        def clear(dz=dz, dx=dx):
            for k in range(kv_local):
                sel[slot(dz, dx), k] = jnp.zeros(sel.shape[2:], bf16)

        pl.when(jnp.logical_not(present(dz, dx)))(clear)
    for d in range(1, owners):

        def clear_sums(d=d):
            for k in range(kv_local):
                sums[me + d, k] = jnp.zeros(sums.shape[2:], bf16)

        pl.when(me + d < owners)(clear_sums)


    def remote(src, dst, send, recv, target):
        return pltpu.make_async_remote_copy(
            src_ref=src,
            dst_ref=dst,
            send_sem=send,
            recv_sem=recv,
            device_id={"kv": target},
            device_id_type=MESH,
        )

    above = lax.rem(me + across, owners)

    def own_copy(k, at):
        return remote(own.at[k, at], col[k].at[at], own_send.at[k], col_recv.at[k, 0], above)

    def col_of(dz, k):
        return col[(dz - 1) * kv_local + k]

    def up_copy(dz, k):
        return remote(
            col_of(dz, k), col_of(dz + 1, k), col_send.at[k, dz - 1], col_recv.at[k, dz], above
        )

    def side_copy(dz, dx, k):
        return remote(
            stage_x.at[dz, dx - 1, k],
            sel.at[slot(dz, dx), k],
            x_send.at[dz if dz else planes + dx - 1],
            near_recv.at[slot(dz, dx), k],
            z * across + (x + dx) % across,
        )

    def rank_at(step):
        if ranks % 2:
            return (rank + 1 + step) % ranks
        chip = (rank // 2 + 1 + step // 2) % (ranks // 2)
        return chip * 2 + (rank + step + 1) % 2

    def rank_from(step):
        if ranks % 2:
            return (rank + 2 * ranks - 1 - step) % ranks
        chip = (rank // 2 + ranks - 1 - step // 2) % (ranks // 2)
        return chip * 2 + (rank + step + 1) % 2

    own_group = pl.ds(rank * group, group)

    def piece_at(piece):
        return pl.ds(rank_at(piece) * group, group)

    def far_side_copy(dz, dx, k, piece):
        at = piece_at(piece)
        return remote(
            stage_x.at[dz, dx - 1, k, at],
            sel.at[slot(dz, dx), k, at],
            x_send.at[dz],
            far_recv.at[k, piece],
            z * across + (x + dx) % across,
        )

    def top_copy(dz, dx, k, piece):
        at = piece_at(piece)
        return remote(
            stage_t.at[dz - 1, dx, k, at],
            sel.at[slot(dz + 1, dx), k, at],
            t_send.at[dz - 1, 0 if dx == 0 else 1],
            far_recv.at[k, piece],
            lax.rem((z + 1) * across + (x + dx) % across, owners),
        )

    def help_copy(dz, dx, k):
        return remote(
            stage_t.at[dz - 1, dx, k, own_group],
            help_sel.at[dz - 1, dx - 1, k],
            t_send.at[dz - 1, 1],
            help_recv.at[k],
            z * across + (x + dx) % across,
        )

    def help_queries():
        at = pl.ds(pl.multiple_of(rank * rank_rows, rank_rows), rank_rows)
        below = lax.rem(me + owners - across, owners)
        return remote(qt.at[:, :, :, at], help_q, query_send.at[0], query_recv.at[0], below)

    def help_answer(k, n):
        src, dst = ((help_out, got_out), (help_stat, got_stat))[n]
        return remote(src.at[k], dst.at[k], answer_send.at[k, n], answer_recv.at[k, n], above)

    def gather(src, dst, source, k, device):
        row, base = source * kv_local + k, device * q_blocks

        def one(j, carry):
            dst[j] = src[jnp.maximum(pick[row, base + j], 0)]
            return carry

        lax.fori_loop(0, q_blocks, one, 0, unroll=4)

    def relay(dz, k):
        whole = (z >= dz) & ((z < last) | (dz == 1))

        def go():
            remote(col_of(dz, k), col_of(dz, k), own_send.at[k], col_recv.at[k, dz - 1], above).wait_recv()
            source = me - dz * across
            if dz + 1 < last:
                pl.when(z + 1 < last)(lambda: up_copy(dz, k).start())
            if dz + 1 <= last:

                def to_top():
                    for dx in range(across):
                        gather(
                            col_of(dz, k),
                            stage_t.at[dz - 1, dx, k],
                            source,
                            k,
                            (z + 1) * across + (x + dx) % across,
                        )
                    for dx in range(1, across):
                        help_copy(dz, dx, k).start()
                    for s in range(ranks - 1):
                        for dx in range(across):
                            top_copy(dz, dx, k, s).start()

                pl.when(z + 1 == last)(to_top)
            for dx in range(1, across):
                there = z * across + (x + dx) % across
                gather(col_of(dz, k), stage_x.at[dz, dx - 1, k], source, k, there)
                if dz < 2:
                    side_copy(dz, dx, k).start()
                else:
                    for piece in range(ranks):
                        far_side_copy(dz, dx, k, piece).start()
            gather(col_of(dz, k), sel.at[slot(dz, 0), k], source, k, me)

        pl.when(whole)(go)


    def norm_tile(i):
        t = tok[lax.rem(i, ring)].astype(f32)
        inv = lax.rsqrt(jnp.mean(t * t, axis=-1, keepdims=True) + norm_eps)
        normed[rows_at(i), :] = (t * inv * gain_row[...]).astype(bf16)
        pl.when(i + ring < tiles)(lambda: tok_copy(i + ring).start())

    def tables(i):
        row = pl.ds(me * tiles + i, 1)
        cos_c, sin_c = coarse[0, row, :], coarse[1, row, :]
        return fine[0] * cos_c - fine[1] * sin_c, fine[1] * cos_c + fine[0] * sin_c

    def project_kv(i):
        at = rows_at(i)
        y = jnp.dot(normed[at, :], w_kv[...], preferred_element_type=f32)
        cosine, sine = tables(i)
        for k in range(kv_local):
            if kv_local == 1:
                value = y[:, :LANES]
                key = turn(value, cosine, sine)
                keys, first = key, HEAD_DIM
            elif k % 2 == 0:
                key = turn(y[:, k * HEAD_DIM : k * HEAD_DIM + LANES], cosine, sine)
                value = y[:, kv_width + k * HEAD_DIM : kv_width + k * HEAD_DIM + LANES]
                keys, first = key, 0
            else:
                keys, first = swap(key), HEAD_DIM
            for t in range(TILE // (2 * SEL_BLOCK)):
                two = slice(t * 2 * SEL_BLOCK, (t + 1) * 2 * SEL_BLOCK)
                turned = value[two].T[first : first + HEAD_DIM]
                a, b = pack_pair(keys[two], turned)
                own[k, i * (TILE // SEL_BLOCK) + 2 * t] = a
                own[k, i * (TILE // SEL_BLOCK) + 2 * t + 1] = b
        ck[at, :] = y[:, 2 * kv_width : 3 * kv_width].astype(bf16).astype(f32)
        cv[at, :] = y[:, 3 * kv_width : 4 * kv_width].astype(bf16).astype(f32)

    def send_tile(i):
        here = pl.ds(i * (TILE // SEL_BLOCK), TILE // SEL_BLOCK)
        if planes > 1:
            pl.when(z < last)(lambda: own_copy(0, here).start())

    copies[0].wait()
    for c in range(gain_ref.shape[0]):
        gain_row[:, c * LANES : (c + 1) * LANES] = gain_ref[c : c + 1, :].astype(f32)
    tok_copy(0).wait()
    norm_tile(0)
    for copy in copies[1 : len(early)]:
        copy.wait()
    for i in range(2, min(ring, tiles)):
        tok_copy(i).start()
    for copy in copies[len(early) :]:
        copy.start()
    pl.semaphore_wait(barrier, owners + ranks - 2)

    def first_pass(i, carry):
        pl.when(i > 0)(lambda: send_tile(i - 1))
        tok_copy(i + 1).wait()
        norm_tile(i + 1)
        project_kv(i)
        return carry

    lax.fori_loop(0, tiles - 1, first_pass, 0)
    if tiles > 1:
        send_tile(tiles - 2)
    project_kv(tiles - 1)

    for copy in copies[len(early) : len(early) + len(late)]:
        copy.wait()
    send_tile(tiles - 1)


    for s in range(owners):
        for k in range(kv_local):
            place = chosen_ref[k] - s * span
            place = jnp.where((place >= 0) & (place < span), place, -1)
            found[s * kv_local + k : s * kv_local + k + 1, :] = jnp.max(place, axis=0, keepdims=True)
    to_smem.start()

    quarter = span // 4
    for k in range(1, kv_local):
        if planes > 1:
            pl.when(z < last)(lambda k=k: own_copy(k, pl.ds(0, quarter)).start())


    def summarize(x_ref, e_ref, i_ref, o_ref):
        embed = jnp.concatenate([e_ref[k].astype(f32) for k in range(kv_local)], axis=1)
        parts = [
            x_ref[pl.ds(c, blocks, stride=CMP_BLOCK), :] + embed[c : c + 1] for c in range(CMP_BLOCK)
        ]
        result = []
        for k in range(kv_local):
            if kv_local == 1:
                flat = jnp.concatenate([p.astype(bf16) for p in parts], axis=1)
            else:
                g, odd = k // 2 * LANES, k % 2
                low = low_lanes((blocks, LANES))
                cut = []
                for c in range(0, CMP_BLOCK, 2):
                    a, b = parts[c][:, g : g + LANES], parts[c + 1][:, g : g + LANES]
                    both = jnp.where(low, swap(a), b) if odd else jnp.where(low, a, swap(b))
                    cut.append(both.astype(bf16))
                flat = jnp.concatenate(cut, axis=1)
            hidden = jax.nn.gelu(nt_dot(flat, i_ref[k])).astype(bf16)
            result.append(jnp.dot(hidden, o_ref[k], preferred_element_type=f32))
        return result

    sk = summarize(ck, ke_ref, ki, ko_ref)
    sv = summarize(cv, ve_ref, vi, vo_ref)
    for k in range(kv_local):
        sums[me, k] = jnp.concatenate([sk[k], sv[k].T], axis=1).astype(bf16)

    def sum_up(dz, source):
        there = lax.rem(me + dz * across, owners)
        return remote(sums.at[source], sums.at[source], sum_send.at[0, dz], sum_recv.at[0, dz], there)

    def sum_side(dz, dx, source):
        there = z * across + (x + dx) % across
        return remote(sums.at[source], sums.at[source], sum_send.at[dx, dz], sum_recv.at[dx, dz], there)

    for dz in range(1, planes):
        pl.when(z + dz <= last)(lambda dz=dz: sum_up(dz, me).start())
    for dx in range(1, across):
        pl.when(x + dx < across)(lambda dx=dx: sum_side(0, dx, me).start())
    to_smem.wait()
    for dx in range(1, across):
        for k in range(kv_local):
            gather(own.at[k], stage_x.at[0, dx - 1, k], me, k, z * across + (x + dx) % across)
    everything = pl.ds(0, span)
    for k in range(1, kv_local):
        if planes > 1:
            pl.when(z < last)(lambda k=k: own_copy(k, pl.ds(quarter, span - quarter)).start())
    for dx in range(1, across):
        pl.when(x + dx < across)(lambda dx=dx: side_copy(0, dx, 0).start())


    mine = lax.broadcasted_iota(jnp.int32, (w_own.shape[0], w_gate.shape[0]), 0)
    branch = jnp.where(mine >= heads_local, 1, 0)
    wanted = branch * heads + rank * heads_local + mine - branch * heads_local
    wanted = jnp.where(mine < 2 * heads_local, wanted, -1)
    source = lax.broadcasted_iota(jnp.int32, mine.shape, 1)
    chooser = jnp.where(source == wanted, 1.0, 0.0).astype(bf16)
    w_own[...] = jnp.dot(chooser, w_gate[...], preferred_element_type=f32).astype(bf16)

    def second_pass(i, carry):
        at = rows_at(i)
        n = normed[at, :]
        y = jnp.dot(n, w_q[...], preferred_element_type=f32)
        cosine, sine = tables(i)
        for k in range(kv_local):
            v = y[:, k * LANES : (k + 1) * LANES] * scale
            for ref, q in ((qp, v), (qt, turn(v, cosine, sine))):
                turned = q.T.astype(bf16)
                for u in range(2):
                    ref[k, u, :HEAD_DIM, at] = turned[u * HEAD_DIM : (u + 1) * HEAD_DIM]
        gate[:, at] = jax.nn.sigmoid(nt_dot(w_own[...], n))
        return carry

    lax.fori_loop(0, tiles // 2, second_pass, 0)
    for dz in range(1, planes):

        def pass_on(dz=dz):
            below = me - dz * across
            sum_up(dz, below).wait_recv()
            for dx in range(1, across):
                sum_side(dz, dx, below).start()

        pl.when(z >= dz)(pass_on)
    lax.fori_loop(tiles // 2, tiles, second_pass, 0)
    if planes > 2:
        pl.when(z == last)(lambda: help_queries().start())
    relays = [(dz, k) for dz in range(1, max(2, last)) for k in range(kv_local)] if planes > 1 else []


    if relays:
        relay(*relays[0])
    for dx in range(1, across):
        for k in range(1, kv_local):
            pl.when(x + dx < across)(lambda dx=dx, k=k: side_copy(0, dx, k).start())
    for dz in range(planes):
        for dx in range(1, across):
            there = lax.rem((z - dz + planes) * across + (x + across - dx) % across, owners)
            pl.when(present(dz, dx))(
                lambda dz=dz, dx=dx, there=there: sum_side(dz, dx, there).wait_recv()
            )

    def gate_row(branch, head, at):
        return gate[branch * heads_local + head : branch * heads_local + head + 1, at]

    for k in range(kv_local):
        vsum[k] = values_of([sums[s, k] for s in range(owners)])

    def compress(i, carry):
        at = rows_at(i)
        lane = lax.broadcasted_iota(jnp.int32, (1, 2 * TILE), 1)
        pos = me * rows + i * TILE + jnp.where(lane >= TILE, lane - TILE, lane)
        block = lax.broadcasted_iota(jnp.int32, (owners * blocks, 1), 0)
        allowed = (block + 1) * CMP_BLOCK - 1 <= pos
        for k in range(kv_local):
            keys = jnp.concatenate([sums[s, k] for s in range(owners)], axis=0)
            q = jnp.concatenate([qp[k, 0, :, at], qp[k, 1, :, at]], axis=1)
            s = jnp.where(allowed, jnp.dot(keys, q, preferred_element_type=f32), MASKED)
            top = jnp.max(s, axis=0, keepdims=True)
            e = jnp.exp(s - top).astype(bf16)
            o = jnp.dot(vsum[k], e, preferred_element_type=f32)
            o = jnp.where(pos >= CMP_BLOCK - 1, o[:HEAD_DIM] / o[HEAD_DIM : HEAD_DIM + 1], 0.0)
            for u in range(2):
                part = o[:, u * TILE : (u + 1) * TILE] * gate_row(0, 2 * k + u, at)
                oc[k, u * HEAD_DIM : (u + 1) * HEAD_DIM, at] = part
        return carry

    bounds = [tiles * n // kv_local for n in range(kv_local + 1)]
    for k in range(kv_local):
        if k > 0 and planes > 1:
            relay(1, k)
        lax.fori_loop(bounds[k], bounds[k + 1], compress, 0)


    def is_top(dz):
        return (z == last) & (dz >= 2)

    def wait_side(dz, dx, k):
        pl.when(present(dz, dx))(lambda: side_copy(dz, dx, k).wait_recv())

    def bias_of(usable):
        return [jnp.where(u, 0.0, MASKED).astype(f32) for u in usable]

    def add_bias(s, bias):
        cut = [s[n * SEL_BLOCK : (n + 1) * SEL_BLOCK] + b for n, b in enumerate(bias)]
        return jnp.concatenate(cut, axis=0)

    def far_parts(some_moves, k, j):
        parts, usable = [], []
        for dz, dx in some_moves:
            parts.append(sel[slot(dz, dx), k, j])
            source = lax.rem(me - dz * across - x + (x + across - dx) % across + owners, owners)
            usable.append((pick[source * kv_local + k, me * q_blocks + j] >= 0) & present(dz, dx))
        return parts, usable

    near_moves = [m for m in moves if m[0] < 2]
    far_moves = [m for m in moves if m[0] >= 2]
    own_blocks = Q_BLOCK // SEL_BLOCK

    def queries(k, j):
        at = pl.ds(pl.multiple_of(j * Q_BLOCK, Q_BLOCK), Q_BLOCK)
        return jnp.concatenate([qt[k, 0, :, at], qt[k, 1, :, at]], axis=1)

    def scores(parts, k, j):
        keys = jnp.concatenate(parts, axis=0)
        return jnp.dot(keys, queries(k, j), preferred_element_type=f32)

    unroll = group if group < 4 else 4

    def answer(k):
        def go():
            if k == 0:
                help_queries().wait_recv()
            if across > 1:
                everyone = help_sel.at[:, :, k]
                remote(everyone, everyone, t_send.at[0, 0], help_recv.at[k], above).wait_recv()
            fars, ss = [], []
            for u in range(group):
                parts, usable = [], []
                for dz in range(1, planes - 1):
                    for dx in range(across):
                        block = stage_t[dz - 1, 0, k, rank * group + u] if dx == 0 else help_sel[dz - 1, dx - 1, k, u]
                        source = lax.rem((z - dz + planes) * across + (x + across - dx) % across, owners)
                        there = lax.rem(me + across, owners) * q_blocks + rank * group + u
                        parts.append(block)
                        usable.append(pick[source * kv_local + k, there] >= 0)
                cut = slice(u * Q_BLOCK, (u + 1) * Q_BLOCK)
                q = jnp.concatenate([help_q[k, 0, :, cut], help_q[k, 1, :, cut]], axis=1)
                s = jnp.dot(jnp.concatenate(parts, axis=0), q, preferred_element_type=f32)
                fars.append(parts)
                ss.append(add_bias(s, bias_of(usable)))
            tops = [jnp.max(s, axis=0, keepdims=True) for s in ss]
            es = [jnp.exp(s - t).astype(bf16) for s, t in zip(ss, tops)]
            outs = [jnp.dot(values_of(p), e, preferred_element_type=f32) for p, e in zip(fars, es)]
            row = lax.broadcasted_iota(jnp.int32, (2, 2 * Q_BLOCK), 0)
            for u in range(group):
                help_out[k, u] = outs[u][:HEAD_DIM].astype(bf16)
                help_stat[k, u] = jnp.where(row == 0, outs[u][HEAD_DIM : HEAD_DIM + 1], tops[u])
            for n in range(2):
                help_answer(k, n).start()

        pl.when(z == last - 1)(go)

    def near(k, some, carry):
        row = lax.broadcasted_iota(jnp.int32, (Q_BLOCK, 2 * Q_BLOCK), 0)
        lane = lax.broadcasted_iota(jnp.int32, row.shape, 1)
        lane = jnp.where(lane >= Q_BLOCK, lane - Q_BLOCK, lane)
        js = [some * unroll + u for u in range(unroll)]
        all_parts, ss = [], []
        for j in js:
            parts = [own[k, j * own_blocks + b] for b in range(own_blocks)]
            mine = pick[me * kv_local + k, me * q_blocks + j]
            parts.append(own[k, jnp.maximum(mine, 0)])
            more, usable = far_parts(near_moves, k, j)
            bias = bias_of([(mine >= 0) & (mine < j * own_blocks)] + usable)
            all_parts.append(parts + more)
            s = scores(all_parts[-1], k, j)
            close = jnp.where(row > lane, MASKED, s[:Q_BLOCK])
            ss.append(jnp.concatenate([close, add_bias(s[Q_BLOCK:], bias)], axis=0))
        tops = [jnp.max(s, axis=0, keepdims=True) for s in ss]
        es = [jnp.exp(s - top).astype(bf16) for s, top in zip(ss, tops)]
        for j, parts, e, top in zip(js, all_parts, es, tops):
            part_out[k, j] = jnp.dot(values_of(parts), e, preferred_element_type=f32)
            part_top[k, j] = top
        return carry

    for k in range(kv_local):
        for dz, dx in near_moves:
            if dx:
                wait_side(dz, dx, k)
        lax.fori_loop(0, q_blocks // unroll, functools.partial(near, k), 0)
        if k > 0 and far_moves:
            answer(k - 1)
        for dz in range(2, last):
            relay(dz, k)

    def wait_far(piece, k):
        if not far_moves:
            return
        at = piece_at(piece)
        own_piece = isinstance(piece, int) and piece == ranks - 1

        def wait(first, count):
            region = sel.at[pl.ds(first, count), k, at]
            remote(region, region, x_send.at[0], far_recv.at[k, piece], above).wait_recv()

        if not own_piece:
            pl.when(z == last)(lambda: wait(slot(2, 0), (planes - 2) * across))
        if across > 1:
            for dz in range(2, last):
                pl.when(z == dz)(lambda: wait(slot(2, 1), across - 1))

    def mix_copy(k, step):
        target = rank_at(step)
        at = pl.ds(pl.multiple_of(target * rank_rows, rank_rows), rank_rows)
        return pltpu.make_async_remote_copy(
            src_ref=mix.at[k, at],
            dst_ref=got.at[rank, k],
            send_sem=mix_send.at[k],
            recv_sem=mix_recv.at[k],
            device_id={"tp": target},
            device_id_type=MESH,
        )

    def outputs(k, u, size):
        at = pl.ds(pl.multiple_of(u * Q_BLOCK, Q_BLOCK), size * Q_BLOCK)
        from_mix = pl.ds(pl.multiple_of(rank * rank_rows + u * Q_BLOCK, Q_BLOCK), size * Q_BLOCK)
        shares, weights = [], []
        for step in range(ranks):
            source = rank_from(step) if step < ranks - 1 else rank
            shares.append(got[source, k, at, :] if step < ranks - 1 else mix[k, from_mix, :])
            weights.append(wo[pl.ds(pl.multiple_of((source * kv_local + k) * LANES, LANES), LANES), :])
        shares, weights = jnp.concatenate(shares, axis=1), jnp.concatenate(weights, axis=0)
        return at, jnp.dot(shares, weights, preferred_element_type=f32)

    def every_mix(k):
        return pltpu.make_async_remote_copy(
            src_ref=got.at[pl.ds(0, ranks - 1), k],
            dst_ref=got.at[pl.ds(0, ranks - 1), k],
            send_sem=mix_send.at[k],
            recv_sem=mix_recv.at[k],
            device_id={"tp": rank_at(0)},
            device_id_type=MESH,
        )

    def add_head(k):
        every_mix(k).wait_recv()

        two = 2 if group % 2 == 0 else 1

        def part(n, carry):
            at, more = outputs(k, n * two, two)
            acc[at, :] = more if k == 0 else acc[at, :] + more
            return carry

        lax.fori_loop(0, group // two, part, 0)

    copies[-1].wait()

    def late(k, blocks_of):
        ats = [pl.ds(pl.multiple_of(j * Q_BLOCK, Q_BLOCK), Q_BLOCK) for j in blocks_of]
        outs = [part_out[k, j] for j in blocks_of]
        if far_moves:
            fars = [far_parts(far_moves, k, j) for j in blocks_of]
            ss = [scores(parts, k, j) for (parts, _), j in zip(fars, blocks_of)]
            ss = [add_bias(s, bias_of(usable)) for s, (_, usable) in zip(ss, fars)]
            old = [part_top[k, j] for j in blocks_of]
            new = [jnp.maximum(t, jnp.max(s, axis=0, keepdims=True)) for t, s in zip(old, ss)]
            es = [jnp.exp(s - t).astype(bf16) for s, t in zip(ss, new)]
            more = [
                jnp.dot(values_of(parts), e, preferred_element_type=f32) for (parts, _), e in zip(fars, es)
            ]
            outs = [o * jnp.exp(a - b) + m for o, a, b, m in zip(outs, old, new, more)]
        settle(k, ats, [(out[:HEAD_DIM], out[HEAD_DIM : HEAD_DIM + 1]) for out in outs])

    def settle(k, ats, outs):
        for at, (value, total) in zip(ats, outs):
            o = value / total
            o = [o[:, n * Q_BLOCK : (n + 1) * Q_BLOCK] * gate_row(1, 2 * k + n, at) for n in range(2)]
            turned = oc[k, :, at] + jnp.concatenate(o, axis=0)
            mix[k, at, :] = turned.T.astype(bf16)

    def answered(k):
        for n in range(2):
            help_answer(k, n).wait_recv()
        ats, outs = [], []
        for u in range(group):
            j = rank * group + u
            out, top, more, stat = part_out[k, j], part_top[k, j], got_out[k, u].astype(f32), got_stat[k, u]
            both = jnp.maximum(top, stat[1:2])
            a, b = jnp.exp(top - both), jnp.exp(stat[1:2] - both)
            total = out[HEAD_DIM : HEAD_DIM + 1] * a + stat[0:1] * b
            ats.append(pl.ds(pl.multiple_of(j * Q_BLOCK, Q_BLOCK), Q_BLOCK))
            outs.append((out[:HEAD_DIM] * a + more * b, total))
        settle(k, ats, outs)

    def choose(k, step, carry):
        pl.when((step > 0) & (step < ranks - 2))(lambda: mix_copy(k, step - 1).start())
        wait_far(step, k)
        late(k, [rank_at(step) * group + u for u in range(group)])
        return carry

    for k in range(kv_local):
        lax.fori_loop(0, ranks - 2, functools.partial(choose, k), 0)
        if ranks > 2:
            mix_copy(k, ranks - 3).start()
        if k == 0 and far_moves:
            answer(kv_local - 1)
        if k > 0:
            add_head(k - 1)
        lax.fori_loop(ranks - 2, ranks - 1, functools.partial(choose, k), 0)
        mix_copy(k, ranks - 2).start()
        def mine(k=k):
            wait_far(ranks - 1, k)
            late(k, [rank * group + u for u in range(group)])

        if far_moves:
            pl.when(z == last)(functools.partial(answered, k))
            pl.when(z < last)(mine)
        else:
            mine()
    every_mix(kv_local - 1).wait_recv()
    two = 2 if group % 2 == 0 else 1
    for n in range(0, group, two):
        at, more = outputs(kv_local - 1, n, two)
        out_ref[at, :] = (more if kv_local == 1 else acc[at, :] + more).astype(bf16)


    for k in range(kv_local):
        if planes > 1:
            pl.when(z < last)(lambda k=k: own_copy(k, everything).wait_send())

    def sent(region, send):
        return remote(region, region, send, sum_recv.at[0, 0], above)

    for dx in range(1, across):
        pl.when(x + dx < across)(
            lambda dx=dx: sent(stage_x.at[0, dx - 1], x_send.at[planes + dx - 1]).wait_send()
        )
    for dz, k in relays:
        whole = (z >= dz) & ((z < last) | (dz == 1))
        if dz + 1 < last:
            pl.when(whole & (z + 1 < last))(lambda dz=dz, k=k: up_copy(dz, k).wait_send())
        if k == 0 and dz + 1 <= last:

            def sent_top(dz=dz):
                most = pl.ds(0, q_blocks - group)
                sent(stage_t.at[dz - 1, 0, :, most], t_send.at[dz - 1, 0]).wait_send()
                if across > 1:
                    sent(stage_t.at[dz - 1, pl.ds(1, across - 1)], t_send.at[dz - 1, 1]).wait_send()

            pl.when(whole & (z + 1 == last))(sent_top)
        if k == 0 and across > 1:
            pl.when(whole)(lambda dz=dz: sent(stage_x.at[dz], x_send.at[dz]).wait_send())
    for dz in range(1, planes):
        pl.when(z + dz <= last)(lambda dz=dz: sum_up(dz, me).wait_send())
    for dx in range(1, across):
        pl.when(x + dx < across)(lambda dx=dx: sum_side(0, dx, me).wait_send())
        for dz in range(1, planes):
            pl.when(z >= dz)(lambda dz=dz, dx=dx: sum_side(dz, dx, me - dz * across).wait_send())
    for k in range(kv_local):
        every_mix(k).wait_send()
        if far_moves:
            for n in range(2):
                pl.when(z == last - 1)(lambda k=k, n=n: help_answer(k, n).wait_send())
    if far_moves:
        pl.when(z == last)(lambda: help_queries().wait_send())


def position_tables(rows, owners):
    half = HEAD_DIM // 2
    lane = np.arange(LANES)
    inverse = ROPE_BASE ** (-(lane % half).astype(np.float64) / half)
    sign = np.where(lane % HEAD_DIM < half, -1.0, 1.0)

    def both(positions):
        phase = positions[:, None].astype(np.float64) * inverse[None, :]
        return np.stack([np.cos(phase), np.sin(phase) * sign]).astype(np.float32)

    return both(np.arange(TILE)), both(np.arange(0, owners * rows, TILE))


def per_device(
    tokens,
    norm_gain,
    query_weight,
    cmp_key_weight,
    cmp_value_weight,
    sel_key_weight,
    sel_value_weight,
    branch_weight,
    key_embed,
    key_inner,
    key_outer,
    value_embed,
    value_inner,
    value_outer,
    out_weight,
    chosen,
):
    rows, width = tokens.shape
    kv_local = key_embed.shape[0]
    owners, ranks = lax.axis_size("kv"), lax.axis_size("tp")
    planes = PLANES if owners % PLANES == 0 else 1
    across = owners // planes
    span = rows // SEL_BLOCK
    q_blocks = rows // Q_BLOCK
    blocks = rows // CMP_BLOCK
    rank_rows = rows // ranks
    kv_width = kv_local * HEAD_DIM

    weights = [sel_key_weight, sel_value_weight, cmp_key_weight, cmp_value_weight]
    if kv_width % LANES:
        weights = [jnp.concatenate(weights, axis=1)]
    fine, coarse = position_tables(rows, owners)
    operands = (
        chosen.transpose(0, 2, 1),
        norm_gain.reshape(width // LANES, LANES),
        key_embed,
        key_outer,
        value_embed,
        value_outer,
        tokens,
        query_weight,
        branch_weight.transpose(0, 2, 1),
        key_inner.transpose(0, 2, 1),
        value_inner.transpose(0, 2, 1),
        out_weight,
        jnp.asarray(fine),
        jnp.asarray(coarse),
        *weights,
    )
    vmem = pl.BlockSpec(memory_space=pltpu.VMEM)
    hbm = pl.BlockSpec(memory_space=pl.ANY)
    dma = pltpu.SemaphoreType.DMA
    picked = (q_blocks, SEL_BLOCK, LANES)
    whole = (span, SEL_BLOCK, LANES)
    n_local = 3 + len(weights) + 8 + 2 + 2
    picks = (owners * kv_local, chosen.shape[1])
    down = max(planes - 2, 1)
    n_pieces = ranks
    group = rank_rows // Q_BLOCK
    return pl.pallas_call(
        functools.partial(layer_kernel, planes, len(weights)),
        in_specs=[hbm] * len(operands),
        out_specs=vmem,
        out_shape=pltpu.VMEM((rank_rows, out_weight.shape[1]), bf16),
        scratch_shapes=[
            pltpu.SMEM(picks, jnp.int32),
            pltpu.VMEM(picks, jnp.int32),
            pltpu.VMEM((kv_local, chosen.shape[2], chosen.shape[1]), jnp.int32),
            pltpu.VMEM((width // LANES, LANES), bf16),
            pltpu.VMEM((1, width), f32),
            pltpu.VMEM(key_embed.shape, bf16),
            pltpu.VMEM(key_outer.shape, bf16),
            pltpu.VMEM(value_embed.shape, bf16),
            pltpu.VMEM(value_outer.shape, bf16),
            pltpu.VMEM((kv_local, *whole), bf16),
            pltpu.VMEM((max(owners - 1, 1), kv_local, *picked), bf16),
            pltpu.VMEM((kv_local, q_blocks, HEAD_DIM + ONES, 2 * Q_BLOCK), f32),
            pltpu.VMEM((kv_local, q_blocks, 1, 2 * Q_BLOCK), f32),
            pltpu.VMEM((max(planes - 1, 1), max(across - 1, 1), kv_local, *picked), bf16),
            pltpu.VMEM((down, across, kv_local, *picked), bf16),
            pltpu.VMEM((kv_local, 2, LANES, rank_rows), bf16),
            pltpu.VMEM((down, max(across - 1, 1), kv_local, group, SEL_BLOCK, LANES), bf16),
            pltpu.VMEM((kv_local, group, HEAD_DIM, 2 * Q_BLOCK), bf16),
            pltpu.VMEM((kv_local, group, 2, 2 * Q_BLOCK), f32),
            pltpu.VMEM((kv_local, group, HEAD_DIM, 2 * Q_BLOCK), bf16),
            pltpu.VMEM((kv_local, group, 2, 2 * Q_BLOCK), f32),
            pltpu.VMEM((min(3, rows // TILE), TILE, width), bf16),
            pltpu.VMEM(tokens.shape, bf16),
            pltpu.VMEM((width, 4 * kv_width), bf16),
            pltpu.VMEM(query_weight.shape, bf16),
            pltpu.VMEM((2 * branch_weight.shape[2], width), bf16),
            pltpu.VMEM((16, width), bf16),
            pltpu.VMEM(out_weight.shape, bf16),
            pltpu.VMEM(fine.shape, f32),
            pltpu.VMEM(coarse.shape, f32),
            pltpu.VMEM((kv_local, HEAD_DIM, key_inner.shape[1]), bf16),
            pltpu.VMEM((kv_local, HEAD_DIM, key_inner.shape[1]), bf16),
            pltpu.VMEM((kv_local, 2, LANES, rows), bf16),
            pltpu.VMEM((kv_local, 2, LANES, rows), bf16),
            pltpu.VMEM((kv_local, HEAD_DIM + ONES, owners * blocks), bf16),
            pltpu.VMEM((rows, kv_width), f32),
            pltpu.VMEM((rows, kv_width), f32),
            pltpu.VMEM((16, rows), f32),
            pltpu.VMEM((owners, kv_local, blocks, LANES), bf16),
            pltpu.VMEM((kv_local, LANES, rows), f32),
            pltpu.VMEM((kv_local, rows, LANES), bf16),
            pltpu.VMEM((ranks, kv_local, rank_rows, LANES), bf16),
            pltpu.VMEM((rank_rows, out_weight.shape[1]), f32),
            dma((min(3, rows // TILE),)),
            dma((n_local,)),
            dma((kv_local,)),
            dma((kv_local, down)),
            dma((kv_local, max(planes - 1, 1))),
            dma((planes + across,)),
            dma((down, 2)),
            dma((max(2 * across - 1, 1), kv_local)),
            dma((kv_local, n_pieces)),
            dma((across, planes)),
            dma((across, planes)),
            dma((kv_local,)),
            dma((kv_local,)),
            dma((1,)),
            dma((1,)),
            dma((kv_local,)),
            dma((kv_local, 2)),
            dma((kv_local, 2)),
        ]
        + [pltpu.VMEM(whole, bf16)] * (kv_local * max(planes - 1, 1)),
        compiler_params=pltpu.CompilerParams(
            collective_id=0, has_side_effects=True, vmem_limit_bytes=56 * 1024 * 1024
        ),
        cost_estimate=pl.CostEstimate(flops=int(3e10), bytes_accessed=int(2e7), transcendentals=0),
        name="layer",
    )(*operands)


def solution(mesh):
    placed = (
        P("kv", None),
        P(),
        P(None, "tp"),
        P(None, "tp"),
        P(None, "tp"),
        P(None, "tp"),
        P(None, "tp"),
        P(),
        P("tp", None, None),
        P("tp", None, None),
        P("tp", None, None),
        P("tp", None, None),
        P("tp", None, None),
        P("tp", None, None),
        P(),
        P("tp", None, None),
    )
    return jax.shard_map(
        per_device, mesh=mesh, in_specs=placed, out_specs=P(("kv", "tp"), None), check_vma=False
    )
```
